512 devices in a mesh: kv: 64 (over z, y), tp: 8 (over x, core).
Axes of the slice: x: 4, y: 8, z: 8, core: 2. Of those that a mesh axis runs over, the one named last changes fastest.
Arguments:
- tokens: bfloat16 [128, 4096], P(None, 'kv'), may hold values from -16 to 16
- mix_gain: bfloat16 [4096], P('kv'), may hold values from 0.099609375 to 1.8984375
- ffn_gain: bfloat16 [4096], P('kv'), may hold values from 0.099609375 to 1.8984375
- w_query: bfloat16 [4096, 2048], P('kv', 'tp'), may hold values from -0.09375 to 0.09375
- w_key: bfloat16 [4096, 2048], P('kv', 'tp'), may hold values from -0.09375 to 0.09375
- w_value: bfloat16 [4096, 4096], P('kv', 'tp'), may hold values from -0.09375 to 0.09375
- w_gate: bfloat16 [4096, 4096], P('kv', 'tp'), may hold values from -0.09375 to 0.09375
- w_decay: bfloat16 [4096, 2048], P('kv', 'tp'), may hold values from -0.375 to 0.375
- decay_bias: float32 [2048], P('tp'), may hold values from -7 to 4
- head_gain: bfloat16 [512], replicated, may hold values from 0.099609375 to 1.8984375
- w_output: bfloat16 [4096, 4096], P('tp', 'kv'), may hold values from -0.09375 to 0.09375
- w_ffgate: bfloat16 [4096, 11008], P('kv', 'tp'), may hold values from -0.09375 to 0.09375
- w_ffup: bfloat16 [4096, 11008], P('kv', 'tp'), may hold values from -0.09375 to 0.09375
- w_down: bfloat16 [11008, 4096], P('tp', 'kv'), may hold values from -0.0546875 to 0.0546875
- state: float32 [128, 8, 256, 512], P('kv', 'tp'), may hold values from -6 to 6
Outputs:
- mixed: bfloat16 [128, 4096], P(None, 'kv')
- new_state: float32 [128, 8, 256, 512], P('kv', 'tp')
The draws below stay inside these ranges and needn't reach their ends.
All inputs are finite; a program needn't handle non-finite values.
Results may differ from the reference program's by a relative error of at most 0.015.
Values may be sent and summed in bfloat16 or wider, within the bound.
No kernel may reach another device: no remote copies, remote signals or barrier semaphores. Data moves between devices by JAX's collectives and lax.ppermute only.
A program may use at most 64 MiB of HBM per device.

```python
import jax
import jax.numpy as jnp
from jax import lax

D = 4096
HEADS = 8
DK = 256
DV = 512
FF = 11008
SEQS = 128
GROUPS = 8


def draw_tokens(key, part):
    column = jnp.arange(D, dtype=jnp.float32) / D
    column_scale = 0.4 * jnp.exp(jnp.log(6.0) * column)
    values = jnp.clip(jax.random.normal(key, (SEQS, D), jnp.float32), -4.0, 4.0) * column_scale
    return values.astype(jnp.bfloat16)


def shard_levels(key, dims, pieces, least, largest):
    def one(dim, parts):
        steps = jax.random.uniform(jax.random.fold_in(jax.random.fold_in(key, 6), dim), (parts,), jnp.float32, least / len(pieces), largest / len(pieces))
        return jnp.repeat(jnp.exp(steps), dims[dim] // parts).reshape((-1,) + (1,) * (len(dims) - dim - 1))

    factor_of = one(*pieces[0])
    for cut in pieces[1:]:
        factor_of = factor_of * one(*cut)
    return factor_of


def normal_values(stream_key, extent, scale, reach, cuts=(), kind=jnp.bfloat16):
    values = jax.random.normal(stream_key, extent, jnp.float32) * scale
    if len(cuts) > 0:
        values = shard_levels(stream_key, extent, cuts, -0.22, 0.18) * values
    return jnp.clip(values, min=-reach, max=reach).astype(kind)


def setup_inputs(seed: int = 0) -> dict:
    key_of = jax.random.split(jax.random.key(seed), 16)
    tokens = draw_tokens(jax.random.fold_in(key_of[15], 71), 0)
    mix_gain = jnp.clip(1.0 + 0.18 * jax.random.normal(key_of[1], (D,), jnp.float32), 0.099609375, 1.8984375).astype(jnp.bfloat16)
    ffn_gain = jnp.clip(1.0 + 0.18 * jax.random.normal(key_of[2], (D,), jnp.float32), 0.099609375, 1.8984375).astype(jnp.bfloat16)
    w_query = normal_values(key_of[3], (D, HEADS * DK), D ** -0.5, 0.09375, ((0, 64), (1, 8)))
    w_key = normal_values(key_of[4], (D, HEADS * DK), D ** -0.5, 0.09375, ((0, 64), (1, 8)))
    w_value = normal_values(key_of[5], (D, HEADS * DV), D ** -0.5, 0.09375, ((0, 64), (1, 8)))
    w_gate = normal_values(key_of[6], (D, HEADS * DV), D ** -0.5, 0.09375, ((0, 64), (1, 8)))
    w_decay = normal_values(key_of[7], (D, HEADS * DK), (D // 16) ** -0.5, 0.375, ((0, 64), (1, 8)))
    decay_bias = jnp.clip(-7.0 + 11.0 * jax.random.uniform(key_of[8], (HEADS * DK,), jnp.float32) ** shard_levels(key_of[8], (HEADS * DK,), ((0, 8),), -0.2, 0.2), -7.0, 4.0)
    head_gain = jnp.clip(1.0 + 0.18 * jax.random.normal(key_of[9], (DV,), jnp.float32), 0.099609375, 1.8984375).astype(jnp.bfloat16)
    w_output = normal_values(key_of[10], (HEADS * DV, D), (HEADS * DV) ** -0.5, 0.09375, ((0, 8), (1, 64)))
    w_ffgate = normal_values(key_of[11], (D, FF), D ** -0.5, 0.09375, ((0, 64), (1, 8)))
    w_ffup = normal_values(key_of[12], (D, FF), D ** -0.5, 0.09375, ((0, 64), (1, 8)))
    w_down = normal_values(key_of[13], (FF, D), FF ** -0.5, 0.0546875, ((0, 8), (1, 64)))
    state = normal_values(key_of[14], (SEQS, HEADS, DK, DV), 1.0, 6.0, ((0, 64), (1, 8)), jnp.float32)
    return {"tokens": tokens, "mix_gain": mix_gain, "ffn_gain": ffn_gain, "w_query": w_query, "w_key": w_key, "w_value": w_value, "w_gate": w_gate, "w_decay": w_decay, "decay_bias": decay_bias, "head_gain": head_gain, "w_output": w_output, "w_ffgate": w_ffgate, "w_ffup": w_ffup, "w_down": w_down, "state": state}


epsilon = 1e-06

def reference(tokens, mix_gain, ffn_gain, w_query, w_key, w_value, w_gate, w_decay, decay_bias, head_gain, w_output, w_ffgate, w_ffup, w_down, state):
    seq_count = tokens.shape[0]
    model_width = tokens.shape[1]
    head_count = state.shape[1]
    key_dim = state.shape[2]
    val_dim = state.shape[3]
    token_f32 = tokens.astype(jnp.float32)
    mix_rms = lax.rsqrt(lax.optimization_barrier(jnp.sum(token_f32 * token_f32, axis=1)) / model_width + epsilon)[:, None]
    mix_in = (token_f32 * mix_gain.astype(jnp.float32)).astype(jnp.bfloat16)

    def project(weight):
        return jnp.dot(mix_in, weight, preferred_element_type=jnp.float32) * mix_rms
    queries = project(w_query).reshape(seq_count, head_count, key_dim) * key_dim ** (-0.5)
    key_rows = project(w_key).reshape(seq_count, head_count, key_dim)
    value_rows = project(w_value).reshape(seq_count, head_count, val_dim)
    gate_rows = project(w_gate).reshape(seq_count, head_count, val_dim)
    decay_rows = (project(w_decay) + decay_bias).reshape(seq_count, head_count, key_dim)
    log_decay = jax.nn.log_sigmoid(decay_rows) / 16.0
    new_state = jnp.exp(log_decay)[..., None] * state + key_rows[..., :, None] * value_rows[..., None, :]
    attended = jnp.einsum('bhk,bhkv->bhv', queries, new_state, precision=lax.Precision.HIGHEST)
    attended = attended * lax.rsqrt(lax.optimization_barrier(jnp.sum(attended * attended, axis=2, keepdims=True)) / val_dim + epsilon)
    head_out = (attended * head_gain.astype(jnp.float32) * jax.nn.silu(gate_rows)).reshape(seq_count, head_count * val_dim).astype(jnp.bfloat16)
    group_cols = head_count * val_dim // GROUPS
    attn_out = jnp.zeros((seq_count, model_width), jnp.float32)
    for group_idx in range(GROUPS):
        partial_value = jnp.dot(head_out[:, group_idx * group_cols:(group_idx + 1) * group_cols], w_output[group_idx * group_cols:(group_idx + 1) * group_cols], preferred_element_type=jnp.float32)
        attn_out = attn_out + lax.optimization_barrier(partial_value.astype(jnp.bfloat16)).astype(jnp.float32)
    residual_mid = (token_f32 + attn_out).astype(jnp.bfloat16)
    mid_f32 = residual_mid.astype(jnp.float32)
    ffn_rms = lax.rsqrt(lax.optimization_barrier(jnp.sum(mid_f32 * mid_f32, axis=1)) / model_width + epsilon)[:, None]
    ffn_in = (mid_f32 * ffn_gain.astype(jnp.float32)).astype(jnp.bfloat16)
    gate_sum = jnp.dot(ffn_in, w_ffgate, preferred_element_type=jnp.float32)
    up_sum = jnp.dot(ffn_in, w_ffup, preferred_element_type=jnp.float32)
    hidden = (jax.nn.silu(gate_sum * ffn_rms) * (up_sum * ffn_rms)).astype(jnp.bfloat16)
    unit_cols = hidden.shape[1] // GROUPS
    ffn_out = jnp.zeros((seq_count, model_width), jnp.float32)
    for group_idx in range(GROUPS):
        partial_value = jnp.dot(hidden[:, group_idx * unit_cols:(group_idx + 1) * unit_cols], w_down[group_idx * unit_cols:(group_idx + 1) * unit_cols], preferred_element_type=jnp.float32)
        ffn_out = ffn_out + lax.optimization_barrier(partial_value.astype(jnp.bfloat16)).astype(jnp.float32)
    mixed = (mid_f32 + ffn_out).astype(jnp.bfloat16)
    return (mixed, new_state)
```

```python
import functools

import jax
import jax.numpy as jnp
from jax import lax
from jax.experimental import pallas as pl
from jax.experimental.pallas import tpu as pltpu
from jax.sharding import PartitionSpec as P

epsilon = 1e-06


def padded(n):
    return -(-n // 128) * 128


def in_vmem(x):
    return pltpu.with_memory_space_constraint(x, pltpu.VMEM)


def project_kernel(tok_ref, gain_ref, wq, wk, wv, wg, wd, out_ref, tok, gain, q, k, v, g, d, sems):
    pairs = ((tok_ref, tok), (gain_ref, gain), (wq, q), (wk, k), (wv, v), (wg, g), (wd, d))
    copies = [pltpu.make_async_copy(a, b, sems.at[i]) for i, (a, b) in enumerate(pairs)]
    for c in copies:
        c.start()
    copies[0].wait()
    copies[1].wait()
    x = tok[...].astype(jnp.float32).T
    mix_in = (x * gain[...].astype(jnp.float32)).astype(jnp.bfloat16)
    squares = jnp.sum(x * x, axis=1, keepdims=True)
    at = 0
    for i, w in enumerate((q, k, v, g, d)):
        copies[2 + i].wait()
        n = w.shape[1]
        part = jnp.dot(mix_in, w[...], preferred_element_type=jnp.float32)
        out_ref[:, at : at + n] = part.astype(jnp.bfloat16)
        at += n
    rest = out_ref.shape[1] - at
    lane = lax.broadcasted_iota(jnp.int32, (x.shape[0], rest), 1)
    out_ref[:, at:] = jnp.where(lane == 0, squares, 0.0).astype(jnp.bfloat16)


def project(tok_t, gain, weights):
    width, rows = tok_t.shape
    total = sum(w.shape[1] for w in weights)
    arrays = (tok_t, gain, *weights)
    return pl.pallas_call(
        project_kernel,
        out_shape=pltpu.VMEM((rows, total + 128), jnp.bfloat16),
        in_specs=[pl.BlockSpec(memory_space=pl.ANY)] * len(arrays),
        out_specs=pl.BlockSpec(memory_space=pltpu.VMEM),
        scratch_shapes=[pltpu.VMEM(a.shape, a.dtype) for a in arrays]
        + [pltpu.SemaphoreType.DMA((len(arrays),))],
        name="project",
    )(*arrays)


def widen_kernel(parts, tok_ref, gain_ref, wg, wu, out_ref, mid_ref):
    mid = (tok_ref[...].astype(jnp.float32) + jnp.sum(parts[...].astype(jnp.float32), axis=0)).astype(
        jnp.bfloat16
    )
    mid_ref[...] = mid
    x = mid.astype(jnp.float32).T
    ffn_in = (x * gain_ref[...].astype(jnp.float32)).astype(jnp.bfloat16)
    squares = jnp.sum(x * x, axis=1, keepdims=True)
    n = wg.shape[1]
    m = out_ref.shape[1] // 2
    gate = jnp.dot(ffn_in, wg[...], preferred_element_type=jnp.float32)
    up = jnp.dot(ffn_in, wu[...], preferred_element_type=jnp.float32)
    lane = lax.broadcasted_iota(jnp.int32, (x.shape[0], m - n), 1)
    out_ref[:, :n] = gate.astype(jnp.bfloat16)
    out_ref[:, n:m] = jnp.where(lane == 0, squares, 0.0).astype(jnp.bfloat16)
    out_ref[:, m : m + n] = up.astype(jnp.bfloat16)
    out_ref[:, m + n :] = jnp.zeros((x.shape[0], m - n), jnp.bfloat16)


def widen(parts, tok_t, gain, wg, wu):
    width, rows = tok_t.shape
    return pl.pallas_call(
        widen_kernel,
        out_shape=(
            pltpu.VMEM((rows, 2 * padded(wg.shape[1] + 1)), jnp.bfloat16),
            pltpu.VMEM(tok_t.shape, jnp.bfloat16),
        ),
        in_specs=[pl.BlockSpec(memory_space=pltpu.VMEM)] * 5,
        out_specs=[pl.BlockSpec(memory_space=pltpu.VMEM)] * 2,
        name="widen",
    )(*(in_vmem(a) for a in (parts, tok_t, gain, wg, wu)))


def exchanged(blocks, axis):
    return lax.all_to_all(blocks, axis, 0, 0, tiled=True)


def summed(blocks):
    return jnp.sum(blocks.astype(jnp.float32), axis=0)


def to_all(x, axis):
    return exchanged(jnp.broadcast_to(x[None], (lax.axis_size(axis), *x.shape)), axis)


def local(
    tokens,
    mix_gain,
    ffn_gain,
    w_query,
    w_key,
    w_value,
    w_gate,
    w_decay,
    decay_bias,
    head_gain,
    w_output,
    w_ffgate,
    w_ffup,
    w_down,
    state,
):
    own_rows, heads, key_dim, val_dim = state.shape
    kv = lax.axis_size("kv")
    model_width = tokens.shape[1] * kv
    tok_t = tokens.T
    made = project(tok_t, mix_gain[None, :], (w_query, w_key, w_value, w_gate, w_decay))
    arrived, head_gain = lax.optimization_barrier(
        (exchanged(made.reshape(kv, own_rows, -1), "kv"), head_gain)
    )
    sums = summed(arrived)
    kd, vd = heads * key_dim, heads * val_dim
    ends = (kd, 2 * kd, 2 * kd + vd, 2 * kd + 2 * vd, 3 * kd + 2 * vd)
    query_sum, key_sum, value_sum, gate_sum, decay_sum = (
        sums[:, a:b] for a, b in zip((0,) + ends[:-1], ends)
    )
    mix_rms = lax.rsqrt(sums[:, ends[-1] : ends[-1] + 1] / model_width + epsilon)
    queries = (query_sum * mix_rms).reshape(own_rows, heads, key_dim) * key_dim ** (-0.5)
    key_rows = (key_sum * mix_rms).reshape(own_rows, heads, key_dim)
    value_rows = (value_sum * mix_rms).reshape(own_rows, heads, val_dim)
    gate_rows = (gate_sum * mix_rms).reshape(own_rows, heads, val_dim)
    decay_rows = (decay_sum * mix_rms + decay_bias).reshape(own_rows, heads, key_dim)
    log_decay = jax.nn.log_sigmoid(decay_rows) / 16.0
    new_state = (
        jnp.exp(log_decay)[..., None] * state + key_rows[..., :, None] * value_rows[..., None, :]
    )
    attended = jnp.einsum("bhk,bhkv->bhv", queries, new_state, precision=lax.Precision.HIGHEST)
    attended = attended * lax.rsqrt(
        jnp.sum(attended * attended, axis=2, keepdims=True) / val_dim + epsilon
    )
    head_out = (
        (attended * head_gain.astype(jnp.float32) * jax.nn.silu(gate_rows))
        .reshape(own_rows, vd)
        .astype(jnp.bfloat16)
    )
    heads_all = to_all(head_out, "kv").reshape(-1, vd)
    attn_part = lax.dot_general(
        w_output, heads_all, (((0,), (1,)), ((), ())), preferred_element_type=jnp.float32
    ).astype(jnp.bfloat16)
    attn_parts = to_all(attn_part, "tp")
    wide, mid_t = widen(attn_parts, tok_t, ffn_gain[None, :], w_ffgate, w_ffup)
    sums = summed(exchanged(wide.reshape(kv, own_rows, -1), "kv"))
    units = w_ffgate.shape[1]
    half = wide.shape[1] // 2
    ffn_rms = lax.rsqrt(sums[:, units : units + 1] / model_width + epsilon)
    hidden = (
        jax.nn.silu(sums[:, :units] * ffn_rms) * (sums[:, half : half + units] * ffn_rms)
    ).astype(jnp.bfloat16)
    hidden_all = to_all(hidden, "kv").reshape(-1, units)
    down_part = lax.dot_general(
        w_down, hidden_all, (((0,), (1,)), ((), ())), preferred_element_type=jnp.float32
    ).astype(jnp.bfloat16)
    mixed = (mid_t.astype(jnp.float32) + summed(to_all(down_part, "tp"))).astype(jnp.bfloat16)
    return (mixed.T, new_state)


def solution(mesh):
    in_specs = (
        P(None, "kv"),
        P("kv"),
        P("kv"),
        P("kv", "tp"),
        P("kv", "tp"),
        P("kv", "tp"),
        P("kv", "tp"),
        P("kv", "tp"),
        P("tp"),
        P(),
        P("tp", "kv"),
        P("kv", "tp"),
        P("kv", "tp"),
        P("tp", "kv"),
        P("kv", "tp", None, None),
    )
    out_specs = (P(None, "kv"), P("kv", "tp", None, None))
    return jax.shard_map(local, mesh=mesh, in_specs=in_specs, out_specs=out_specs, check_vma=False)
```

```python
import functools

import jax
import jax.numpy as jnp
from jax import lax
from jax.experimental import pallas as pl
from jax.experimental.pallas import tpu as pltpu
from jax.sharding import Mesh
from jax.sharding import PartitionSpec as P

epsilon = 1e-06
KV = ("z", "h", "r")
LINE = ("z", "h")


def padded(n):
    return -(-n // 128) * 128


def in_vmem(x):
    return pltpu.with_memory_space_constraint(x, pltpu.VMEM)


def whole(count):
    return [pl.BlockSpec(memory_space=pltpu.VMEM)] * count


def cut_of(units):
    return units // 256 * 128


def half_of(units):
    return padded(units - cut_of(units) + 1)


def project_kernel(*refs, count):
    sources, outs = (refs[:count], refs[count : count + 3])
    held, sems = (refs[count + 3 : -1], refs[-1])
    copies = [pltpu.make_async_copy(a, b, sems.at[i]) for i, (a, b) in enumerate(zip(sources, held))]
    for c in copies:
        c.start()
    out_ref, mine_ref, sent_ref = outs
    tok, gain, ffn_gain = held[:3]
    weights, splits = (held[3:-3], held[-3:])
    copies[0].wait()
    copies[1].wait()
    x = tok[...].astype(jnp.float32).T
    mix_in = (x * gain[...].astype(jnp.float32)).astype(jnp.bfloat16)
    squares = jnp.sum(x * x, axis=1, keepdims=True)
    at = 0
    for i, w in enumerate(weights):
        copies[3 + i].wait()
        n = w.shape[1]
        part = jnp.dot(mix_in, w[...], preferred_element_type=jnp.float32)
        out_ref[:, at : at + n] = part.astype(jnp.bfloat16)
        at += n
    rest = out_ref.shape[1] - at
    lane = lax.broadcasted_iota(jnp.int32, (x.shape[0], rest), 1)
    out_ref[:, at:] = jnp.where(lane == 0, squares, 0.0).astype(jnp.bfloat16)
    copies[2].wait()
    for c in copies[3 + len(weights) :]:
        c.wait()
    rows, units = splits[0].shape
    cut, half = (cut_of(units), half_of(units))

    def fill(ref, member, first):
        a, b = ((0, cut), (cut, units))[member]
        for i, w in enumerate(splits):
            ref[:, i * half : i * half + b - a] = w[:, a:b]
            ref[:, i * half + b - a : (i + 1) * half] = jnp.zeros((rows, half - (b - a)), w.dtype)
        seqs = tok.shape[1]
        end = len(splits) * half
        ref[:, end : end + seqs] = tok[...]
        ref[:, end + seqs :] = jnp.zeros((rows, 2 * rows), ref.dtype)
        side = 0 if first else rows
        ref[0:1, end + seqs + side : end + seqs + side + rows] = ffn_gain[...]

    for member in range(2):

        @pl.when(lax.axis_index("r") == member)
        def _():
            fill(mine_ref, member, True)
            fill(sent_ref, 1 - member, False)


def project(tok_t, gain, ffn_gain, weights, splits):
    width, rows = tok_t.shape
    total = sum(w.shape[1] for w in weights)
    pack = len(splits) * half_of(splits[0].shape[1]) + rows + 2 * width
    arrays = (tok_t, gain, ffn_gain, *weights, *splits)
    return pl.pallas_call(
        functools.partial(project_kernel, count=len(arrays)),
        out_shape=(
            pltpu.VMEM((rows, total + 128), jnp.bfloat16),
            pltpu.VMEM((width, pack), jnp.bfloat16),
            pltpu.VMEM((width, pack), jnp.bfloat16),
        ),
        in_specs=[pl.BlockSpec(memory_space=pl.ANY)] * len(arrays),
        out_specs=whole(3),
        scratch_shapes=[pltpu.VMEM(a.shape, a.dtype) for a in arrays]
        + [pltpu.SemaphoreType.DMA((len(arrays),))],
        name="project",
    )(*arrays)


def widen_kernel(parts, mine, got, out_ref, mid_ref):
    r = lax.axis_index("r")
    _, seqs = mid_ref.shape
    half = out_ref.shape[1] // 2
    end = 3 * half

    def mid_of(ref, at):
        total = jnp.sum(parts[at].astype(jnp.float32), axis=0)
        return (ref[:, end : end + seqs].astype(jnp.float32) + total).astype(jnp.bfloat16)

    own = mid_of(mine, r)
    mid_ref[...] = own
    x = jnp.concatenate([own, mid_of(got, 1 - r)], axis=0).astype(jnp.float32).T
    gains = mine[0:1, end + seqs :].astype(jnp.float32) + got[0:1, end + seqs :].astype(jnp.float32)
    ffn_in = (x * gains).astype(jnp.bfloat16)
    squares = jnp.sum(x * x, axis=1, keepdims=True)
    weights = jnp.concatenate([mine[:, : 2 * half], got[:, : 2 * half]], axis=0)
    made = jnp.dot(ffn_in, weights, preferred_element_type=jnp.float32)
    lane = lax.broadcasted_iota(jnp.int32, (seqs, 128), 1)
    out_ref[...] = made.astype(jnp.bfloat16)
    out_ref[:, half - 128 : half] = jnp.where(lane == 127, squares, made[:, half - 128 : half]).astype(
        jnp.bfloat16
    )


def widen(parts, mine, got, half):
    width, seqs = parts.shape[2:]
    return pl.pallas_call(
        widen_kernel,
        out_shape=(
            pltpu.VMEM((seqs, 2 * half), jnp.bfloat16),
            pltpu.VMEM((width, seqs), jnp.bfloat16),
        ),
        in_specs=whole(3),
        out_specs=whole(2),
        name="widen",
    )(*(in_vmem(a) for a in (parts, mine, got)))


def narrow_kernel(hidden, mine, got, out_ref):
    r = lax.axis_index("r")
    half = hidden.shape[1]
    copies, _ = out_ref.shape[1:3]
    for ref, at in ((mine, r), (got, 1 - r)):
        made = lax.dot_general(
            ref[:, 2 * half : 3 * half],
            hidden[...],
            (((1,), (1,)), ((), ())),
            preferred_element_type=jnp.float32,
        ).astype(jnp.bfloat16)
        for j in range(copies):
            out_ref[at, j] = made


def narrow(hidden, mine, got, tp):
    width, seqs = (mine.shape[0], hidden.shape[0])
    return pl.pallas_call(
        narrow_kernel,
        out_shape=pltpu.VMEM((2, tp, width, seqs), jnp.bfloat16),
        in_specs=whole(3),
        out_specs=pl.BlockSpec(memory_space=pltpu.VMEM),
        name="narrow",
    )(*(in_vmem(a) for a in (hidden, mine, got)))


def exchanged(blocks, axis):
    return lax.all_to_all(blocks, axis, 0, 0, tiled=True)


def summed(blocks):
    return jnp.sum(blocks.astype(jnp.float32), axis=0)


def to_all(x, axis):
    return exchanged(jnp.broadcast_to(x[None], (lax.axis_size(axis), *x.shape)), axis)


def local(
    tokens,
    mix_gain,
    ffn_gain,
    w_query,
    w_key,
    w_value,
    w_gate,
    w_decay,
    decay_bias,
    head_gain,
    w_output,
    w_ffgate,
    w_ffup,
    w_down,
    state,
):
    own_rows, heads, key_dim, val_dim = state.shape
    kv, tp, line = (lax.axis_size(a) for a in (KV, "tp", LINE))
    model_width = tokens.shape[1] * kv
    made, mine, sent = project(
        tokens.T,
        mix_gain[None, :],
        ffn_gain[None, :],
        (w_query, w_key, w_value, w_gate, w_decay),
        (w_ffgate, w_ffup, w_down.T),
    )
    got = lax.ppermute(sent, "r", ((0, 1), (1, 0)))
    arrived = exchanged(made.reshape(kv, own_rows, -1), KV)
    arrived, head_gain = lax.optimization_barrier((arrived, head_gain))
    sums = summed(arrived)
    kd, vd = heads * key_dim, heads * val_dim
    ends = (kd, 2 * kd, 2 * kd + vd, 2 * kd + 2 * vd, 3 * kd + 2 * vd)
    query_sum, key_sum, value_sum, gate_sum, decay_sum = (
        sums[:, a:b] for a, b in zip((0,) + ends[:-1], ends)
    )
    mix_rms = lax.rsqrt(sums[:, ends[-1] : ends[-1] + 1] / model_width + epsilon)
    queries = (query_sum * mix_rms).reshape(own_rows, heads, key_dim) * key_dim ** (-0.5)
    key_rows = (key_sum * mix_rms).reshape(own_rows, heads, key_dim)
    value_rows = (value_sum * mix_rms).reshape(own_rows, heads, val_dim)
    gate_rows = (gate_sum * mix_rms).reshape(own_rows, heads, val_dim)
    decay_rows = (decay_sum * mix_rms + decay_bias).reshape(own_rows, heads, key_dim)
    log_decay = jax.nn.log_sigmoid(decay_rows) / 16.0
    new_state = (
        jnp.exp(log_decay)[..., None] * state + key_rows[..., :, None] * value_rows[..., None, :]
    )
    attended = jnp.einsum("bhk,bhkv->bhv", queries, new_state, precision=lax.Precision.HIGHEST)
    attended = attended * lax.rsqrt(
        jnp.sum(attended * attended, axis=2, keepdims=True) / val_dim + epsilon
    )
    head_out = (
        (attended * head_gain.astype(jnp.float32) * jax.nn.silu(gate_rows))
        .reshape(own_rows, vd)
        .astype(jnp.bfloat16)
    )
    heads_all = to_all(head_out, KV).reshape(-1, vd)
    attn_part = lax.dot_general(
        w_output, heads_all, (((0,), (1,)), ((), ())), preferred_element_type=jnp.float32
    ).astype(jnp.bfloat16)
    attn_part, got = lax.optimization_barrier((attn_part, got))
    width, seqs = attn_part.shape
    attn_parts = to_all(attn_part, ("r", "tp")).reshape(2, tp, width, seqs)
    half = half_of(w_ffgate.shape[1])
    wide, mid_t = widen(attn_parts, mine, got, half)
    sums = summed(exchanged(wide.reshape(line, seqs // line, -1), LINE))
    ffn_rms = lax.rsqrt(sums[:, half - 1 : half] / model_width + epsilon)
    gated = jax.nn.silu(sums[:, :half] * ffn_rms) * (sums[:, half:] * ffn_rms)
    hidden = gated.astype(jnp.bfloat16)
    hidden_all = to_all(hidden, LINE).reshape(seqs, half)
    down_parts = narrow(hidden_all, mine, got, tp).reshape(2 * tp, width, seqs)
    mixed = (mid_t.astype(jnp.float32) + summed(exchanged(down_parts, ("r", "tp")))).astype(
        jnp.bfloat16
    )
    return (mixed.T, new_state)


def solution(mesh):
    in_specs = (
        P(None, KV),
        P(KV),
        P(KV),
        P(KV, "tp"),
        P(KV, "tp"),
        P(KV, "tp"),
        P(KV, "tp"),
        P(KV, "tp"),
        P("tp"),
        P(),
        P("tp", KV),
        P(KV, "tp"),
        P(KV, "tp"),
        P("tp", KV),
        P(KV, "tp", None, None),
    )
    out_specs = (P(None, KV), P(KV, "tp", None, None))
    kv, tp = mesh.devices.shape
    lines = Mesh(mesh.devices.reshape(8, kv // 16, 2, tp), (*KV, "tp"))
    return jax.shard_map(local, mesh=lines, in_specs=in_specs, out_specs=out_specs, check_vma=False)
```

```python
import functools

import jax
import jax.numpy as jnp
from jax import lax
from jax.experimental import pallas as pl
from jax.experimental.pallas import tpu as pltpu
from jax.sharding import PartitionSpec as P

epsilon = 1e-06


def member(kv):
    return (kv ^ (kv >> 2)) & 1


def lines(kv):
    return [[i for i in range(kv) if member(i) == m] for m in range(2)]


def pairs(kv, tp):
    return [
        [i * tp + t for i in sorted((j, j + 1), key=member) for t in range(tp)]
        for j in range(0, kv, 2)
    ]


def padded(n):
    return -(-n // 128) * 128


def in_vmem(x):
    return pltpu.with_memory_space_constraint(x, pltpu.VMEM)


def whole(count):
    return [pl.BlockSpec(memory_space=pltpu.VMEM)] * count


def cut_of(units):
    return units // 256 * 128


def half_of(units):
    return padded(units - cut_of(units) + 1)


def project_kernel(*refs, count):
    sources, outs = (refs[:count], refs[count : count + 5])
    held, sems = (refs[count + 5 : -1] + outs[3:], refs[-1])
    copies = [pltpu.make_async_copy(a, b, sems.at[i]) for i, (a, b) in enumerate(zip(sources, held))]
    for c in copies:
        c.start()
    out_ref, mine_ref, sent_ref = outs[:3]
    tok, gain, ffn_gain = held[:3]
    weights, splits = (held[3:-5], held[-5:-2])
    copies[0].wait()
    copies[1].wait()
    x = tok[...].astype(jnp.float32).T
    mix_in = (x * gain[...].astype(jnp.float32)).astype(jnp.bfloat16)
    squares = jnp.sum(x * x, axis=1, keepdims=True)
    at = 0
    for i, w in enumerate(weights):
        copies[3 + i].wait()
        n = w.shape[1]
        part = jnp.dot(mix_in, w[...], preferred_element_type=jnp.float32)
        out_ref[:, at : at + n] = part.astype(jnp.bfloat16)
        at += n
    rest = out_ref.shape[1] - at
    lane = lax.broadcasted_iota(jnp.int32, (x.shape[0], rest), 1)
    out_ref[:, at:] = jnp.where(lane == 0, squares, 0.0).astype(jnp.bfloat16)
    copies[2].wait()
    for c in copies[3 + len(weights) :]:
        c.wait()
    rows, units = splits[0].shape
    cut, half = (cut_of(units), half_of(units))

    def fill(ref, m, first):
        a, b = ((0, cut), (cut, units))[m]
        for i, w in enumerate(splits):
            ref[:, i * half : i * half + b - a] = w[:, a:b]
            ref[:, i * half + b - a : (i + 1) * half] = jnp.zeros((rows, half - (b - a)), w.dtype)
        seqs = tok.shape[1]
        end = len(splits) * half
        ref[:, end : end + seqs] = tok[...]
        ref[:, end + seqs :] = jnp.zeros((rows, 2 * rows), ref.dtype)
        side = 0 if first else rows
        ref[0:1, end + seqs + side : end + seqs + side + rows] = ffn_gain[...]

    for m in range(2):

        @pl.when(member(lax.axis_index("kv")) == m)
        def _():
            fill(mine_ref, m, True)
            fill(sent_ref, 1 - m, False)


def project(tok_t, gain, ffn_gain, weights, splits, kept):
    width, rows = tok_t.shape
    total = sum(w.shape[1] for w in weights)
    pack = len(splits) * half_of(splits[0].shape[1]) + rows + 2 * width
    arrays = (tok_t, gain, ffn_gain, *weights, *splits, *kept)
    return pl.pallas_call(
        functools.partial(project_kernel, count=len(arrays)),
        out_shape=(
            pltpu.VMEM((rows, total + 128), jnp.bfloat16),
            pltpu.VMEM((width, pack), jnp.bfloat16),
            pltpu.VMEM((width, pack), jnp.bfloat16),
            *(pltpu.VMEM(a.shape, a.dtype) for a in kept),
        ),
        in_specs=[pl.BlockSpec(memory_space=pl.ANY)] * len(arrays),
        out_specs=whole(5),
        scratch_shapes=[pltpu.VMEM(a.shape, a.dtype) for a in arrays[:-2]]
        + [pltpu.SemaphoreType.DMA((len(arrays),))],
        name="project",
    )(*arrays)


def attend_kernel(sums, bias, gain, state, key_ref, value_ref, decay_ref, out_ref, *, model_width):
    rows, _, kd, vd = state.shape
    base = sums[...]
    rms = lax.rsqrt(base[:, 3 * kd + 2 * vd : 3 * kd + 2 * vd + 1] / model_width + epsilon)
    q = base[:, :kd] * rms * kd**-0.5
    k = base[:, kd : 2 * kd] * rms
    v = base[:, 2 * kd : 2 * kd + vd] * rms
    g = base[:, 2 * kd + vd : 2 * kd + 2 * vd] * rms
    x = base[:, 2 * kd + 2 * vd : 3 * kd + 2 * vd] * rms + bias[...]
    log_sigmoid = jnp.minimum(x, 0.0) - jnp.log1p(jnp.exp(-jnp.abs(x)))
    decay = jnp.exp(log_sigmoid / 16.0)
    key_ref[...] = k
    value_ref[...] = v
    decay_ref[...] = decay
    fresh = jnp.sum(q * k, axis=1, keepdims=True) * v
    columns = jnp.concatenate([q * decay, jnp.zeros((8 - rows, kd), jnp.float32)], axis=0).T
    step = 32
    found = []
    for s in range(rows):
        total = jnp.zeros((8, vd), jnp.float32)
        for at in range(0, kd, step):
            read = columns[at : at + step, s : s + 1] * state[s, 0, at : at + step]
            total = total + jnp.sum(read.reshape(step // 8, 8, vd), axis=0)
        found.append(jnp.sum(total, axis=0, keepdims=True))
    attended = jnp.concatenate(found, axis=0) + fresh
    scale = lax.rsqrt(jnp.sum(attended * attended, axis=1, keepdims=True) / vd + epsilon)
    gains = jnp.concatenate([gain[i : i + 1] for i in range(gain.shape[0])], axis=1)
    gated = attended * scale * gains.astype(jnp.float32) * (g / (1.0 + jnp.exp(-g)))
    out_ref[...] = gated.astype(jnp.bfloat16)


def attend(sums, bias, gain, state, model_width):
    rows, _, kd, vd = state.shape
    return pl.pallas_call(
        functools.partial(attend_kernel, model_width=model_width),
        out_shape=(
            pltpu.VMEM((rows, kd), jnp.float32),
            pltpu.VMEM((rows, vd), jnp.float32),
            pltpu.VMEM((rows, kd), jnp.float32),
            pltpu.VMEM((rows, vd), jnp.bfloat16),
        ),
        in_specs=whole(4),
        out_specs=whole(4),
        name="attend",
    )(*(in_vmem(a) for a in (sums, bias, gain, state)))


def widen_kernel(parts, mine, got, _, out_ref, mid_ref):
    r = member(lax.axis_index("kv"))
    _, seqs = mid_ref.shape
    half = out_ref.shape[1] // 2
    end = 3 * half

    def mid_of(ref, at):
        total = jnp.sum(parts[at].astype(jnp.float32), axis=0)
        return (ref[:, end : end + seqs].astype(jnp.float32) + total).astype(jnp.bfloat16)

    own = mid_of(mine, r)
    mid_ref[...] = own
    x = jnp.concatenate([own, mid_of(got, 1 - r)], axis=0).astype(jnp.float32).T
    gains = mine[0:1, end + seqs :].astype(jnp.float32) + got[0:1, end + seqs :].astype(jnp.float32)
    ffn_in = (x * gains).astype(jnp.bfloat16)
    squares = jnp.sum(x * x, axis=1, keepdims=True)
    weights = jnp.concatenate([mine[:, : 2 * half], got[:, : 2 * half]], axis=0)
    made = jnp.dot(ffn_in, weights, preferred_element_type=jnp.float32)
    lane = lax.broadcasted_iota(jnp.int32, (seqs, 128), 1)
    out_ref[...] = made.astype(jnp.bfloat16)
    out_ref[:, half - 128 : half] = jnp.where(lane == 127, squares, made[:, half - 128 : half]).astype(
        jnp.bfloat16
    )


def widen(parts, mine, got, new_state, half):
    width, seqs = parts.shape[2:]
    return pl.pallas_call(
        widen_kernel,
        out_shape=(
            pltpu.VMEM((seqs, 2 * half), jnp.bfloat16),
            pltpu.VMEM((width, seqs), jnp.bfloat16),
        ),
        in_specs=whole(4),
        out_specs=whole(2),
        name="widen",
    )(*(in_vmem(a) for a in (parts, mine, got, new_state)))


def narrow_kernel(hidden, mine, got, out_ref):
    r = member(lax.axis_index("kv"))
    half = hidden.shape[1]
    copies, _ = out_ref.shape[1:3]
    for ref, at in ((mine, r), (got, 1 - r)):
        made = lax.dot_general(
            ref[:, 2 * half : 3 * half],
            hidden[...],
            (((1,), (1,)), ((), ())),
            preferred_element_type=jnp.float32,
        ).astype(jnp.bfloat16)
        for j in range(copies):
            out_ref[at, j] = made


def narrow(hidden, mine, got, tp):
    width, seqs = (mine.shape[0], hidden.shape[0])
    return pl.pallas_call(
        narrow_kernel,
        out_shape=pltpu.VMEM((2, tp, width, seqs), jnp.bfloat16),
        in_specs=whole(3),
        out_specs=pl.BlockSpec(memory_space=pltpu.VMEM),
        name="narrow",
    )(*(in_vmem(a) for a in (hidden, mine, got)))


def exchanged(blocks, axis, groups=None):
    return lax.all_to_all(blocks, axis, 0, 0, axis_index_groups=groups, tiled=True)


def summed(blocks):
    return jnp.sum(blocks.astype(jnp.float32), axis=0)


def copies_of(x, count):
    return jnp.broadcast_to(x[None], (count, *x.shape))


def local(
    tokens,
    mix_gain,
    ffn_gain,
    w_query,
    w_key,
    w_value,
    w_gate,
    w_decay,
    decay_bias,
    head_gain,
    w_output,
    w_ffgate,
    w_ffup,
    w_down,
    state,
):
    own_rows, heads, _, val_dim = state.shape
    kv, tp = (lax.axis_size(a) for a in ("kv", "tp"))
    model_width = tokens.shape[1] * kv
    made, mine, sent, bias, head_scale = project(
        tokens.T,
        mix_gain[None, :],
        ffn_gain[None, :],
        (w_query, w_key, w_value, w_gate, w_decay),
        (w_ffgate, w_ffup, w_down.T),
        (decay_bias[None, :], head_gain.reshape(-1, 128)),
    )
    got = lax.ppermute(sent, "kv", [(i, i ^ 1) for i in range(kv)])
    arrived = exchanged(made.reshape(kv, own_rows, -1), "kv")
    keys, values, decay, head_out = attend(summed(arrived), bias, head_scale, state, model_width)
    new_state = (
        decay[:, None, :, None] * state + keys[:, None, :, None] * values[:, None, None, :]
    )
    head_out, new_state = lax.optimization_barrier((head_out, new_state))
    heads_all = exchanged(copies_of(head_out, kv), "kv").reshape(-1, heads * val_dim)
    attn_part = lax.dot_general(
        w_output, heads_all, (((0,), (1,)), ((), ())), preferred_element_type=jnp.float32
    ).astype(jnp.bfloat16)
    attn_part, got = lax.optimization_barrier((attn_part, got))
    width, seqs = attn_part.shape
    pair, line = (pairs(kv, tp), lines(kv))
    attn_parts = exchanged(copies_of(attn_part, 2 * tp), ("kv", "tp"), pair)
    half = half_of(w_ffgate.shape[1])
    wide, mid_t = widen(attn_parts.reshape(2, tp, width, seqs), mine, got, new_state, half)
    count = len(line[0])
    sums = summed(exchanged(wide.reshape(count, seqs // count, -1), "kv", line))
    ffn_rms = lax.rsqrt(sums[:, half - 1 : half] / model_width + epsilon)
    gated = jax.nn.silu(sums[:, :half] * ffn_rms) * (sums[:, half:] * ffn_rms)
    hidden = gated.astype(jnp.bfloat16)
    hidden_all = exchanged(copies_of(hidden, count), "kv", line).reshape(seqs, half)
    down_parts = narrow(hidden_all, mine, got, tp).reshape(2 * tp, width, seqs)
    mixed = (
        mid_t.astype(jnp.float32) + summed(exchanged(down_parts, ("kv", "tp"), pair))
    ).astype(jnp.bfloat16)
    return (mixed.T, new_state)


def solution(mesh):
    in_specs = (
        P(None, "kv"),
        P("kv"),
        P("kv"),
        P("kv", "tp"),
        P("kv", "tp"),
        P("kv", "tp"),
        P("kv", "tp"),
        P("kv", "tp"),
        P("tp"),
        P(),
        P("tp", "kv"),
        P("kv", "tp"),
        P("kv", "tp"),
        P("tp", "kv"),
        P("kv", "tp", None, None),
    )
    out_specs = (P(None, "kv"), P("kv", "tp", None, None))
    return jax.shard_map(local, mesh=mesh, in_specs=in_specs, out_specs=out_specs, check_vma=False)
```

```python
import functools

import jax
import jax.numpy as jnp
from jax import lax
from jax.experimental import pallas as pl
from jax.experimental.pallas import tpu as pltpu
from jax.sharding import PartitionSpec as P

epsilon = 1e-06


def member(kv):
    return (kv ^ (kv >> 2)) & 1


def lines(kv):
    return [[i for i in range(kv) if member(i) == m] for m in range(2)]


def pairs(kv, tp):
    return [
        [i * tp + t for i in sorted((j, j + 1), key=member) for t in range(tp)]
        for j in range(0, kv, 2)
    ]


def padded(n):
    return -(-n // 128) * 128


def in_vmem(x):
    return pltpu.with_memory_space_constraint(x, pltpu.VMEM)


def whole(count):
    return [pl.BlockSpec(memory_space=pltpu.VMEM)] * count


def cut_of(units):
    return units // 256 * 128


def half_of(units):
    return padded(units - cut_of(units) + 1)


def fetch(sources, held, sems):
    copies = [pltpu.make_async_copy(a, b, sems.at[i]) for i, (a, b) in enumerate(zip(sources, held))]
    for c in copies:
        c.start()
    return copies


def project_kernel(*refs, count, kept):
    sources, out_ref = (refs[:count], refs[count])
    held = refs[count + 1 + kept : -1] + refs[count + 1 : count + 1 + kept]
    copies = fetch(sources, held, refs[-1])
    tok, gain = held[:2]
    copies[0].wait()
    copies[1].wait()
    x = tok[...].astype(jnp.float32).T
    mix_in = (x * gain[...].astype(jnp.float32)).astype(jnp.bfloat16)
    squares = jnp.sum(x * x, axis=1, keepdims=True)
    at = 0
    for copy, w in zip(copies[2 : count - kept], held[2 : count - kept]):
        copy.wait()
        n = w.shape[1]
        part = jnp.dot(mix_in, w[...], preferred_element_type=jnp.float32)
        out_ref[:, at : at + n] = part.astype(jnp.bfloat16)
        at += n
    rest = out_ref.shape[1] - at
    lane = lax.broadcasted_iota(jnp.int32, (x.shape[0], rest), 1)
    out_ref[:, at:] = jnp.where(lane == 0, squares, 0.0).astype(jnp.bfloat16)
    for copy in copies[count - kept :]:
        copy.wait()


def project(tok_t, gain, weights, kept):
    total = sum(w.shape[1] for w in weights)
    arrays = (tok_t, gain, *weights, *kept)
    return pl.pallas_call(
        functools.partial(project_kernel, count=len(arrays), kept=len(kept)),
        out_shape=(
            pltpu.VMEM((tok_t.shape[1], total + 128), jnp.bfloat16),
            *(pltpu.VMEM(a.shape, a.dtype) for a in kept),
        ),
        in_specs=[pl.BlockSpec(memory_space=pl.ANY)] * len(arrays),
        out_specs=whole(1 + len(kept)),
        scratch_shapes=[pltpu.VMEM(a.shape, a.dtype) for a in arrays[: len(arrays) - len(kept)]]
        + [pltpu.SemaphoreType.DMA((len(arrays),))],
        name="project",
    )(*arrays)


def pack_kernel(_, *refs, count):
    sources, outs = (refs[:count], refs[count : count + 2])
    held, sems = (refs[count + 2 : -1], refs[-1])
    for c in fetch(sources, held, sems):
        c.wait()
    tok, ffn_gain, splits = (held[0], held[1], held[2:])
    mine_ref, sent_ref = outs
    rows, units = splits[0].shape
    cut, half = (cut_of(units), half_of(units))

    def fill(ref, m, first):
        a, b = ((0, cut), (cut, units))[m]
        for i, w in enumerate(splits):
            ref[:, i * half : i * half + b - a] = w[:, a:b]
            ref[:, i * half + b - a : (i + 1) * half] = jnp.zeros((rows, half - (b - a)), w.dtype)
        seqs = tok.shape[1]
        end = len(splits) * half
        ref[:, end : end + seqs] = tok[...]
        ref[:, end + seqs :] = jnp.zeros((rows, 2 * rows), ref.dtype)
        side = 0 if first else rows
        ref[0:1, end + seqs + side : end + seqs + side + rows] = ffn_gain[...]

    for m in range(2):

        @pl.when(member(lax.axis_index("kv")) == m)
        def _():
            fill(mine_ref, m, True)
            fill(sent_ref, 1 - m, False)


def pack(after, tok_t, ffn_gain, splits):
    width, rows = tok_t.shape
    lanes = len(splits) * half_of(splits[0].shape[1]) + rows + 2 * width
    arrays = (tok_t, ffn_gain, *splits)
    return pl.pallas_call(
        functools.partial(pack_kernel, count=len(arrays)),
        out_shape=(pltpu.VMEM((width, lanes), jnp.bfloat16),) * 2,
        in_specs=whole(1) + [pl.BlockSpec(memory_space=pl.ANY)] * len(arrays),
        out_specs=whole(2),
        scratch_shapes=[pltpu.VMEM(a.shape, a.dtype) for a in arrays]
        + [pltpu.SemaphoreType.DMA((len(arrays),))],
        compiler_params=pltpu.CompilerParams(vmem_limit_bytes=8 << 20),
        name="pack",
    )(in_vmem(after), *arrays)


def attend_kernel(sums, bias, gain, state, key_ref, value_ref, decay_ref, out_ref, *, model_width):
    rows, _, kd, vd = state.shape
    base = sums[...]
    rms = lax.rsqrt(base[:, 3 * kd + 2 * vd : 3 * kd + 2 * vd + 1] / model_width + epsilon)
    q = base[:, :kd] * rms * kd**-0.5
    k = base[:, kd : 2 * kd] * rms
    v = base[:, 2 * kd : 2 * kd + vd] * rms
    g = base[:, 2 * kd + vd : 2 * kd + 2 * vd] * rms
    x = base[:, 2 * kd + 2 * vd : 3 * kd + 2 * vd] * rms + bias[...]
    log_sigmoid = jnp.minimum(x, 0.0) - jnp.log1p(jnp.exp(-jnp.abs(x)))
    decay = jnp.exp(log_sigmoid / 16.0)
    key_ref[...] = k
    value_ref[...] = v
    decay_ref[...] = decay
    fresh = jnp.sum(q * k, axis=1, keepdims=True) * v
    columns = jnp.concatenate([q * decay, jnp.zeros((8 - rows, kd), jnp.float32)], axis=0).T
    step = 32
    found = []
    for s in range(rows):
        total = jnp.zeros((8, vd), jnp.float32)
        for at in range(0, kd, step):
            read = columns[at : at + step, s : s + 1] * state[s, 0, at : at + step]
            total = total + jnp.sum(read.reshape(step // 8, 8, vd), axis=0)
        found.append(jnp.sum(total, axis=0, keepdims=True))
    attended = jnp.concatenate(found, axis=0) + fresh
    scale = lax.rsqrt(jnp.sum(attended * attended, axis=1, keepdims=True) / vd + epsilon)
    gains = jnp.concatenate([gain[i : i + 1] for i in range(gain.shape[0])], axis=1)
    gated = attended * scale * gains.astype(jnp.float32) * (g / (1.0 + jnp.exp(-g)))
    out_ref[...] = gated.astype(jnp.bfloat16)


def attend(sums, bias, gain, state, model_width):
    rows, _, kd, vd = state.shape
    return pl.pallas_call(
        functools.partial(attend_kernel, model_width=model_width),
        out_shape=(
            pltpu.VMEM((rows, kd), jnp.float32),
            pltpu.VMEM((rows, vd), jnp.float32),
            pltpu.VMEM((rows, kd), jnp.float32),
            pltpu.VMEM((rows, vd), jnp.bfloat16),
        ),
        in_specs=whole(4),
        out_specs=whole(4),
        compiler_params=pltpu.CompilerParams(vmem_limit_bytes=8 << 20),
        name="attend",
    )(*(in_vmem(a) for a in (sums, bias, gain, state)))


def widen_kernel(parts, mine, got, _, out_ref, mid_ref):
    r = member(lax.axis_index("kv"))
    _, seqs = mid_ref.shape
    half = out_ref.shape[1] // 2
    end = 3 * half

    def mid_of(ref, at):
        total = jnp.sum(parts[at].astype(jnp.float32), axis=0)
        return (ref[:, end : end + seqs].astype(jnp.float32) + total).astype(jnp.bfloat16)

    own = mid_of(mine, r)
    mid_ref[...] = own
    x = jnp.concatenate([own, mid_of(got, 1 - r)], axis=0).astype(jnp.float32).T
    gains = mine[0:1, end + seqs :].astype(jnp.float32) + got[0:1, end + seqs :].astype(jnp.float32)
    ffn_in = (x * gains).astype(jnp.bfloat16)
    squares = jnp.sum(x * x, axis=1, keepdims=True)
    weights = jnp.concatenate([mine[:, : 2 * half], got[:, : 2 * half]], axis=0)
    made = jnp.dot(ffn_in, weights, preferred_element_type=jnp.float32)
    lane = lax.broadcasted_iota(jnp.int32, (seqs, 128), 1)
    out_ref[...] = made.astype(jnp.bfloat16)
    out_ref[:, half - 128 : half] = jnp.where(lane == 127, squares, made[:, half - 128 : half]).astype(
        jnp.bfloat16
    )


def widen(parts, mine, got, new_state, half):
    width, seqs = parts.shape[2:]
    return pl.pallas_call(
        widen_kernel,
        out_shape=(
            pltpu.VMEM((seqs, 2 * half), jnp.bfloat16),
            pltpu.VMEM((width, seqs), jnp.bfloat16),
        ),
        in_specs=whole(4),
        out_specs=whole(2),
        compiler_params=pltpu.CompilerParams(vmem_limit_bytes=8 << 20),
        name="widen",
    )(*(in_vmem(a) for a in (parts, mine, got, new_state)))


def narrow_kernel(hidden, mine, got, out_ref):
    r = member(lax.axis_index("kv"))
    half = hidden.shape[1]
    copies, _ = out_ref.shape[1:3]
    for ref, at in ((mine, r), (got, 1 - r)):
        made = lax.dot_general(
            ref[:, 2 * half : 3 * half],
            hidden[...],
            (((1,), (1,)), ((), ())),
            preferred_element_type=jnp.float32,
        ).astype(jnp.bfloat16)
        for j in range(copies):
            out_ref[at, j] = made


def narrow(hidden, mine, got, tp):
    width, seqs = (mine.shape[0], hidden.shape[0])
    return pl.pallas_call(
        narrow_kernel,
        out_shape=pltpu.VMEM((2, tp, width, seqs), jnp.bfloat16),
        in_specs=whole(3),
        out_specs=pl.BlockSpec(memory_space=pltpu.VMEM),
        compiler_params=pltpu.CompilerParams(vmem_limit_bytes=8 << 20),
        name="narrow",
    )(*(in_vmem(a) for a in (hidden, mine, got)))


def exchanged(blocks, axis, groups=None):
    return lax.all_to_all(blocks, axis, 0, 0, axis_index_groups=groups, tiled=True)


def summed(blocks):
    return jnp.sum(blocks.astype(jnp.float32), axis=0)


def copies_of(x, count):
    return jnp.broadcast_to(x[None], (count, *x.shape))


def local(
    tokens,
    mix_gain,
    ffn_gain,
    w_query,
    w_key,
    w_value,
    w_gate,
    w_decay,
    decay_bias,
    head_gain,
    w_output,
    w_ffgate,
    w_ffup,
    w_down,
    state,
):
    own_rows, heads, _, val_dim = state.shape
    kv, tp = (lax.axis_size(a) for a in ("kv", "tp"))
    model_width = tokens.shape[1] * kv
    made, bias, head_scale = project(
        tokens.T,
        mix_gain[None, :],
        (w_query, w_key, w_value, w_gate, w_decay),
        (decay_bias[None, :], head_gain.reshape(-1, 128)),
    )
    arrived = exchanged(made.reshape(kv, own_rows, -1), "kv")
    keys, values, decay, head_out = attend(summed(arrived), bias, head_scale, state, model_width)
    heads_all = exchanged(copies_of(head_out, kv), "kv")
    mine, sent = pack(head_out, tokens.T, ffn_gain[None, :], (w_ffgate, w_ffup, w_down.T))
    got = lax.ppermute(sent, "kv", [(i, i ^ 1) for i in range(kv)])
    new_state = (
        decay[:, None, :, None] * state + keys[:, None, :, None] * values[:, None, None, :]
    )
    heads_all = heads_all.reshape(-1, heads * val_dim)
    attn_part = lax.dot_general(
        w_output, heads_all, (((0,), (1,)), ((), ())), preferred_element_type=jnp.float32
    ).astype(jnp.bfloat16)
    attn_part, got, new_state = lax.optimization_barrier((attn_part, got, new_state))
    width, seqs = attn_part.shape
    pair, line = (pairs(kv, tp), lines(kv))
    attn_parts = exchanged(copies_of(attn_part, 2 * tp), ("kv", "tp"), pair)
    half = half_of(w_ffgate.shape[1])
    wide, mid_t = widen(attn_parts.reshape(2, tp, width, seqs), mine, got, new_state, half)
    count = len(line[0])
    sums = summed(exchanged(wide.reshape(count, seqs // count, -1), "kv", line))
    ffn_rms = lax.rsqrt(sums[:, half - 1 : half] / model_width + epsilon)
    gated = jax.nn.silu(sums[:, :half] * ffn_rms) * (sums[:, half:] * ffn_rms)
    hidden = gated.astype(jnp.bfloat16)
    hidden_all = exchanged(copies_of(hidden, count), "kv", line).reshape(seqs, half)
    down_parts = narrow(hidden_all, mine, got, tp).reshape(2 * tp, width, seqs)
    mixed = (
        mid_t.astype(jnp.float32) + summed(exchanged(down_parts, ("kv", "tp"), pair))
    ).astype(jnp.bfloat16)
    return (mixed.T, new_state)


def solution(mesh):
    in_specs = (
        P(None, "kv"),
        P("kv"),
        P("kv"),
        P("kv", "tp"),
        P("kv", "tp"),
        P("kv", "tp"),
        P("kv", "tp"),
        P("kv", "tp"),
        P("tp"),
        P(),
        P("tp", "kv"),
        P("kv", "tp"),
        P("kv", "tp"),
        P("tp", "kv"),
        P("kv", "tp", None, None),
    )
    out_specs = (P(None, "kv"), P("kv", "tp", None, None))
    return jax.shard_map(local, mesh=mesh, in_specs=in_specs, out_specs=out_specs, check_vma=False)
```

```python
import functools

import jax
import jax.numpy as jnp
from jax import lax
from jax.experimental import pallas as pl
from jax.experimental.pallas import tpu as pltpu
from jax.sharding import PartitionSpec as P

epsilon = 1e-06


def member(kv):
    return (kv ^ (kv >> 2)) & 1


def lines(kv):
    return [[i for i in range(kv) if member(i) == m] for m in range(2)]


def pairs(kv, tp):
    return [
        [i * tp + t for i in sorted((j, j + 1), key=member) for t in range(tp)]
        for j in range(0, kv, 2)
    ]


def padded(n):
    return -(-n // 128) * 128


def in_vmem(x):
    return pltpu.with_memory_space_constraint(x, pltpu.VMEM)


def whole(count):
    return [pl.BlockSpec(memory_space=pltpu.VMEM)] * count


def cut_of(units):
    return units // 256 * 128


def half_of(units):
    return padded(units - cut_of(units) + 1)


def fetch(sources, held, sems):
    copies = [pltpu.make_async_copy(a, b, sems.at[i]) for i, (a, b) in enumerate(zip(sources, held))]
    for c in copies:
        c.start()
    return copies


def project_kernel(*refs, count, kept):
    sources, out_ref = (refs[:count], refs[count])
    held = refs[count + 1 + kept : -1] + refs[count + 1 : count + 1 + kept]
    copies = fetch(sources, held, refs[-1])
    tok, gain = held[:2]
    copies[0].wait()
    copies[1].wait()
    x = tok[...].astype(jnp.float32).T
    mix_in = (x * gain[...].astype(jnp.float32)).astype(jnp.bfloat16)
    squares = jnp.sum(x * x, axis=1, keepdims=True)
    at = 0
    for copy, w in zip(copies[2 : count - kept], held[2 : count - kept]):
        copy.wait()
        n = w.shape[1]
        part = jnp.dot(mix_in, w[...], preferred_element_type=jnp.float32)
        out_ref[:, at : at + n] = part.astype(jnp.bfloat16)
        at += n
    rest = out_ref.shape[1] - at
    lane = lax.broadcasted_iota(jnp.int32, (x.shape[0], rest), 1)
    out_ref[:, at:] = jnp.where(lane == 0, squares, 0.0).astype(jnp.bfloat16)
    for copy in copies[count - kept :]:
        copy.wait()


def project(tok_t, gain, weights, kept):
    total = sum(w.shape[1] for w in weights)
    arrays = (tok_t, gain, *weights, *kept)
    return pl.pallas_call(
        functools.partial(project_kernel, count=len(arrays), kept=len(kept)),
        out_shape=(
            pltpu.VMEM((tok_t.shape[1], total + 128), jnp.bfloat16),
            *(pltpu.VMEM(a.shape, a.dtype) for a in kept),
        ),
        in_specs=[pl.BlockSpec(memory_space=pl.ANY)] * len(arrays),
        out_specs=whole(1 + len(kept)),
        scratch_shapes=[pltpu.VMEM(a.shape, a.dtype) for a in arrays[: len(arrays) - len(kept)]]
        + [pltpu.SemaphoreType.DMA((len(arrays),))],
        name="project",
    )(*arrays)


def pack_kernel(_, tok, ffn_gain, *refs):
    splits, (mine_ref, sent_ref) = (refs[:-2], refs[-2:])
    rows, units = splits[0].shape
    cut, half = (cut_of(units), half_of(units))

    def fill(ref, m, first):
        a, b = ((0, cut), (cut, units))[m]
        for i, w in enumerate(splits):
            ref[:, i * half : i * half + b - a] = w[:, a:b]
            ref[:, i * half + b - a : (i + 1) * half] = jnp.zeros((rows, half - (b - a)), w.dtype)
        seqs = tok.shape[1]
        end = len(splits) * half
        ref[:, end : end + seqs] = tok[...]
        ref[:, end + seqs :] = jnp.zeros((rows, 2 * rows), ref.dtype)
        side = 0 if first else rows
        ref[0:1, end + seqs + side : end + seqs + side + rows] = ffn_gain[...]

    for m in range(2):

        @pl.when(member(lax.axis_index("kv")) == m)
        def _():
            fill(mine_ref, m, True)
            fill(sent_ref, 1 - m, False)


def pack(after, tok_t, ffn_gain, splits):
    width, rows = tok_t.shape
    lanes = len(splits) * half_of(splits[0].shape[1]) + rows + 2 * width
    arrays = (after, tok_t, ffn_gain, *splits)
    return pl.pallas_call(
        pack_kernel,
        out_shape=(pltpu.VMEM((width, lanes), jnp.bfloat16),) * 2,
        in_specs=whole(len(arrays)),
        out_specs=whole(2),
        compiler_params=pltpu.CompilerParams(vmem_limit_bytes=8 << 20),
        name="pack",
    )(*(in_vmem(a) for a in arrays))


def attend_kernel(sums, bias, gain, state, key_ref, value_ref, decay_ref, out_ref, *, model_width):
    rows, _, kd, vd = state.shape
    base = sums[...]
    rms = lax.rsqrt(base[:, 3 * kd + 2 * vd : 3 * kd + 2 * vd + 1] / model_width + epsilon)
    q = base[:, :kd] * rms * kd**-0.5
    k = base[:, kd : 2 * kd] * rms
    v = base[:, 2 * kd : 2 * kd + vd] * rms
    g = base[:, 2 * kd + vd : 2 * kd + 2 * vd] * rms
    x = base[:, 2 * kd + 2 * vd : 3 * kd + 2 * vd] * rms + bias[...]
    log_sigmoid = jnp.minimum(x, 0.0) - jnp.log1p(jnp.exp(-jnp.abs(x)))
    decay = jnp.exp(log_sigmoid / 16.0)
    key_ref[...] = k
    value_ref[...] = v
    decay_ref[...] = decay
    fresh = jnp.sum(q * k, axis=1, keepdims=True) * v
    columns = jnp.concatenate([q * decay, jnp.zeros((8 - rows, kd), jnp.float32)], axis=0).T
    step = 32
    found = []
    for s in range(rows):
        total = jnp.zeros((8, vd), jnp.float32)
        for at in range(0, kd, step):
            read = columns[at : at + step, s : s + 1] * state[s, 0, at : at + step]
            total = total + jnp.sum(read.reshape(step // 8, 8, vd), axis=0)
        found.append(jnp.sum(total, axis=0, keepdims=True))
    attended = jnp.concatenate(found, axis=0) + fresh
    scale = lax.rsqrt(jnp.sum(attended * attended, axis=1, keepdims=True) / vd + epsilon)
    gains = jnp.concatenate([gain[i : i + 1] for i in range(gain.shape[0])], axis=1)
    gated = attended * scale * gains.astype(jnp.float32) * (g / (1.0 + jnp.exp(-g)))
    out_ref[...] = gated.astype(jnp.bfloat16)


def attend(sums, bias, gain, state, model_width):
    rows, _, kd, vd = state.shape
    return pl.pallas_call(
        functools.partial(attend_kernel, model_width=model_width),
        out_shape=(
            pltpu.VMEM((rows, kd), jnp.float32),
            pltpu.VMEM((rows, vd), jnp.float32),
            pltpu.VMEM((rows, kd), jnp.float32),
            pltpu.VMEM((rows, vd), jnp.bfloat16),
        ),
        in_specs=whole(4),
        out_specs=whole(4),
        compiler_params=pltpu.CompilerParams(vmem_limit_bytes=8 << 20),
        name="attend",
    )(*(in_vmem(a) for a in (sums, bias, gain, state)))


def total_kernel(parts, out_ref):
    out_ref[...] = jnp.sum(parts[...].astype(jnp.float32), axis=1)


def total(parts):
    return pl.pallas_call(
        total_kernel,
        out_shape=pltpu.VMEM((parts.shape[0], *parts.shape[2:]), jnp.float32),
        in_specs=whole(1),
        out_specs=pl.BlockSpec(memory_space=pltpu.VMEM),
        compiler_params=pltpu.CompilerParams(vmem_limit_bytes=8 << 20),
        name="total",
    )(in_vmem(parts))


def widen_kernel(parts, mine, got, _, out_ref, mid_ref):
    r = member(lax.axis_index("kv"))
    _, seqs = mid_ref.shape
    half = out_ref.shape[1] // 2
    end = 3 * half

    def mid_of(ref, at):
        return (ref[:, end : end + seqs].astype(jnp.float32) + parts[at]).astype(jnp.bfloat16)

    own = mid_of(mine, r)
    mid_ref[...] = own
    x = jnp.concatenate([own, mid_of(got, 1 - r)], axis=0).astype(jnp.float32).T
    gains = mine[0:1, end + seqs :].astype(jnp.float32) + got[0:1, end + seqs :].astype(jnp.float32)
    ffn_in = (x * gains).astype(jnp.bfloat16)
    squares = jnp.sum(x * x, axis=1, keepdims=True)
    weights = jnp.concatenate([mine[:, : 2 * half], got[:, : 2 * half]], axis=0)
    made = jnp.dot(ffn_in, weights, preferred_element_type=jnp.float32)
    lane = lax.broadcasted_iota(jnp.int32, (seqs, 128), 1)
    out_ref[...] = made.astype(jnp.bfloat16)
    out_ref[:, half - 128 : half] = jnp.where(lane == 127, squares, made[:, half - 128 : half]).astype(
        jnp.bfloat16
    )


def widen(parts, mine, got, new_state, half):
    width, seqs = parts.shape[1:]
    return pl.pallas_call(
        widen_kernel,
        out_shape=(
            pltpu.VMEM((seqs, 2 * half), jnp.bfloat16),
            pltpu.VMEM((width, seqs), jnp.bfloat16),
        ),
        in_specs=whole(4),
        out_specs=whole(2),
        compiler_params=pltpu.CompilerParams(vmem_limit_bytes=8 << 20),
        name="widen",
    )(*(in_vmem(a) for a in (parts, mine, got, new_state)))


def narrow_kernel(hidden, mine, got, out_ref):
    r = member(lax.axis_index("kv"))
    half = hidden.shape[1]
    copies, _ = out_ref.shape[1:3]
    for ref, at in ((mine, r), (got, 1 - r)):
        made = lax.dot_general(
            ref[:, 2 * half : 3 * half],
            hidden[...],
            (((1,), (1,)), ((), ())),
            preferred_element_type=jnp.float32,
        ).astype(jnp.bfloat16)
        for j in range(copies):
            out_ref[at, j] = made


def narrow(hidden, mine, got, tp):
    width, seqs = (mine.shape[0], hidden.shape[0])
    return pl.pallas_call(
        narrow_kernel,
        out_shape=pltpu.VMEM((2, tp, width, seqs), jnp.bfloat16),
        in_specs=whole(3),
        out_specs=pl.BlockSpec(memory_space=pltpu.VMEM),
        compiler_params=pltpu.CompilerParams(vmem_limit_bytes=8 << 20),
        name="narrow",
    )(*(in_vmem(a) for a in (hidden, mine, got)))


def exchanged(blocks, axis, groups=None):
    return lax.all_to_all(blocks, axis, 0, 0, axis_index_groups=groups, tiled=True)


def summed(blocks):
    return jnp.sum(blocks.astype(jnp.float32), axis=0)


def copies_of(x, count):
    return jnp.broadcast_to(x[None], (count, *x.shape))


def local(
    tokens,
    mix_gain,
    ffn_gain,
    w_query,
    w_key,
    w_value,
    w_gate,
    w_decay,
    decay_bias,
    head_gain,
    w_output,
    w_ffgate,
    w_ffup,
    w_down,
    state,
):
    own_rows, heads, _, val_dim = state.shape
    kv, tp = (lax.axis_size(a) for a in ("kv", "tp"))
    model_width = tokens.shape[1] * kv
    made, bias, head_scale, ffn_scale = project(
        tokens.T,
        mix_gain[None, :],
        (w_query, w_key, w_value, w_gate, w_decay),
        (decay_bias[None, :], head_gain.reshape(-1, 128), ffn_gain[None, :]),
    )
    arrived = exchanged(made.reshape(kv, own_rows, -1), "kv")
    keys, values, decay, head_out = attend(summed(arrived), bias, head_scale, state, model_width)
    heads_all = exchanged(copies_of(head_out, kv), "kv")
    mine, sent = pack(head_out, tokens.T, ffn_scale, (w_ffgate, w_ffup, w_down.T))
    got = lax.ppermute(sent, "kv", [(i, i ^ 1) for i in range(kv)])
    new_state = (
        decay[:, None, :, None] * state + keys[:, None, :, None] * values[:, None, None, :]
    )
    heads_all = heads_all.reshape(-1, heads * val_dim)
    attn_part = lax.dot_general(
        w_output, heads_all, (((0,), (1,)), ((), ())), preferred_element_type=jnp.float32
    ).astype(jnp.bfloat16)
    attn_part, new_state = lax.optimization_barrier((attn_part, new_state))
    width, seqs = attn_part.shape
    pair, line = (pairs(kv, tp), lines(kv))
    attn_parts = exchanged(copies_of(attn_part, 2 * tp), ("kv", "tp"), pair)
    half = half_of(w_ffgate.shape[1])
    attn_sums = total(attn_parts.reshape(2, tp, width, seqs))
    wide, mid_t = widen(attn_sums, mine, got, new_state, half)
    count = len(line[0])
    sums = summed(exchanged(wide.reshape(count, seqs // count, -1), "kv", line))
    ffn_rms = lax.rsqrt(sums[:, half - 1 : half] / model_width + epsilon)
    gated = jax.nn.silu(sums[:, :half] * ffn_rms) * (sums[:, half:] * ffn_rms)
    hidden = gated.astype(jnp.bfloat16)
    hidden_all = exchanged(copies_of(hidden, count), "kv", line).reshape(seqs, half)
    down_parts = narrow(hidden_all, mine, got, tp).reshape(2 * tp, width, seqs)
    mixed = (
        mid_t.astype(jnp.float32) + summed(exchanged(down_parts, ("kv", "tp"), pair))
    ).astype(jnp.bfloat16)
    return (mixed.T, new_state)


def solution(mesh):
    in_specs = (
        P(None, "kv"),
        P("kv"),
        P("kv"),
        P("kv", "tp"),
        P("kv", "tp"),
        P("kv", "tp"),
        P("kv", "tp"),
        P("kv", "tp"),
        P("tp"),
        P(),
        P("tp", "kv"),
        P("kv", "tp"),
        P("kv", "tp"),
        P("tp", "kv"),
        P("kv", "tp", None, None),
    )
    out_specs = (P(None, "kv"), P("kv", "tp", None, None))
    return jax.shard_map(local, mesh=mesh, in_specs=in_specs, out_specs=out_specs, check_vma=False)
```

```python
import functools

import jax
import jax.numpy as jnp
from jax import lax
from jax.experimental import pallas as pl
from jax.experimental.pallas import tpu as pltpu
from jax.sharding import PartitionSpec as P

epsilon = 1e-06


def member(kv):
    return (kv ^ (kv >> 2)) & 1


def lines(kv):
    return [[i for i in range(kv) if member(i) == m] for m in range(2)]


def pairs(kv, tp):
    return [
        [i * tp + t for i in sorted((j, j + 1), key=member) for t in range(tp)]
        for j in range(0, kv, 2)
    ]


def padded(n):
    return -(-n // 128) * 128


def in_vmem(x):
    return pltpu.with_memory_space_constraint(x, pltpu.VMEM)


def whole(count):
    return [pl.BlockSpec(memory_space=pltpu.VMEM)] * count


def widths(units):
    half = units // 2
    return half, padded(2 * half + 1), padded(half)


def fetch(sources, held, sems):
    copies = [pltpu.make_async_copy(a, b, sems.at[i]) for i, (a, b) in enumerate(zip(sources, held))]
    for c in copies:
        c.start()
    return copies


def project_kernel(*refs, count, kept):
    sources, out_ref = (refs[:count], refs[count])
    held = refs[count + 1 + kept : -1] + refs[count + 1 : count + 1 + kept]
    copies = fetch(sources, held, refs[-1])
    tok, gain = held[:2]
    copies[0].wait()
    copies[1].wait()
    x = tok[...].astype(jnp.float32).T
    mix_in = (x * gain[...].astype(jnp.float32)).astype(jnp.bfloat16)
    squares = jnp.sum(x * x, axis=1, keepdims=True)
    at = 0
    for copy, w in zip(copies[2 : count - kept], held[2 : count - kept]):
        copy.wait()
        n = w.shape[1]
        part = jnp.dot(mix_in, w[...], preferred_element_type=jnp.float32)
        out_ref[:, at : at + n] = part.astype(jnp.bfloat16)
        at += n
    rest = out_ref.shape[1] - at
    lane = lax.broadcasted_iota(jnp.int32, (x.shape[0], rest), 1)
    out_ref[:, at:] = jnp.where(lane == 0, squares, 0.0).astype(jnp.bfloat16)
    for copy in copies[count - kept :]:
        copy.wait()


def project(tok_t, gain, weights, kept):
    total = sum(w.shape[1] for w in weights)
    arrays = (tok_t, gain, *weights, *kept)
    return pl.pallas_call(
        functools.partial(project_kernel, count=len(arrays), kept=len(kept)),
        out_shape=(
            pltpu.VMEM((tok_t.shape[1], total + 128), jnp.bfloat16),
            *(pltpu.VMEM(a.shape, a.dtype) for a in kept),
        ),
        in_specs=[pl.BlockSpec(memory_space=pl.ANY)] * len(arrays),
        out_specs=whole(1 + len(kept)),
        scratch_shapes=[pltpu.VMEM(a.shape, a.dtype) for a in arrays[: len(arrays) - len(kept)]]
        + [pltpu.SemaphoreType.DMA((len(arrays),))],
        name="project",
    )(*arrays)


def pack_kernel(_, tok, ffn_gain, *refs):
    splits, (mine_ref, sent_ref) = (refs[:-2], refs[-2:])
    rows, units = splits[0].shape
    seqs = tok.shape[1]
    half, both, alone = widths(units)

    def fill(ref, m, first):
        gate, up, down = (w[:, m * half : (m + 1) * half] for w in splits)
        ref[:, :half] = gate
        ref[:, half : 2 * half] = up
        ref[:, 2 * half : both] = jnp.zeros((rows, both - 2 * half), ref.dtype)
        ref[:, both : both + half] = down
        ref[:, both + half : both + alone] = jnp.zeros((rows, alone - half), ref.dtype)
        end = both + alone
        ref[:, end : end + seqs] = tok[...]
        ref[:, end + seqs :] = jnp.zeros((rows, 2 * rows), ref.dtype)
        side = 0 if first else rows
        ref[0:1, end + seqs + side : end + seqs + side + rows] = ffn_gain[...]

    for m in range(2):

        @pl.when(member(lax.axis_index("kv")) == m)
        def _():
            fill(mine_ref, m, True)
            fill(sent_ref, 1 - m, False)


def pack(after, tok_t, ffn_gain, splits):
    width, rows = tok_t.shape
    lanes = sum(widths(splits[0].shape[1])[1:]) + rows + 2 * width
    arrays = (after, tok_t, ffn_gain, *splits)
    return pl.pallas_call(
        pack_kernel,
        out_shape=(pltpu.VMEM((width, lanes), jnp.bfloat16),) * 2,
        in_specs=whole(len(arrays)),
        out_specs=whole(2),
        compiler_params=pltpu.CompilerParams(vmem_limit_bytes=8 << 20),
        name="pack",
    )(*(in_vmem(a) for a in arrays))


def attend_kernel(sums, bias, gain, state, key_ref, value_ref, decay_ref, out_ref, *, model_width):
    rows, _, kd, vd = state.shape
    base = sums[...]
    rms = lax.rsqrt(base[:, 3 * kd + 2 * vd : 3 * kd + 2 * vd + 1] / model_width + epsilon)
    q = base[:, :kd] * rms * kd**-0.5
    k = base[:, kd : 2 * kd] * rms
    v = base[:, 2 * kd : 2 * kd + vd] * rms
    g = base[:, 2 * kd + vd : 2 * kd + 2 * vd] * rms
    x = base[:, 2 * kd + 2 * vd : 3 * kd + 2 * vd] * rms + bias[...]
    log_sigmoid = jnp.minimum(x, 0.0) - jnp.log1p(jnp.exp(-jnp.abs(x)))
    decay = jnp.exp(log_sigmoid / 16.0)
    key_ref[...] = k
    value_ref[...] = v
    decay_ref[...] = decay
    fresh = jnp.sum(q * k, axis=1, keepdims=True) * v
    columns = jnp.concatenate([q * decay, jnp.zeros((8 - rows, kd), jnp.float32)], axis=0).T
    step = 32
    found = []
    for s in range(rows):
        total = jnp.zeros((8, vd), jnp.float32)
        for at in range(0, kd, step):
            read = columns[at : at + step, s : s + 1] * state[s, 0, at : at + step]
            total = total + jnp.sum(read.reshape(step // 8, 8, vd), axis=0)
        found.append(jnp.sum(total, axis=0, keepdims=True))
    attended = jnp.concatenate(found, axis=0) + fresh
    scale = lax.rsqrt(jnp.sum(attended * attended, axis=1, keepdims=True) / vd + epsilon)
    gains = jnp.concatenate([gain[i : i + 1] for i in range(gain.shape[0])], axis=1)
    gated = attended * scale * gains.astype(jnp.float32) * (g / (1.0 + jnp.exp(-g)))
    out_ref[...] = gated.astype(jnp.bfloat16)


def attend(sums, bias, gain, state, model_width):
    rows, _, kd, vd = state.shape
    return pl.pallas_call(
        functools.partial(attend_kernel, model_width=model_width),
        out_shape=(
            pltpu.VMEM((rows, kd), jnp.float32),
            pltpu.VMEM((rows, vd), jnp.float32),
            pltpu.VMEM((rows, kd), jnp.float32),
            pltpu.VMEM((rows, vd), jnp.bfloat16),
        ),
        in_specs=whole(4),
        out_specs=whole(4),
        compiler_params=pltpu.CompilerParams(vmem_limit_bytes=8 << 20),
        name="attend",
    )(*(in_vmem(a) for a in (sums, bias, gain, state)))


def total_kernel(parts, out_ref):
    out_ref[...] = jnp.sum(parts[...].astype(jnp.float32), axis=1)


def total(parts):
    return pl.pallas_call(
        total_kernel,
        out_shape=pltpu.VMEM((parts.shape[0], *parts.shape[2:]), jnp.float32),
        in_specs=whole(1),
        out_specs=pl.BlockSpec(memory_space=pltpu.VMEM),
        compiler_params=pltpu.CompilerParams(vmem_limit_bytes=8 << 20),
        name="total",
    )(in_vmem(parts))


def widen_kernel(parts, mine, got, _, out_ref, mid_ref, *, alone):
    r = member(lax.axis_index("kv"))
    _, seqs = mid_ref.shape
    both = out_ref.shape[-1]
    end = both + alone

    def mid_of(ref, at):
        return (ref[:, end : end + seqs].astype(jnp.float32) + parts[at]).astype(jnp.bfloat16)

    own = mid_of(mine, r)
    mid_ref[...] = own
    x = jnp.concatenate([own, mid_of(got, 1 - r)], axis=0).astype(jnp.float32).T
    gains = mine[0:1, end + seqs :].astype(jnp.float32) + got[0:1, end + seqs :].astype(jnp.float32)
    ffn_in = (x * gains).astype(jnp.bfloat16)
    squares = jnp.sum(x * x, axis=1, keepdims=True)
    weights = jnp.concatenate([mine[:, :both], got[:, :both]], axis=0)
    made = jnp.dot(ffn_in, weights, preferred_element_type=jnp.float32)
    lane = lax.broadcasted_iota(jnp.int32, (seqs, 128), 1)
    out_ref[...] = made.astype(jnp.bfloat16)
    out_ref[:, both - 128 :] = jnp.where(lane == 127, squares, made[:, both - 128 :]).astype(
        jnp.bfloat16
    )


def widen(parts, mine, got, new_state, units):
    width, seqs = parts.shape[1:]
    _, both, alone = widths(units)
    return pl.pallas_call(
        functools.partial(widen_kernel, alone=alone),
        out_shape=(
            pltpu.VMEM((seqs, both), jnp.bfloat16),
            pltpu.VMEM((width, seqs), jnp.bfloat16),
        ),
        in_specs=whole(4),
        out_specs=whole(2),
        compiler_params=pltpu.CompilerParams(vmem_limit_bytes=8 << 20),
        name="widen",
    )(*(in_vmem(a) for a in (parts, mine, got, new_state)))


def gate_kernel(sums, out_ref, *, half, model_width):
    rows, both = sums.shape
    alone = out_ref.shape[-1]
    rms = lax.rsqrt(sums[:, both - 1 :] / model_width + epsilon)
    gate = sums[:, :half] * rms
    up = sums[:, half : 2 * half] * rms
    hidden = gate / (1.0 + jnp.exp(-gate)) * up
    filled = jnp.concatenate([hidden, jnp.zeros((rows, alone - half), jnp.float32)], axis=1)
    out_ref[...] = jnp.broadcast_to(filled.astype(jnp.bfloat16)[None], out_ref.shape)


def gate_units(sums, units, model_width, copies):
    half, _, alone = widths(units)
    return pl.pallas_call(
        functools.partial(gate_kernel, half=half, model_width=model_width),
        out_shape=pltpu.VMEM((copies, sums.shape[0], alone), jnp.bfloat16),
        in_specs=whole(1),
        out_specs=pl.BlockSpec(memory_space=pltpu.VMEM),
        compiler_params=pltpu.CompilerParams(vmem_limit_bytes=8 << 20),
        name="gate",
    )(in_vmem(sums))


def narrow_kernel(hidden, mine, got, out_ref, *, both):
    r = member(lax.axis_index("kv"))
    alone = hidden.shape[1]
    copies, _ = out_ref.shape[1:3]
    for ref, at in ((mine, r), (got, 1 - r)):
        made = lax.dot_general(
            ref[:, both : both + alone],
            hidden[...],
            (((1,), (1,)), ((), ())),
            preferred_element_type=jnp.float32,
        ).astype(jnp.bfloat16)
        for j in range(copies):
            out_ref[at, j] = made


def narrow(hidden, mine, got, units, tp):
    width, seqs = (mine.shape[0], hidden.shape[0])
    return pl.pallas_call(
        functools.partial(narrow_kernel, both=widths(units)[1]),
        out_shape=pltpu.VMEM((2, tp, width, seqs), jnp.bfloat16),
        in_specs=whole(3),
        out_specs=pl.BlockSpec(memory_space=pltpu.VMEM),
        compiler_params=pltpu.CompilerParams(vmem_limit_bytes=8 << 20),
        name="narrow",
    )(*(in_vmem(a) for a in (hidden, mine, got)))


def exchanged(blocks, axis, groups=None):
    return lax.all_to_all(blocks, axis, 0, 0, axis_index_groups=groups, tiled=True)


def summed(blocks):
    return jnp.sum(blocks.astype(jnp.float32), axis=0)


def copies_of(x, count):
    return jnp.broadcast_to(x[None], (count, *x.shape))


def local(
    tokens,
    mix_gain,
    ffn_gain,
    w_query,
    w_key,
    w_value,
    w_gate,
    w_decay,
    decay_bias,
    head_gain,
    w_output,
    w_ffgate,
    w_ffup,
    w_down,
    state,
):
    own_rows, heads, _, val_dim = state.shape
    kv, tp = (lax.axis_size(a) for a in ("kv", "tp"))
    model_width = tokens.shape[1] * kv
    made, bias, head_scale, ffn_scale = project(
        tokens.T,
        mix_gain[None, :],
        (w_query, w_key, w_value, w_gate, w_decay),
        (decay_bias[None, :], head_gain.reshape(-1, 128), ffn_gain[None, :]),
    )
    arrived = exchanged(made.reshape(kv, own_rows, -1), "kv")
    keys, values, decay, head_out = attend(summed(arrived), bias, head_scale, state, model_width)
    heads_all = exchanged(copies_of(head_out, kv), "kv")
    mine, sent = pack(head_out, tokens.T, ffn_scale, (w_ffgate, w_ffup, w_down.T))
    got = lax.ppermute(sent, "kv", [(i, i ^ 1) for i in range(kv)])
    new_state = (
        decay[:, None, :, None] * state + keys[:, None, :, None] * values[:, None, None, :]
    )
    heads_all = heads_all.reshape(-1, heads * val_dim)
    attn_part = lax.dot_general(
        w_output, heads_all, (((0,), (1,)), ((), ())), preferred_element_type=jnp.float32
    ).astype(jnp.bfloat16)
    attn_part, new_state = lax.optimization_barrier((attn_part, new_state))
    width, seqs = attn_part.shape
    pair, line = (pairs(kv, tp), lines(kv))
    attn_parts = exchanged(copies_of(attn_part, 2 * tp), ("kv", "tp"), pair)
    units = w_ffgate.shape[1]
    attn_sums = total(attn_parts.reshape(2, tp, width, seqs))
    wide, mid_t = widen(attn_sums, mine, got, new_state, units)
    count = len(line[0])
    sums = summed(exchanged(wide.reshape(count, seqs // count, -1), "kv", line))
    hidden = exchanged(gate_units(sums, units, model_width, count), "kv", line)
    down_parts = narrow(hidden.reshape(seqs, -1), mine, got, units, tp).reshape(2 * tp, width, seqs)
    mixed = (
        mid_t.astype(jnp.float32) + summed(exchanged(down_parts, ("kv", "tp"), pair))
    ).astype(jnp.bfloat16)
    return (mixed.T, new_state)


def solution(mesh):
    in_specs = (
        P(None, "kv"),
        P("kv"),
        P("kv"),
        P("kv", "tp"),
        P("kv", "tp"),
        P("kv", "tp"),
        P("kv", "tp"),
        P("kv", "tp"),
        P("tp"),
        P(),
        P("tp", "kv"),
        P("kv", "tp"),
        P("kv", "tp"),
        P("tp", "kv"),
        P("kv", "tp", None, None),
    )
    out_specs = (P(None, "kv"), P("kv", "tp", None, None))
    return jax.shard_map(local, mesh=mesh, in_specs=in_specs, out_specs=out_specs, check_vma=False)
```

```python
import functools

import jax
import jax.numpy as jnp
from jax import lax
from jax.experimental import pallas as pl
from jax.experimental.pallas import tpu as pltpu
from jax.sharding import PartitionSpec as P

epsilon = 1e-06


def member(kv):
    return (kv ^ (kv >> 2)) & 1


def lines(kv):
    return [[i for i in range(kv) if member(i) == m] for m in range(2)]


def pairs(kv, tp):
    return [
        [i * tp + t for i in sorted((j, j + 1), key=member) for t in range(tp)]
        for j in range(0, kv, 2)
    ]


def padded(n):
    return -(-n // 128) * 128


def in_vmem(x):
    return pltpu.with_memory_space_constraint(x, pltpu.VMEM)


def whole(count):
    return [pl.BlockSpec(memory_space=pltpu.VMEM)] * count


def widths(units):
    half = units // 2
    return half, padded(2 * half + 1), padded(half)


def fetch(sources, held, sems):
    copies = [pltpu.make_async_copy(a, b, sems.at[i]) for i, (a, b) in enumerate(zip(sources, held))]
    for c in copies:
        c.start()
    return copies


def project_kernel(*refs, count, kept):
    sources, out_ref = (refs[:count], refs[count])
    held = refs[count + 1 + kept : -1] + refs[count + 1 : count + 1 + kept]
    copies = fetch(sources, held, refs[-1])
    tok, gain = held[:2]
    copies[0].wait()
    copies[1].wait()
    x = tok[...].astype(jnp.float32).T
    mix_in = (x * gain[...].astype(jnp.float32)).astype(jnp.bfloat16)
    squares = jnp.sum(x * x, axis=1, keepdims=True)
    at = 0
    for copy, w in zip(copies[2 : count - kept], held[2 : count - kept]):
        copy.wait()
        n = w.shape[1]
        part = jnp.dot(mix_in, w[...], preferred_element_type=jnp.float32)
        out_ref[..., at : at + n] = part.reshape(*out_ref.shape[:2], n).astype(jnp.bfloat16)
        at += n
    rest = out_ref.shape[2] - at
    lane = lax.broadcasted_iota(jnp.int32, (x.shape[0], rest), 1)
    last = jnp.where(lane == 0, squares, 0.0)
    out_ref[..., at:] = last.reshape(*out_ref.shape[:2], rest).astype(jnp.bfloat16)
    for copy in copies[count - kept :]:
        copy.wait()


def project(tok_t, gain, weights, kept, count):
    total = sum(w.shape[1] for w in weights)
    arrays = (tok_t, gain, *weights, *kept)
    return pl.pallas_call(
        functools.partial(project_kernel, count=len(arrays), kept=len(kept)),
        out_shape=(
            pltpu.VMEM((count, tok_t.shape[1] // count, total + 128), jnp.bfloat16),
            *(pltpu.VMEM(a.shape, a.dtype) for a in kept),
        ),
        in_specs=[pl.BlockSpec(memory_space=pl.ANY)] * len(arrays),
        out_specs=whole(1 + len(kept)),
        scratch_shapes=[pltpu.VMEM(a.shape, a.dtype) for a in arrays[: len(arrays) - len(kept)]]
        + [pltpu.SemaphoreType.DMA((len(arrays),))],
        name="project",
    )(*arrays)


def pack_kernel(_, tok, ffn_gain, *refs):
    splits, (mine_ref, sent_ref) = (refs[:-2], refs[-2:])
    rows, units = splits[0].shape
    seqs = tok.shape[1]
    half, both, alone = widths(units)

    def fill(ref, m, first):
        gate, up, down = (w[:, m * half : (m + 1) * half] for w in splits)
        ref[:, :half] = gate
        ref[:, half : 2 * half] = up
        ref[:, 2 * half : both] = jnp.zeros((rows, both - 2 * half), ref.dtype)
        ref[:, both : both + half] = down
        ref[:, both + half : both + alone] = jnp.zeros((rows, alone - half), ref.dtype)
        end = both + alone
        ref[:, end : end + seqs] = tok[...]
        ref[:, end + seqs :] = jnp.zeros((rows, 2 * rows), ref.dtype)
        side = 0 if first else rows
        ref[0:1, end + seqs + side : end + seqs + side + rows] = ffn_gain[...]

    for m in range(2):

        @pl.when(member(lax.axis_index("kv")) == m)
        def _():
            fill(mine_ref, m, True)
            fill(sent_ref, 1 - m, False)


def pack(after, tok_t, ffn_gain, splits):
    width, rows = tok_t.shape
    lanes = sum(widths(splits[0].shape[1])[1:]) + rows + 2 * width
    arrays = (after, tok_t, ffn_gain, *splits)
    return pl.pallas_call(
        pack_kernel,
        out_shape=(pltpu.VMEM((width, lanes), jnp.bfloat16),) * 2,
        in_specs=whole(len(arrays)),
        out_specs=whole(2),
        compiler_params=pltpu.CompilerParams(vmem_limit_bytes=8 << 20),
        name="pack",
    )(*(in_vmem(a) for a in arrays))


def attend_kernel(sums, bias, gain, state, key_ref, value_ref, decay_ref, out_ref, *, model_width):
    rows, _, kd, vd = state.shape
    base = sums[...]
    rms = lax.rsqrt(base[:, 3 * kd + 2 * vd : 3 * kd + 2 * vd + 1] / model_width + epsilon)
    q = base[:, :kd] * rms * kd**-0.5
    k = base[:, kd : 2 * kd] * rms
    v = base[:, 2 * kd : 2 * kd + vd] * rms
    g = base[:, 2 * kd + vd : 2 * kd + 2 * vd] * rms
    x = base[:, 2 * kd + 2 * vd : 3 * kd + 2 * vd] * rms + bias[...]
    log_sigmoid = jnp.minimum(x, 0.0) - jnp.log1p(jnp.exp(-jnp.abs(x)))
    decay = jnp.exp(log_sigmoid / 16.0)
    key_ref[...] = k
    value_ref[...] = v
    decay_ref[...] = decay
    fresh = jnp.sum(q * k, axis=1, keepdims=True) * v
    columns = jnp.concatenate([q * decay, jnp.zeros((8 - rows, kd), jnp.float32)], axis=0).T
    step = 32
    found = []
    for s in range(rows):
        total = jnp.zeros((8, vd), jnp.float32)
        for at in range(0, kd, step):
            read = columns[at : at + step, s : s + 1] * state[s, 0, at : at + step]
            total = total + jnp.sum(read.reshape(step // 8, 8, vd), axis=0)
        found.append(jnp.sum(total, axis=0, keepdims=True))
    attended = jnp.concatenate(found, axis=0) + fresh
    scale = lax.rsqrt(jnp.sum(attended * attended, axis=1, keepdims=True) / vd + epsilon)
    gains = jnp.concatenate([gain[i : i + 1] for i in range(gain.shape[0])], axis=1)
    gated = attended * scale * gains.astype(jnp.float32) * (g / (1.0 + jnp.exp(-g)))
    out_ref[...] = gated.astype(jnp.bfloat16)


def attend(sums, bias, gain, state, model_width):
    rows, _, kd, vd = state.shape
    return pl.pallas_call(
        functools.partial(attend_kernel, model_width=model_width),
        out_shape=(
            pltpu.VMEM((rows, kd), jnp.float32),
            pltpu.VMEM((rows, vd), jnp.float32),
            pltpu.VMEM((rows, kd), jnp.float32),
            pltpu.VMEM((rows, vd), jnp.bfloat16),
        ),
        in_specs=whole(4),
        out_specs=whole(4),
        compiler_params=pltpu.CompilerParams(vmem_limit_bytes=8 << 20),
        name="attend",
    )(*(in_vmem(a) for a in (sums, bias, gain, state)))


def total_kernel(parts, out_ref):
    out_ref[...] = jnp.sum(parts[...].astype(jnp.float32), axis=1)


def total(parts):
    return pl.pallas_call(
        total_kernel,
        out_shape=pltpu.VMEM((parts.shape[0], *parts.shape[2:]), jnp.float32),
        in_specs=whole(1),
        out_specs=pl.BlockSpec(memory_space=pltpu.VMEM),
        compiler_params=pltpu.CompilerParams(vmem_limit_bytes=8 << 20),
        name="total",
    )(in_vmem(parts))


def widen_kernel(parts, mine, got, _, out_ref, mid_ref, *, alone):
    r = member(lax.axis_index("kv"))
    _, seqs = mid_ref.shape
    both = out_ref.shape[-1]
    end = both + alone

    def mid_of(ref, at):
        return (ref[:, end : end + seqs].astype(jnp.float32) + parts[at]).astype(jnp.bfloat16)

    own = mid_of(mine, r)
    mid_ref[...] = own
    x = jnp.concatenate([own, mid_of(got, 1 - r)], axis=0).astype(jnp.float32).T
    gains = mine[0:1, end + seqs :].astype(jnp.float32) + got[0:1, end + seqs :].astype(jnp.float32)
    ffn_in = (x * gains).astype(jnp.bfloat16)
    squares = jnp.sum(x * x, axis=1, keepdims=True)
    weights = jnp.concatenate([mine[:, :both], got[:, :both]], axis=0)
    made = jnp.dot(ffn_in, weights, preferred_element_type=jnp.float32)
    lane = lax.broadcasted_iota(jnp.int32, (seqs, 128), 1)
    last = jnp.where(lane == 127, squares, made[:, both - 128 :])
    made = jnp.concatenate([made[:, : both - 128], last], axis=1)
    out_ref[...] = made.reshape(out_ref.shape).astype(jnp.bfloat16)


def widen(parts, mine, got, new_state, units, count):
    width, seqs = parts.shape[1:]
    _, both, alone = widths(units)
    return pl.pallas_call(
        functools.partial(widen_kernel, alone=alone),
        out_shape=(
            pltpu.VMEM((count, seqs // count, both), jnp.bfloat16),
            pltpu.VMEM((width, seqs), jnp.bfloat16),
        ),
        in_specs=whole(4),
        out_specs=whole(2),
        compiler_params=pltpu.CompilerParams(vmem_limit_bytes=8 << 20),
        name="widen",
    )(*(in_vmem(a) for a in (parts, mine, got, new_state)))


def gate_kernel(sums, out_ref, *, half, model_width):
    rows, both = sums.shape
    alone = out_ref.shape[-1]
    rms = lax.rsqrt(sums[:, both - 1 :] / model_width + epsilon)
    gate = sums[:, :half] * rms
    up = sums[:, half : 2 * half] * rms
    hidden = gate / (1.0 + jnp.exp(-gate)) * up
    filled = jnp.concatenate([hidden, jnp.zeros((rows, alone - half), jnp.float32)], axis=1)
    out_ref[...] = jnp.broadcast_to(filled.astype(jnp.bfloat16)[None], out_ref.shape)


def gate_units(sums, units, model_width, copies):
    half, _, alone = widths(units)
    return pl.pallas_call(
        functools.partial(gate_kernel, half=half, model_width=model_width),
        out_shape=pltpu.VMEM((copies, sums.shape[0], alone), jnp.bfloat16),
        in_specs=whole(1),
        out_specs=pl.BlockSpec(memory_space=pltpu.VMEM),
        compiler_params=pltpu.CompilerParams(vmem_limit_bytes=8 << 20),
        name="gate",
    )(in_vmem(sums))


def narrow_kernel(hidden, mine, got, out_ref, *, both):
    r = member(lax.axis_index("kv"))
    alone = hidden.shape[1]
    copies, _ = out_ref.shape[1:3]
    for ref, at in ((mine, r), (got, 1 - r)):
        made = lax.dot_general(
            ref[:, both : both + alone],
            hidden[...],
            (((1,), (1,)), ((), ())),
            preferred_element_type=jnp.float32,
        ).astype(jnp.bfloat16)
        for j in range(copies):
            out_ref[at, j] = made


def narrow(hidden, mine, got, units, tp):
    width, seqs = (mine.shape[0], hidden.shape[0])
    return pl.pallas_call(
        functools.partial(narrow_kernel, both=widths(units)[1]),
        out_shape=pltpu.VMEM((2, tp, width, seqs), jnp.bfloat16),
        in_specs=whole(3),
        out_specs=pl.BlockSpec(memory_space=pltpu.VMEM),
        compiler_params=pltpu.CompilerParams(vmem_limit_bytes=8 << 20),
        name="narrow",
    )(*(in_vmem(a) for a in (hidden, mine, got)))


def exchanged(blocks, axis, groups=None):
    return lax.all_to_all(blocks, axis, 0, 0, axis_index_groups=groups, tiled=True)


def summed(blocks):
    return jnp.sum(blocks.astype(jnp.float32), axis=0)


def copies_of(x, count):
    return jnp.broadcast_to(x[None], (count, *x.shape))


def local(
    tokens,
    mix_gain,
    ffn_gain,
    w_query,
    w_key,
    w_value,
    w_gate,
    w_decay,
    decay_bias,
    head_gain,
    w_output,
    w_ffgate,
    w_ffup,
    w_down,
    state,
):
    _, heads, _, val_dim = state.shape
    kv, tp = (lax.axis_size(a) for a in ("kv", "tp"))
    model_width = tokens.shape[1] * kv
    made, bias, head_scale, ffn_scale = project(
        tokens.T,
        mix_gain[None, :],
        (w_query, w_key, w_value, w_gate, w_decay),
        (decay_bias[None, :], head_gain.reshape(-1, 128), ffn_gain[None, :]),
        kv,
    )
    arrived = exchanged(made, "kv")
    keys, values, decay, head_out = attend(summed(arrived), bias, head_scale, state, model_width)
    heads_all = exchanged(copies_of(head_out, kv), "kv")
    mine, sent = pack(head_out, tokens.T, ffn_scale, (w_ffgate, w_ffup, w_down.T))
    got = lax.ppermute(sent, "kv", [(i, i ^ 1) for i in range(kv)])
    new_state = (
        decay[:, None, :, None] * state + keys[:, None, :, None] * values[:, None, None, :]
    )
    heads_all = heads_all.reshape(-1, heads * val_dim)
    attn_part = lax.dot_general(
        w_output, heads_all, (((0,), (1,)), ((), ())), preferred_element_type=jnp.float32
    ).astype(jnp.bfloat16)
    attn_part, new_state = lax.optimization_barrier((attn_part, new_state))
    width, seqs = attn_part.shape
    pair, line = (pairs(kv, tp), lines(kv))
    attn_parts = exchanged(copies_of(attn_part, 2 * tp), ("kv", "tp"), pair)
    units = w_ffgate.shape[1]
    attn_sums = total(attn_parts.reshape(2, tp, width, seqs))
    count = len(line[0])
    wide, mid_t = widen(attn_sums, mine, got, new_state, units, count)
    sums = summed(exchanged(wide, "kv", line))
    hidden = exchanged(gate_units(sums, units, model_width, count), "kv", line)
    down_parts = narrow(hidden.reshape(seqs, -1), mine, got, units, tp).reshape(2 * tp, width, seqs)
    mixed = (
        mid_t.astype(jnp.float32) + summed(exchanged(down_parts, ("kv", "tp"), pair))
    ).astype(jnp.bfloat16)
    return (mixed.T, new_state)


def solution(mesh):
    in_specs = (
        P(None, "kv"),
        P("kv"),
        P("kv"),
        P("kv", "tp"),
        P("kv", "tp"),
        P("kv", "tp"),
        P("kv", "tp"),
        P("kv", "tp"),
        P("tp"),
        P(),
        P("tp", "kv"),
        P("kv", "tp"),
        P("kv", "tp"),
        P("tp", "kv"),
        P("kv", "tp", None, None),
    )
    out_specs = (P(None, "kv"), P("kv", "tp", None, None))
    return jax.shard_map(local, mesh=mesh, in_specs=in_specs, out_specs=out_specs, check_vma=False)
```

```python
import functools

import jax
import jax.numpy as jnp
from jax import lax
from jax.experimental import pallas as pl
from jax.experimental.pallas import tpu as pltpu
from jax.sharding import PartitionSpec as P

epsilon = 1e-06


def member(kv):
    return (kv ^ (kv >> 2)) & 1


def lines(kv):
    return [[i for i in range(kv) if member(i) == m] for m in range(2)]


def pairs(kv, tp):
    return [
        [i * tp + t for i in sorted((j, j + 1), key=member) for t in range(tp)]
        for j in range(0, kv, 2)
    ]


def padded(n):
    return -(-n // 128) * 128


def in_vmem(x):
    return pltpu.with_memory_space_constraint(x, pltpu.VMEM)


def whole(count):
    return [pl.BlockSpec(memory_space=pltpu.VMEM)] * count


def widths(units):
    half = units // 2
    return half, padded(2 * half + 1), padded(half)


def fetch(sources, held, sems):
    copies = [pltpu.make_async_copy(a, b, sems.at[i]) for i, (a, b) in enumerate(zip(sources, held))]
    for c in copies:
        c.start()
    return copies


def project_kernel(*refs, count, kept):
    sources, out_ref = (refs[:count], refs[count])
    held = refs[count + 1 + kept : -1] + refs[count + 1 : count + 1 + kept]
    copies = fetch(sources, held, refs[-1])
    tok, gain = held[:2]
    copies[0].wait()
    copies[1].wait()
    x = tok[...].astype(jnp.float32).T
    mix_in = (x * gain[...].astype(jnp.float32)).astype(jnp.bfloat16)
    squares = jnp.sum(x * x, axis=1, keepdims=True)
    at = 0
    for copy, w in zip(copies[2 : count - kept], held[2 : count - kept]):
        copy.wait()
        n = w.shape[1]
        part = jnp.dot(mix_in, w[...], preferred_element_type=jnp.float32)
        out_ref[:, at : at + n] = part.astype(jnp.bfloat16)
        at += n
    rest = out_ref.shape[1] - at
    lane = lax.broadcasted_iota(jnp.int32, (x.shape[0], rest), 1)
    out_ref[:, at:] = jnp.where(lane == 0, squares, 0.0).astype(jnp.bfloat16)
    for copy in copies[count - kept :]:
        copy.wait()


def project(tok_t, gain, weights, kept):
    total = sum(w.shape[1] for w in weights)
    arrays = (tok_t, gain, *weights, *kept)
    return pl.pallas_call(
        functools.partial(project_kernel, count=len(arrays), kept=len(kept)),
        out_shape=(
            pltpu.VMEM((tok_t.shape[1], total + 128), jnp.bfloat16),
            *(pltpu.VMEM(a.shape, a.dtype) for a in kept),
        ),
        in_specs=[pl.BlockSpec(memory_space=pl.ANY)] * len(arrays),
        out_specs=whole(1 + len(kept)),
        scratch_shapes=[pltpu.VMEM(a.shape, a.dtype) for a in arrays[: len(arrays) - len(kept)]]
        + [pltpu.SemaphoreType.DMA((len(arrays),))],
        name="project",
    )(*arrays)


def pack_kernel(_, tok, ffn_gain, *refs):
    splits, (mine_ref, sent_ref) = (refs[:-2], refs[-2:])
    rows, units = splits[0].shape
    seqs = tok.shape[1]
    half, both, alone = widths(units)

    def fill(ref, m, first):
        gate, up, down = (w[:, m * half : (m + 1) * half] for w in splits)
        ref[:, :half] = gate
        ref[:, half : 2 * half] = up
        ref[:, 2 * half : both] = jnp.zeros((rows, both - 2 * half), ref.dtype)
        ref[:, both : both + half] = down
        ref[:, both + half : both + alone] = jnp.zeros((rows, alone - half), ref.dtype)
        end = both + alone
        ref[:, end : end + seqs] = tok[...]
        ref[:, end + seqs :] = jnp.zeros((rows, 2 * rows), ref.dtype)
        side = 0 if first else rows
        ref[0:1, end + seqs + side : end + seqs + side + rows] = ffn_gain[...]

    for m in range(2):

        @pl.when(member(lax.axis_index("kv")) == m)
        def _():
            fill(mine_ref, m, True)
            fill(sent_ref, 1 - m, False)


def pack(after, tok_t, ffn_gain, splits):
    width, rows = tok_t.shape
    lanes = sum(widths(splits[0].shape[1])[1:]) + rows + 2 * width
    arrays = (after, tok_t, ffn_gain, *splits)
    return pl.pallas_call(
        pack_kernel,
        out_shape=(pltpu.VMEM((width, lanes), jnp.bfloat16),) * 2,
        in_specs=whole(len(arrays)),
        out_specs=whole(2),
        compiler_params=pltpu.CompilerParams(vmem_limit_bytes=8 << 20),
        name="pack",
    )(*(in_vmem(a) for a in arrays))


def attend_kernel(sums, bias, gain, state, key_ref, value_ref, decay_ref, out_ref, *, model_width):
    rows, _, kd, vd = state.shape
    base = sums[...]
    rms = lax.rsqrt(base[:, 3 * kd + 2 * vd : 3 * kd + 2 * vd + 1] / model_width + epsilon)
    q = base[:, :kd] * rms * kd**-0.5
    k = base[:, kd : 2 * kd] * rms
    v = base[:, 2 * kd : 2 * kd + vd] * rms
    g = base[:, 2 * kd + vd : 2 * kd + 2 * vd] * rms
    x = base[:, 2 * kd + 2 * vd : 3 * kd + 2 * vd] * rms + bias[...]
    log_sigmoid = jnp.minimum(x, 0.0) - jnp.log1p(jnp.exp(-jnp.abs(x)))
    decay = jnp.exp(log_sigmoid / 16.0)
    key_ref[...] = k
    value_ref[...] = v
    decay_ref[...] = decay
    fresh = jnp.sum(q * k, axis=1, keepdims=True) * v
    columns = jnp.concatenate([q * decay, jnp.zeros((8 - rows, kd), jnp.float32)], axis=0).T
    step = 32
    found = []
    for s in range(rows):
        total = jnp.zeros((8, vd), jnp.float32)
        for at in range(0, kd, step):
            read = columns[at : at + step, s : s + 1] * state[s, 0, at : at + step]
            total = total + jnp.sum(read.reshape(step // 8, 8, vd), axis=0)
        found.append(jnp.sum(total, axis=0, keepdims=True))
    attended = jnp.concatenate(found, axis=0) + fresh
    scale = lax.rsqrt(jnp.sum(attended * attended, axis=1, keepdims=True) / vd + epsilon)
    gains = jnp.concatenate([gain[i : i + 1] for i in range(gain.shape[0])], axis=1)
    gated = attended * scale * gains.astype(jnp.float32) * (g / (1.0 + jnp.exp(-g)))
    out_ref[...] = gated.astype(jnp.bfloat16)


def attend(sums, bias, gain, state, model_width):
    rows, _, kd, vd = state.shape
    return pl.pallas_call(
        functools.partial(attend_kernel, model_width=model_width),
        out_shape=(
            pltpu.VMEM((rows, kd), jnp.float32),
            pltpu.VMEM((rows, vd), jnp.float32),
            pltpu.VMEM((rows, kd), jnp.float32),
            pltpu.VMEM((rows, vd), jnp.bfloat16),
        ),
        in_specs=whole(4),
        out_specs=whole(4),
        compiler_params=pltpu.CompilerParams(vmem_limit_bytes=8 << 20),
        name="attend",
    )(*(in_vmem(a) for a in (sums, bias, gain, state)))


def join_kernel(heads, weights, out_ref):
    made = lax.dot_general(
        weights[...], heads[...], (((1,), (1,)), ((), ())), preferred_element_type=jnp.float32
    ).astype(jnp.bfloat16)
    for j in range(out_ref.shape[0]):
        out_ref[j] = made


def join(heads, weights, copies):
    return pl.pallas_call(
        join_kernel,
        out_shape=pltpu.VMEM((copies, weights.shape[0], heads.shape[0]), jnp.bfloat16),
        in_specs=whole(2),
        out_specs=pl.BlockSpec(memory_space=pltpu.VMEM),
        compiler_params=pltpu.CompilerParams(vmem_limit_bytes=8 << 20),
        name="join",
    )(*(in_vmem(a) for a in (heads, weights)))


def total_kernel(parts, out_ref):
    out_ref[...] = jnp.sum(parts[...].astype(jnp.float32), axis=1)


def total(parts):
    return pl.pallas_call(
        total_kernel,
        out_shape=pltpu.VMEM((parts.shape[0], *parts.shape[2:]), jnp.float32),
        in_specs=whole(1),
        out_specs=pl.BlockSpec(memory_space=pltpu.VMEM),
        compiler_params=pltpu.CompilerParams(vmem_limit_bytes=8 << 20),
        name="total",
    )(in_vmem(parts))


def widen_kernel(parts, mine, got, _, out_ref, mid_ref, *, alone):
    r = member(lax.axis_index("kv"))
    _, seqs = mid_ref.shape
    both = out_ref.shape[-1]
    end = both + alone

    def mid_of(ref, at):
        return (ref[:, end : end + seqs].astype(jnp.float32) + parts[at]).astype(jnp.bfloat16)

    own = mid_of(mine, r)
    mid_ref[...] = own
    x = jnp.concatenate([own, mid_of(got, 1 - r)], axis=0).astype(jnp.float32).T
    gains = mine[0:1, end + seqs :].astype(jnp.float32) + got[0:1, end + seqs :].astype(jnp.float32)
    ffn_in = (x * gains).astype(jnp.bfloat16)
    squares = jnp.sum(x * x, axis=1, keepdims=True)
    weights = jnp.concatenate([mine[:, :both], got[:, :both]], axis=0)
    made = jnp.dot(ffn_in, weights, preferred_element_type=jnp.float32)
    lane = lax.broadcasted_iota(jnp.int32, (seqs, 128), 1)
    last = jnp.where(lane == 127, squares, made[:, both - 128 :])
    made = jnp.concatenate([made[:, : both - 128], last], axis=1)
    out_ref[...] = made.reshape(out_ref.shape).astype(jnp.bfloat16)


def widen(parts, mine, got, new_state, units, count):
    width, seqs = parts.shape[1:]
    _, both, alone = widths(units)
    return pl.pallas_call(
        functools.partial(widen_kernel, alone=alone),
        out_shape=(
            pltpu.VMEM((count, seqs // count, both), jnp.bfloat16),
            pltpu.VMEM((width, seqs), jnp.bfloat16),
        ),
        in_specs=whole(4),
        out_specs=whole(2),
        compiler_params=pltpu.CompilerParams(vmem_limit_bytes=8 << 20),
        name="widen",
    )(*(in_vmem(a) for a in (parts, mine, got, new_state)))


def gate_kernel(sums, out_ref, *, half, model_width):
    rows, both = sums.shape
    alone = out_ref.shape[-1]
    rms = lax.rsqrt(sums[:, both - 1 :] / model_width + epsilon)
    gate = sums[:, :half] * rms
    up = sums[:, half : 2 * half] * rms
    hidden = gate / (1.0 + jnp.exp(-gate)) * up
    filled = jnp.concatenate([hidden, jnp.zeros((rows, alone - half), jnp.float32)], axis=1)
    out_ref[...] = jnp.broadcast_to(filled.astype(jnp.bfloat16)[None], out_ref.shape)


def gate_units(sums, units, model_width, copies):
    half, _, alone = widths(units)
    return pl.pallas_call(
        functools.partial(gate_kernel, half=half, model_width=model_width),
        out_shape=pltpu.VMEM((copies, sums.shape[0], alone), jnp.bfloat16),
        in_specs=whole(1),
        out_specs=pl.BlockSpec(memory_space=pltpu.VMEM),
        compiler_params=pltpu.CompilerParams(vmem_limit_bytes=8 << 20),
        name="gate",
    )(in_vmem(sums))


def narrow_kernel(hidden, mine, got, out_ref, *, both):
    r = member(lax.axis_index("kv"))
    alone = hidden.shape[1]
    copies, width = out_ref.shape[1:3]
    weights = jnp.concatenate([ref[:, both : both + alone] for ref in (mine, got)], axis=0)
    made = lax.dot_general(
        weights, hidden[...], (((1,), (1,)), ((), ())), preferred_element_type=jnp.float32
    ).astype(jnp.bfloat16)
    for j in range(copies):
        out_ref[r, j] = made[:width]
        out_ref[1 - r, j] = made[width:]


def narrow(hidden, mine, got, units, tp):
    width, seqs = (mine.shape[0], hidden.shape[0])
    return pl.pallas_call(
        functools.partial(narrow_kernel, both=widths(units)[1]),
        out_shape=pltpu.VMEM((2, tp, width, seqs), jnp.bfloat16),
        in_specs=whole(3),
        out_specs=pl.BlockSpec(memory_space=pltpu.VMEM),
        compiler_params=pltpu.CompilerParams(vmem_limit_bytes=8 << 20),
        name="narrow",
    )(*(in_vmem(a) for a in (hidden, mine, got)))


def exchanged(blocks, axis, groups=None):
    return lax.all_to_all(blocks, axis, 0, 0, axis_index_groups=groups, tiled=True)


def summed(blocks):
    return jnp.sum(blocks.astype(jnp.float32), axis=0)


def copies_of(x, count):
    return jnp.broadcast_to(x[None], (count, *x.shape))


def local(
    tokens,
    mix_gain,
    ffn_gain,
    w_query,
    w_key,
    w_value,
    w_gate,
    w_decay,
    decay_bias,
    head_gain,
    w_output,
    w_ffgate,
    w_ffup,
    w_down,
    state,
):
    own_rows, heads, _, val_dim = state.shape
    kv, tp = (lax.axis_size(a) for a in ("kv", "tp"))
    model_width = tokens.shape[1] * kv
    made, bias, head_scale, ffn_scale = project(
        tokens.T,
        mix_gain[None, :],
        (w_query, w_key, w_value, w_gate, w_decay),
        (decay_bias[None, :], head_gain.reshape(-1, 128), ffn_gain[None, :]),
    )
    arrived = exchanged(made.reshape(kv, own_rows, -1), "kv")
    keys, values, decay, head_out = attend(summed(arrived), bias, head_scale, state, model_width)
    heads_all = exchanged(copies_of(head_out, kv), "kv")
    mine, sent = pack(head_out, tokens.T, ffn_scale, (w_ffgate, w_ffup, w_down.T))
    got = lax.ppermute(sent, "kv", [(i, i ^ 1) for i in range(kv)])
    new_state = (
        decay[:, None, :, None] * state + keys[:, None, :, None] * values[:, None, None, :]
    )
    heads_all = heads_all.reshape(-1, heads * val_dim)
    attn_copies = join(heads_all, w_output.T, 2 * tp)
    attn_copies, new_state = lax.optimization_barrier((attn_copies, new_state))
    width, seqs = attn_copies.shape[1:]
    pair, line = (pairs(kv, tp), lines(kv))
    attn_parts = exchanged(attn_copies, ("kv", "tp"), pair)
    units = w_ffgate.shape[1]
    attn_sums = total(attn_parts.reshape(2, tp, width, seqs))
    count = len(line[0])
    wide, mid_t = widen(attn_sums, mine, got, new_state, units, count)
    sums = summed(exchanged(wide, "kv", line))
    hidden = exchanged(gate_units(sums, units, model_width, count), "kv", line)
    down_parts = narrow(hidden.reshape(seqs, -1), mine, got, units, tp).reshape(2 * tp, width, seqs)
    mixed = (
        mid_t.astype(jnp.float32) + summed(exchanged(down_parts, ("kv", "tp"), pair))
    ).astype(jnp.bfloat16)
    return (mixed.T, new_state)


def solution(mesh):
    in_specs = (
        P(None, "kv"),
        P("kv"),
        P("kv"),
        P("kv", "tp"),
        P("kv", "tp"),
        P("kv", "tp"),
        P("kv", "tp"),
        P("kv", "tp"),
        P("tp"),
        P(),
        P("tp", "kv"),
        P("kv", "tp"),
        P("kv", "tp"),
        P("tp", "kv"),
        P("kv", "tp", None, None),
    )
    out_specs = (P(None, "kv"), P("kv", "tp", None, None))
    return jax.shard_map(local, mesh=mesh, in_specs=in_specs, out_specs=out_specs, check_vma=False)
```

```python
import functools

import jax
import jax.numpy as jnp
from jax import lax
from jax.experimental import pallas as pl
from jax.experimental.pallas import tpu as pltpu
from jax.sharding import PartitionSpec as P

epsilon = 1e-06


STRIDE = 8


def member(kv):
    place = kv // STRIDE
    return (place ^ (place >> 2)) & 1


def lines(kv):
    return [[i for i in range(kv) if member(i) == m] for m in range(2)]


def pairs(kv, tp):
    return [
        [i * tp + t for i in sorted((j, j ^ STRIDE), key=member) for t in range(tp)]
        for j in range(kv)
        if j < j ^ STRIDE
    ]


def padded(n):
    return -(-n // 128) * 128


def in_vmem(x):
    return pltpu.with_memory_space_constraint(x, pltpu.VMEM)


def whole(count):
    return [pl.BlockSpec(memory_space=pltpu.VMEM)] * count


def widths(units):
    half = units // 2
    return half, padded(2 * half + 1), padded(half)


def fetch(sources, held, sems):
    copies = [pltpu.make_async_copy(a, b, sems.at[i]) for i, (a, b) in enumerate(zip(sources, held))]
    for c in copies:
        c.start()
    return copies


def project_kernel(*refs, count, kept):
    sources, out_ref = (refs[:count], refs[count])
    held = refs[count + 1 + kept : -1] + refs[count + 1 : count + 1 + kept]
    copies = fetch(sources, held, refs[-1])
    tok, gain = held[:2]
    copies[0].wait()
    copies[1].wait()
    x = tok[...].astype(jnp.float32).T
    mix_in = (x * gain[...].astype(jnp.float32)).astype(jnp.bfloat16)
    squares = jnp.sum(x * x, axis=1, keepdims=True)
    at = 0
    for copy, w in zip(copies[2 : count - kept], held[2 : count - kept]):
        copy.wait()
        n = w.shape[1]
        part = jnp.dot(mix_in, w[...], preferred_element_type=jnp.float32)
        out_ref[:, at : at + n] = part.astype(jnp.bfloat16)
        at += n
    rest = out_ref.shape[1] - at
    lane = lax.broadcasted_iota(jnp.int32, (x.shape[0], rest), 1)
    out_ref[:, at:] = jnp.where(lane == 0, squares, 0.0).astype(jnp.bfloat16)
    for copy in copies[count - kept :]:
        copy.wait()


def project(tok_t, gain, weights, kept):
    total = sum(w.shape[1] for w in weights)
    arrays = (tok_t, gain, *weights, *kept)
    return pl.pallas_call(
        functools.partial(project_kernel, count=len(arrays), kept=len(kept)),
        out_shape=(
            pltpu.VMEM((tok_t.shape[1], total + 128), jnp.bfloat16),
            *(pltpu.VMEM(a.shape, a.dtype) for a in kept),
        ),
        in_specs=[pl.BlockSpec(memory_space=pl.ANY)] * len(arrays),
        out_specs=whole(1 + len(kept)),
        scratch_shapes=[pltpu.VMEM(a.shape, a.dtype) for a in arrays[: len(arrays) - len(kept)]]
        + [pltpu.SemaphoreType.DMA((len(arrays),))],
        name="project",
    )(*arrays)


def pack_kernel(_, tok, ffn_gain, *refs):
    splits, (mine_ref, sent_ref) = (refs[:-2], refs[-2:])
    rows, units = splits[0].shape
    seqs = tok.shape[1]
    half, both, alone = widths(units)

    def fill(ref, m, first):
        gate, up, down = (w[:, m * half : (m + 1) * half] for w in splits)
        ref[:, :half] = gate
        ref[:, half : 2 * half] = up
        ref[:, 2 * half : both] = jnp.zeros((rows, both - 2 * half), ref.dtype)
        ref[:, both : both + half] = down
        ref[:, both + half : both + alone] = jnp.zeros((rows, alone - half), ref.dtype)
        end = both + alone
        ref[:, end : end + seqs] = tok[...]
        ref[:, end + seqs :] = jnp.zeros((rows, 2 * rows), ref.dtype)
        side = 0 if first else rows
        ref[0:1, end + seqs + side : end + seqs + side + rows] = ffn_gain[...]

    for m in range(2):

        @pl.when(member(lax.axis_index("kv")) == m)
        def _():
            fill(mine_ref, m, True)
            fill(sent_ref, 1 - m, False)


def pack(after, tok_t, ffn_gain, splits):
    width, rows = tok_t.shape
    lanes = sum(widths(splits[0].shape[1])[1:]) + rows + 2 * width
    arrays = (after, tok_t, ffn_gain, *splits)
    return pl.pallas_call(
        pack_kernel,
        out_shape=(pltpu.VMEM((width, lanes), jnp.bfloat16),) * 2,
        in_specs=whole(len(arrays)),
        out_specs=whole(2),
        compiler_params=pltpu.CompilerParams(vmem_limit_bytes=8 << 20),
        name="pack",
    )(*(in_vmem(a) for a in arrays))


def attend_kernel(sums, bias, gain, state, key_ref, value_ref, decay_ref, out_ref, *, model_width):
    rows, _, kd, vd = state.shape
    base = sums[...]
    rms = lax.rsqrt(base[:, 3 * kd + 2 * vd : 3 * kd + 2 * vd + 1] / model_width + epsilon)
    q = base[:, :kd] * rms * kd**-0.5
    k = base[:, kd : 2 * kd] * rms
    v = base[:, 2 * kd : 2 * kd + vd] * rms
    g = base[:, 2 * kd + vd : 2 * kd + 2 * vd] * rms
    x = base[:, 2 * kd + 2 * vd : 3 * kd + 2 * vd] * rms + bias[...]
    log_sigmoid = jnp.minimum(x, 0.0) - jnp.log1p(jnp.exp(-jnp.abs(x)))
    decay = jnp.exp(log_sigmoid / 16.0)
    key_ref[...] = k
    value_ref[...] = v
    decay_ref[...] = decay
    fresh = jnp.sum(q * k, axis=1, keepdims=True) * v
    columns = jnp.concatenate([q * decay, jnp.zeros((8 - rows, kd), jnp.float32)], axis=0).T
    step = 32
    found = []
    for s in range(rows):
        total = jnp.zeros((8, vd), jnp.float32)
        for at in range(0, kd, step):
            read = columns[at : at + step, s : s + 1] * state[s, 0, at : at + step]
            total = total + jnp.sum(read.reshape(step // 8, 8, vd), axis=0)
        found.append(jnp.sum(total, axis=0, keepdims=True))
    attended = jnp.concatenate(found, axis=0) + fresh
    scale = lax.rsqrt(jnp.sum(attended * attended, axis=1, keepdims=True) / vd + epsilon)
    gains = jnp.concatenate([gain[i : i + 1] for i in range(gain.shape[0])], axis=1)
    gated = attended * scale * gains.astype(jnp.float32) * (g / (1.0 + jnp.exp(-g)))
    out_ref[...] = gated.astype(jnp.bfloat16)


def attend(sums, bias, gain, state, model_width):
    rows, _, kd, vd = state.shape
    return pl.pallas_call(
        functools.partial(attend_kernel, model_width=model_width),
        out_shape=(
            pltpu.VMEM((rows, kd), jnp.float32),
            pltpu.VMEM((rows, vd), jnp.float32),
            pltpu.VMEM((rows, kd), jnp.float32),
            pltpu.VMEM((rows, vd), jnp.bfloat16),
        ),
        in_specs=whole(4),
        out_specs=whole(4),
        compiler_params=pltpu.CompilerParams(vmem_limit_bytes=8 << 20),
        name="attend",
    )(*(in_vmem(a) for a in (sums, bias, gain, state)))


def join_kernel(heads, weights, out_ref):
    made = lax.dot_general(
        weights[...], heads[...], (((1,), (1,)), ((), ())), preferred_element_type=jnp.float32
    ).astype(jnp.bfloat16)
    for j in range(out_ref.shape[0]):
        out_ref[j] = made


def join(heads, weights, copies):
    return pl.pallas_call(
        join_kernel,
        out_shape=pltpu.VMEM((copies, weights.shape[0], heads.shape[0]), jnp.bfloat16),
        in_specs=whole(2),
        out_specs=pl.BlockSpec(memory_space=pltpu.VMEM),
        compiler_params=pltpu.CompilerParams(vmem_limit_bytes=8 << 20),
        name="join",
    )(*(in_vmem(a) for a in (heads, weights)))


def total_kernel(parts, out_ref):
    out_ref[...] = jnp.sum(parts[...].astype(jnp.float32), axis=1)


def total(parts):
    return pl.pallas_call(
        total_kernel,
        out_shape=pltpu.VMEM((parts.shape[0], *parts.shape[2:]), jnp.float32),
        in_specs=whole(1),
        out_specs=pl.BlockSpec(memory_space=pltpu.VMEM),
        compiler_params=pltpu.CompilerParams(vmem_limit_bytes=8 << 20),
        name="total",
    )(in_vmem(parts))


def widen_kernel(parts, mine, got, _, out_ref, mid_ref, *, alone):
    r = member(lax.axis_index("kv"))
    _, seqs = mid_ref.shape
    both = out_ref.shape[-1]
    end = both + alone

    def mid_of(ref, at):
        return (ref[:, end : end + seqs].astype(jnp.float32) + parts[at]).astype(jnp.bfloat16)

    own = mid_of(mine, r)
    mid_ref[...] = own
    x = jnp.concatenate([own, mid_of(got, 1 - r)], axis=0).astype(jnp.float32).T
    gains = mine[0:1, end + seqs :].astype(jnp.float32) + got[0:1, end + seqs :].astype(jnp.float32)
    ffn_in = (x * gains).astype(jnp.bfloat16)
    squares = jnp.sum(x * x, axis=1, keepdims=True)
    weights = jnp.concatenate([mine[:, :both], got[:, :both]], axis=0)
    made = jnp.dot(ffn_in, weights, preferred_element_type=jnp.float32)
    lane = lax.broadcasted_iota(jnp.int32, (seqs, 128), 1)
    last = jnp.where(lane == 127, squares, made[:, both - 128 :])
    made = jnp.concatenate([made[:, : both - 128], last], axis=1)
    out_ref[...] = made.reshape(out_ref.shape).astype(jnp.bfloat16)


def widen(parts, mine, got, new_state, units, count):
    width, seqs = parts.shape[1:]
    _, both, alone = widths(units)
    return pl.pallas_call(
        functools.partial(widen_kernel, alone=alone),
        out_shape=(
            pltpu.VMEM((count, seqs // count, both), jnp.bfloat16),
            pltpu.VMEM((width, seqs), jnp.bfloat16),
        ),
        in_specs=whole(4),
        out_specs=whole(2),
        compiler_params=pltpu.CompilerParams(vmem_limit_bytes=8 << 20),
        name="widen",
    )(*(in_vmem(a) for a in (parts, mine, got, new_state)))


def gate_kernel(sums, out_ref, *, half, model_width):
    rows, both = sums.shape
    alone = out_ref.shape[-1]
    rms = lax.rsqrt(sums[:, both - 1 :] / model_width + epsilon)
    gate = sums[:, :half] * rms
    up = sums[:, half : 2 * half] * rms
    hidden = gate / (1.0 + jnp.exp(-gate)) * up
    filled = jnp.concatenate([hidden, jnp.zeros((rows, alone - half), jnp.float32)], axis=1)
    out_ref[...] = jnp.broadcast_to(filled.astype(jnp.bfloat16)[None], out_ref.shape)


def gate_units(sums, units, model_width, copies):
    half, _, alone = widths(units)
    return pl.pallas_call(
        functools.partial(gate_kernel, half=half, model_width=model_width),
        out_shape=pltpu.VMEM((copies, sums.shape[0], alone), jnp.bfloat16),
        in_specs=whole(1),
        out_specs=pl.BlockSpec(memory_space=pltpu.VMEM),
        compiler_params=pltpu.CompilerParams(vmem_limit_bytes=8 << 20),
        name="gate",
    )(in_vmem(sums))


def narrow_kernel(hidden, mine, got, out_ref, *, both):
    r = member(lax.axis_index("kv"))
    alone = hidden.shape[1]
    copies, width = out_ref.shape[1:3]
    weights = jnp.concatenate([ref[:, both : both + alone] for ref in (mine, got)], axis=0)
    made = lax.dot_general(
        weights, hidden[...], (((1,), (1,)), ((), ())), preferred_element_type=jnp.float32
    ).astype(jnp.bfloat16)
    for j in range(copies):
        out_ref[r, j] = made[:width]
        out_ref[1 - r, j] = made[width:]


def narrow(hidden, mine, got, units, tp):
    width, seqs = (mine.shape[0], hidden.shape[0])
    return pl.pallas_call(
        functools.partial(narrow_kernel, both=widths(units)[1]),
        out_shape=pltpu.VMEM((2, tp, width, seqs), jnp.bfloat16),
        in_specs=whole(3),
        out_specs=pl.BlockSpec(memory_space=pltpu.VMEM),
        compiler_params=pltpu.CompilerParams(vmem_limit_bytes=8 << 20),
        name="narrow",
    )(*(in_vmem(a) for a in (hidden, mine, got)))


def exchanged(blocks, axis, groups=None):
    return lax.all_to_all(blocks, axis, 0, 0, axis_index_groups=groups, tiled=True)


def summed(blocks):
    return jnp.sum(blocks.astype(jnp.float32), axis=0)


def copies_of(x, count):
    return jnp.broadcast_to(x[None], (count, *x.shape))


def local(
    tokens,
    mix_gain,
    ffn_gain,
    w_query,
    w_key,
    w_value,
    w_gate,
    w_decay,
    decay_bias,
    head_gain,
    w_output,
    w_ffgate,
    w_ffup,
    w_down,
    state,
):
    own_rows, heads, _, val_dim = state.shape
    kv, tp = (lax.axis_size(a) for a in ("kv", "tp"))
    model_width = tokens.shape[1] * kv
    made, bias, head_scale, ffn_scale = project(
        tokens.T,
        mix_gain[None, :],
        (w_query, w_key, w_value, w_gate, w_decay),
        (decay_bias[None, :], head_gain.reshape(-1, 128), ffn_gain[None, :]),
    )
    arrived = exchanged(made.reshape(kv, own_rows, -1), "kv")
    keys, values, decay, head_out = attend(summed(arrived), bias, head_scale, state, model_width)
    heads_all = exchanged(copies_of(head_out, kv), "kv")
    mine, sent = pack(head_out, tokens.T, ffn_scale, (w_ffgate, w_ffup, w_down.T))
    got = lax.ppermute(sent, "kv", [(i, i ^ STRIDE) for i in range(kv)])
    new_state = (
        decay[:, None, :, None] * state + keys[:, None, :, None] * values[:, None, None, :]
    )
    heads_all = heads_all.reshape(-1, heads * val_dim)
    attn_copies = join(heads_all, w_output.T, 2 * tp)
    attn_copies, new_state = lax.optimization_barrier((attn_copies, new_state))
    width, seqs = attn_copies.shape[1:]
    pair, line = (pairs(kv, tp), lines(kv))
    attn_parts = exchanged(attn_copies, ("kv", "tp"), pair)
    units = w_ffgate.shape[1]
    attn_sums = total(attn_parts.reshape(2, tp, width, seqs))
    count = len(line[0])
    wide, mid_t = widen(attn_sums, mine, got, new_state, units, count)
    sums = summed(exchanged(wide, "kv", line))
    hidden = exchanged(gate_units(sums, units, model_width, count), "kv", line)
    down_parts = narrow(hidden.reshape(seqs, -1), mine, got, units, tp).reshape(2 * tp, width, seqs)
    mixed = (
        mid_t.astype(jnp.float32) + summed(exchanged(down_parts, ("kv", "tp"), pair))
    ).astype(jnp.bfloat16)
    return (mixed.T, new_state)


def solution(mesh):
    in_specs = (
        P(None, "kv"),
        P("kv"),
        P("kv"),
        P("kv", "tp"),
        P("kv", "tp"),
        P("kv", "tp"),
        P("kv", "tp"),
        P("kv", "tp"),
        P("tp"),
        P(),
        P("tp", "kv"),
        P("kv", "tp"),
        P("kv", "tp"),
        P("tp", "kv"),
        P("kv", "tp", None, None),
    )
    out_specs = (P(None, "kv"), P("kv", "tp", None, None))
    return jax.shard_map(local, mesh=mesh, in_specs=in_specs, out_specs=out_specs, check_vma=False)
```

```python
import functools

import jax
import jax.numpy as jnp
from jax import lax
from jax.experimental import pallas as pl
from jax.experimental.pallas import tpu as pltpu
from jax.sharding import PartitionSpec as P

epsilon = 1e-06


STRIDE = 8


def member(kv):
    place = kv // STRIDE
    return (place ^ (place >> 2)) & 1


def lines(kv):
    return [[i for i in range(kv) if member(i) == m] for m in range(2)]


def group_order(seqs, kv):
    block = STRIDE * seqs // kv
    places = range(kv // STRIDE)
    order = [i for m in range(2) for i in places if member(i * STRIDE) == m]
    at = lax.broadcasted_iota(jnp.int32, (seqs, seqs), 0)
    source = at
    for i, place in enumerate(order):
        inside = jnp.logical_and(at >= i * block, at < (i + 1) * block)
        source = jnp.where(inside, at + (place - i) * block, source)
    return source == lax.broadcasted_iota(jnp.int32, (seqs, seqs), 1)


def pairs(kv, tp):
    return [
        [i * tp + t for i in sorted((j, j ^ STRIDE), key=member) for t in range(tp)]
        for j in range(kv)
        if j < j ^ STRIDE
    ]


def padded(n):
    return -(-n // 128) * 128


def in_vmem(x):
    return pltpu.with_memory_space_constraint(x, pltpu.VMEM)


def whole(count):
    return [pl.BlockSpec(memory_space=pltpu.VMEM)] * count


def widths(units):
    half = units // 2
    return half, padded(2 * half + 1), padded(half)


def fetch(sources, held, sems):
    copies = [pltpu.make_async_copy(a, b, sems.at[i]) for i, (a, b) in enumerate(zip(sources, held))]
    for c in copies:
        c.start()
    return copies


def project_kernel(*refs, count, kept):
    sources, out_ref = (refs[:count], refs[count])
    held = refs[count + 1 + kept : -1] + refs[count + 1 : count + 1 + kept]
    copies = fetch(sources, held, refs[-1])
    for copy in copies:
        copy.wait()
    tok, gain = held[:2]
    x = tok[...].astype(jnp.float32).T
    mix_in = (x * gain[...].astype(jnp.float32)).astype(jnp.bfloat16)
    at = 0
    for w in held[2 : count - kept]:
        n = w.shape[1]
        part = jnp.dot(mix_in, w[...], preferred_element_type=jnp.float32)
        out_ref[:, at : at + n] = part.astype(jnp.bfloat16)
        at += n
    squares = jnp.sum(x * x, axis=1, keepdims=True)
    rest = out_ref.shape[1] - at
    lane = lax.broadcasted_iota(jnp.int32, (x.shape[0], rest), 1)
    out_ref[:, at:] = jnp.where(lane == 0, squares, 0.0).astype(jnp.bfloat16)


def project(tok_t, gain, weights, kept):
    total = sum(w.shape[1] for w in weights)
    arrays = (tok_t, gain, *weights, *kept)
    return pl.pallas_call(
        functools.partial(project_kernel, count=len(arrays), kept=len(kept)),
        out_shape=(
            pltpu.VMEM((tok_t.shape[1], total + 128), jnp.bfloat16),
            *(pltpu.VMEM(a.shape, a.dtype) for a in kept),
        ),
        in_specs=[pl.BlockSpec(memory_space=pl.ANY)] * len(arrays),
        out_specs=whole(1 + len(kept)),
        scratch_shapes=[pltpu.VMEM(a.shape, a.dtype) for a in arrays[: len(arrays) - len(kept)]]
        + [pltpu.SemaphoreType.DMA((len(arrays),))],
        name="project",
    )(*arrays)


def pack_kernel(_, tok, ffn_gain, *refs):
    splits, (mine_ref, sent_ref, order_ref) = (refs[:-3], refs[-3:])
    rows, units = splits[0].shape
    seqs = tok.shape[1]
    half, both, alone = widths(units)
    order = group_order(seqs, lax.axis_size("kv")).astype(jnp.float32).astype(jnp.bfloat16)
    order_ref[...] = order
    ordered = lax.dot_general(
        tok[...], order, (((1,), (1,)), ((), ())), preferred_element_type=jnp.float32
    ).astype(jnp.bfloat16)

    def fill(ref, m, first):
        gate, up, down = (w[:, m * half : (m + 1) * half] for w in splits)
        ref[:, :half] = gate
        ref[:, half : 2 * half] = up
        ref[:, 2 * half : both] = jnp.zeros((rows, both - 2 * half), ref.dtype)
        ref[:, both : both + half] = down
        ref[:, both + half : both + alone] = jnp.zeros((rows, alone - half), ref.dtype)
        end = both + alone
        ref[:, end : end + seqs] = ordered
        ref[:, end + seqs :] = jnp.zeros((rows, 2 * rows), ref.dtype)
        side = 0 if first else rows
        ref[0:1, end + seqs + side : end + seqs + side + rows] = ffn_gain[...]

    for m in range(2):

        @pl.when(member(lax.axis_index("kv")) == m)
        def _():
            fill(mine_ref, m, True)
            fill(sent_ref, 1 - m, False)


def pack(after, tok_t, ffn_gain, splits):
    width, rows = tok_t.shape
    lanes = sum(widths(splits[0].shape[1])[1:]) + rows + 2 * width
    arrays = (after, tok_t, ffn_gain, *splits)
    return pl.pallas_call(
        pack_kernel,
        out_shape=(
            pltpu.VMEM((width, lanes), jnp.bfloat16),
            pltpu.VMEM((width, lanes), jnp.bfloat16),
            pltpu.VMEM((rows, rows), jnp.bfloat16),
        ),
        in_specs=whole(len(arrays)),
        out_specs=whole(3),
        compiler_params=pltpu.CompilerParams(vmem_limit_bytes=8 << 20),
        name="pack",
    )(*(in_vmem(a) for a in arrays))


def attend_kernel(sums, bias, gain, state, key_ref, value_ref, decay_ref, out_ref, *, model_width):
    rows, _, kd, vd = state.shape
    base = sums[...]
    rms = lax.rsqrt(base[:, 3 * kd + 2 * vd : 3 * kd + 2 * vd + 1] / model_width + epsilon)
    q = base[:, :kd] * rms * kd**-0.5
    k = base[:, kd : 2 * kd] * rms
    v = base[:, 2 * kd : 2 * kd + vd] * rms
    g = base[:, 2 * kd + vd : 2 * kd + 2 * vd] * rms
    x = base[:, 2 * kd + 2 * vd : 3 * kd + 2 * vd] * rms + bias[...]
    log_sigmoid = jnp.minimum(x, 0.0) - jnp.log1p(jnp.exp(-jnp.abs(x)))
    decay = jnp.exp(log_sigmoid / 16.0)
    key_ref[...] = k
    value_ref[...] = v
    decay_ref[...] = decay
    fresh = jnp.sum(q * k, axis=1, keepdims=True) * v
    columns = jnp.concatenate([q * decay, jnp.zeros((8 - rows, kd), jnp.float32)], axis=0).T
    step = 32
    found = []
    for s in range(rows):
        total = jnp.zeros((8, vd), jnp.float32)
        for at in range(0, kd, step):
            read = columns[at : at + step, s : s + 1] * state[s, 0, at : at + step]
            total = total + jnp.sum(read.reshape(step // 8, 8, vd), axis=0)
        found.append(jnp.sum(total, axis=0, keepdims=True))
    attended = jnp.concatenate(found, axis=0) + fresh
    scale = lax.rsqrt(jnp.sum(attended * attended, axis=1, keepdims=True) / vd + epsilon)
    gains = jnp.concatenate([gain[i : i + 1] for i in range(gain.shape[0])], axis=1)
    gated = attended * scale * gains.astype(jnp.float32) * (g / (1.0 + jnp.exp(-g)))
    out_ref[...] = jnp.broadcast_to(gated.astype(jnp.bfloat16)[None], out_ref.shape)


def attend(sums, bias, gain, state, model_width, copies):
    rows, _, kd, vd = state.shape
    return pl.pallas_call(
        functools.partial(attend_kernel, model_width=model_width),
        out_shape=(
            pltpu.VMEM((rows, kd), jnp.float32),
            pltpu.VMEM((rows, vd), jnp.float32),
            pltpu.VMEM((rows, kd), jnp.float32),
            jax.ShapeDtypeStruct((copies, rows, vd), jnp.bfloat16),
        ),
        in_specs=whole(4),
        out_specs=whole(4),
        compiler_params=pltpu.CompilerParams(vmem_limit_bytes=8 << 20),
        name="attend",
    )(*(in_vmem(a) for a in (sums, bias, gain, state)))


def join_kernel(heads, own, other, out_ref, both):
    r = member(lax.axis_index("kv"))
    both[r] = own[...]
    both[1 - r] = other[...]
    weights = both[...].reshape(-1, own.shape[1])
    made = lax.dot_general(
        heads[...], weights, (((1,), (1,)), ((), ())), preferred_element_type=jnp.float32
    ).astype(jnp.bfloat16)
    for j in range(out_ref.shape[0]):
        out_ref[j] = made


def join(heads, own, other, copies):
    return pl.pallas_call(
        join_kernel,
        out_shape=pltpu.VMEM((copies, heads.shape[0], 2 * own.shape[0]), jnp.bfloat16),
        in_specs=whole(3),
        out_specs=pl.BlockSpec(memory_space=pltpu.VMEM),
        scratch_shapes=[pltpu.VMEM((2, *own.shape), own.dtype)],
        compiler_params=pltpu.CompilerParams(vmem_limit_bytes=8 << 20),
        name="join",
    )(*(in_vmem(a) for a in (heads, own, other)))


def total_kernel(parts, out_ref):
    out_ref[...] = jnp.sum(parts[...].astype(jnp.float32), axis=1)


def total(parts):
    return pl.pallas_call(
        total_kernel,
        out_shape=pltpu.VMEM((parts.shape[0], *parts.shape[2:]), jnp.float32),
        in_specs=whole(1),
        out_specs=pl.BlockSpec(memory_space=pltpu.VMEM),
        compiler_params=pltpu.CompilerParams(vmem_limit_bytes=8 << 20),
        name="total",
    )(in_vmem(parts))


def widen_kernel(parts, mine, got, order, _, out_ref, mid_ref, *, alone):
    r = member(lax.axis_index("kv"))
    width, seqs = mid_ref.shape
    both = out_ref.shape[-1]
    end = both + alone
    added = pltpu.roll(parts[...].reshape(seqs, 2 * width), r * width, 1)
    tokens = jnp.concatenate([ref[:, end : end + seqs] for ref in (mine, got)], axis=0)
    x = (tokens.astype(jnp.float32).T + added).astype(jnp.bfloat16).astype(jnp.float32)
    own = x.T[:width].astype(jnp.bfloat16)
    mid_ref[...] = jnp.dot(own, order[...], preferred_element_type=jnp.float32).astype(jnp.bfloat16)
    gains = mine[0:1, end + seqs :].astype(jnp.float32) + got[0:1, end + seqs :].astype(jnp.float32)
    ffn_in = (x * gains).astype(jnp.bfloat16)
    squares = jnp.sum(x * x, axis=1, keepdims=True)
    weights = jnp.concatenate([mine[:, :both], got[:, :both]], axis=0)
    made = jnp.dot(ffn_in, weights, preferred_element_type=jnp.float32)
    lane = lax.broadcasted_iota(jnp.int32, (seqs, 128), 1)
    last = jnp.where(lane == 127, squares, made[:, both - 128 :])
    made = jnp.concatenate([made[:, : both - 128], last], axis=1)
    out_ref[...] = made.reshape(out_ref.shape).astype(jnp.bfloat16)


def widen(parts, mine, got, order, new_state, units, count):
    width, seqs = (mine.shape[0], order.shape[0])
    _, both, alone = widths(units)
    return pl.pallas_call(
        functools.partial(widen_kernel, alone=alone),
        out_shape=(
            pltpu.VMEM((count, seqs // count, both), jnp.bfloat16),
            pltpu.VMEM((width, seqs), jnp.bfloat16),
        ),
        in_specs=whole(5),
        out_specs=whole(2),
        compiler_params=pltpu.CompilerParams(vmem_limit_bytes=8 << 20),
        name="widen",
    )(*(in_vmem(a) for a in (parts, mine, got, order, new_state)))


def gate_kernel(sums, out_ref, *, half, model_width):
    rows, both = sums.shape
    alone = out_ref.shape[-1]
    rms = lax.rsqrt(sums[:, both - 1 :] / model_width + epsilon)
    gate = sums[:, :half] * rms
    up = sums[:, half : 2 * half] * rms
    hidden = gate / (1.0 + jnp.exp(-gate)) * up
    filled = jnp.concatenate([hidden, jnp.zeros((rows, alone - half), jnp.float32)], axis=1)
    out_ref[...] = jnp.broadcast_to(filled.astype(jnp.bfloat16)[None], out_ref.shape)


def gate_units(sums, units, model_width, copies):
    half, _, alone = widths(units)
    return pl.pallas_call(
        functools.partial(gate_kernel, half=half, model_width=model_width),
        out_shape=pltpu.VMEM((copies, sums.shape[0], alone), jnp.bfloat16),
        in_specs=whole(1),
        out_specs=pl.BlockSpec(memory_space=pltpu.VMEM),
        compiler_params=pltpu.CompilerParams(vmem_limit_bytes=8 << 20),
        name="gate",
    )(in_vmem(sums))


def narrow_kernel(hidden, mine, got, order, out_ref, *, both):
    r = member(lax.axis_index("kv"))
    alone = hidden.shape[1]
    copies, width = out_ref.shape[1:3]
    weights = jnp.concatenate([ref[:, both : both + alone] for ref in (mine, got)], axis=0)
    made = lax.dot_general(
        weights, hidden[...], (((1,), (1,)), ((), ())), preferred_element_type=jnp.float32
    ).astype(jnp.bfloat16)
    made = jnp.dot(made, order[...], preferred_element_type=jnp.float32).astype(jnp.bfloat16)
    for j in range(copies):
        out_ref[r, j] = made[:width]
        out_ref[1 - r, j] = made[width:]


def narrow(hidden, mine, got, order, units, tp):
    width, seqs = (mine.shape[0], hidden.shape[0])
    return pl.pallas_call(
        functools.partial(narrow_kernel, both=widths(units)[1]),
        out_shape=pltpu.VMEM((2, tp, width, seqs), jnp.bfloat16),
        in_specs=whole(4),
        out_specs=pl.BlockSpec(memory_space=pltpu.VMEM),
        compiler_params=pltpu.CompilerParams(vmem_limit_bytes=8 << 20),
        name="narrow",
    )(*(in_vmem(a) for a in (hidden, mine, got, order)))


def exchanged(blocks, axis, groups=None):
    return lax.all_to_all(blocks, axis, 0, 0, axis_index_groups=groups, tiled=True)


def summed(blocks):
    return jnp.sum(blocks.astype(jnp.float32), axis=0)


def local(
    tokens,
    mix_gain,
    ffn_gain,
    w_query,
    w_key,
    w_value,
    w_gate,
    w_decay,
    decay_bias,
    head_gain,
    w_output,
    w_ffgate,
    w_ffup,
    w_down,
    state,
):
    own_rows, heads, _, _ = state.shape
    kv, tp = (lax.axis_size(a) for a in ("kv", "tp"))
    model_width = tokens.shape[1] * kv
    made, bias, head_scale, ffn_scale = project(
        tokens.T,
        mix_gain[None, :],
        (w_query, w_key, w_value, w_gate, w_decay),
        (decay_bias[None, :], head_gain.reshape(-1, 128), ffn_gain[None, :]),
    )
    arrived = exchanged(made.reshape(kv, own_rows, -1), "kv")
    pair, line, swap = (pairs(kv, tp), lines(kv), [(i, i ^ STRIDE) for i in range(kv)])
    count = len(line[0])
    seqs, width = tokens.shape
    units = w_ffgate.shape[1]
    keys, values, decay, head_out = attend(
        summed(arrived), bias, head_scale, state, model_width, count
    )
    heads = exchanged(head_out, "kv", line)
    other = lax.ppermute(w_output.T, "kv", swap)
    mine, sent, order = pack(keys, tokens.T, ffn_scale, (w_ffgate, w_ffup, w_down.T))
    got = lax.ppermute(sent, "kv", swap)
    new_state = (
        decay[:, None, :, None] * state + keys[:, None, :, None] * values[:, None, None, :]
    )
    attn_copies = join(heads.reshape(-1, heads.shape[2]), w_output.T, other, 2 * tp)
    attn_copies, new_state = lax.optimization_barrier((attn_copies, new_state))
    attn_parts = exchanged(attn_copies, ("kv", "tp"), pair)
    attn_sums = total(attn_parts.reshape(2, tp, *attn_parts.shape[1:]))
    wide, mid_t = widen(attn_sums, mine, got, order, new_state, units, count)
    sums = summed(exchanged(wide, "kv", line))
    hidden = exchanged(gate_units(sums, units, model_width, count), "kv", line)
    down_parts = narrow(hidden.reshape(seqs, -1), mine, got, order, units, tp)
    down_parts = down_parts.reshape(2 * tp, width, seqs)
    mixed = (
        mid_t.astype(jnp.float32) + summed(exchanged(down_parts, ("kv", "tp"), pair))
    ).astype(jnp.bfloat16)
    return (mixed.T, new_state)


def solution(mesh):
    in_specs = (
        P(None, "kv"),
        P("kv"),
        P("kv"),
        P("kv", "tp"),
        P("kv", "tp"),
        P("kv", "tp"),
        P("kv", "tp"),
        P("kv", "tp"),
        P("tp"),
        P(),
        P("tp", "kv"),
        P("kv", "tp"),
        P("kv", "tp"),
        P("tp", "kv"),
        P("kv", "tp", None, None),
    )
    out_specs = (P(None, "kv"), P("kv", "tp", None, None))
    return jax.shard_map(local, mesh=mesh, in_specs=in_specs, out_specs=out_specs, check_vma=False)
```

```python
import functools

import jax
import jax.numpy as jnp
from jax import lax
from jax.experimental import pallas as pl
from jax.experimental.pallas import tpu as pltpu
from jax.sharding import PartitionSpec as P

epsilon = 1e-06


STRIDE = 8


def member(kv):
    place = kv // STRIDE
    return (place ^ (place >> 2)) & 1


def lines(kv):
    return [[i for i in range(kv) if member(i) == m] for m in range(2)]


def group_order(seqs, kv):
    block = STRIDE * seqs // kv
    places = range(kv // STRIDE)
    order = [i for m in range(2) for i in places if member(i * STRIDE) == m]
    at = lax.broadcasted_iota(jnp.int32, (seqs, seqs), 0)
    source = at
    for i, place in enumerate(order):
        inside = jnp.logical_and(at >= i * block, at < (i + 1) * block)
        source = jnp.where(inside, at + (place - i) * block, source)
    return source == lax.broadcasted_iota(jnp.int32, (seqs, seqs), 1)


def pairs(kv, tp):
    return [
        [i * tp + t for i in sorted((j, j ^ STRIDE), key=member) for t in range(tp)]
        for j in range(kv)
        if j < j ^ STRIDE
    ]


def padded(n):
    return -(-n // 128) * 128


def in_vmem(x):
    return pltpu.with_memory_space_constraint(x, pltpu.VMEM)


def whole(count):
    return [pl.BlockSpec(memory_space=pltpu.VMEM)] * count


def widths(units):
    half = units // 2
    return half, padded(2 * half + 1), padded(half)


def fetch(sources, held, sems):
    copies = [pltpu.make_async_copy(a, b, sems.at[i]) for i, (a, b) in enumerate(zip(sources, held))]
    for c in copies:
        c.start()
    return copies


def project_kernel(*refs, count, kept):
    sources, out_ref = (refs[:count], refs[count])
    held = refs[count + 1 + kept : -1] + refs[count + 1 : count + 1 + kept]
    copies = fetch(sources, held, refs[-1])
    for copy in copies:
        copy.wait()
    tok, gain = held[:2]
    x = tok[...].astype(jnp.float32).T
    mix_in = (x * gain[...].astype(jnp.float32)).astype(jnp.bfloat16)
    at = 0
    for w in held[2 : count - kept]:
        n = w.shape[1]
        part = jnp.dot(mix_in, w[...], preferred_element_type=jnp.float32)
        out_ref[:, at : at + n] = part.astype(jnp.bfloat16)
        at += n
    squares = jnp.sum(x * x, axis=1, keepdims=True)
    rest = out_ref.shape[1] - at
    lane = lax.broadcasted_iota(jnp.int32, (x.shape[0], rest), 1)
    out_ref[:, at:] = jnp.where(lane == 0, squares, 0.0).astype(jnp.bfloat16)


def project(tok_t, gain, weights, kept):
    total = sum(w.shape[1] for w in weights)
    arrays = (tok_t, gain, *weights, *kept)
    return pl.pallas_call(
        functools.partial(project_kernel, count=len(arrays), kept=len(kept)),
        out_shape=(
            pltpu.VMEM((tok_t.shape[1], total + 128), jnp.bfloat16),
            *(pltpu.VMEM(a.shape, a.dtype) for a in kept),
        ),
        in_specs=[pl.BlockSpec(memory_space=pl.ANY)] * len(arrays),
        out_specs=whole(1 + len(kept)),
        scratch_shapes=[pltpu.VMEM(a.shape, a.dtype) for a in arrays[: len(arrays) - len(kept)]]
        + [pltpu.SemaphoreType.DMA((len(arrays),))],
        name="project",
    )(*arrays)


def pack_kernel(_, tok, ffn_gain, *refs):
    splits, (mine_ref, sent_ref, down_ref, order_ref) = (
        refs[:-4],
        refs[-4:],
    )
    rows, units = splits[0].shape
    seqs = tok.shape[1]
    half, both, alone = widths(units)
    order = group_order(seqs, lax.axis_size("kv")).astype(jnp.float32).astype(jnp.bfloat16)
    order_ref[...] = order
    ordered = lax.dot_general(
        tok[...], order, (((1,), (1,)), ((), ())), preferred_element_type=jnp.float32
    ).astype(jnp.bfloat16)

    def fill(ref, m, first):
        gate, up, down = (w[:, m * half : (m + 1) * half] for w in splits)
        ref[:, :half] = gate
        ref[:, half : 2 * half] = up
        ref[:, 2 * half : both] = jnp.zeros((rows, both - 2 * half), ref.dtype)
        ref[:, both : both + seqs] = ordered
        end = both + seqs + 2 * rows
        ref[:, both + seqs : end] = jnp.zeros((rows, 2 * rows), ref.dtype)
        side = both + seqs + (0 if first else rows)
        ref[0:1, side : side + rows] = ffn_gain[...]
        down_to, at = (ref, end) if first else (down_ref, 0)
        down_to[:, at : at + half] = down
        down_to[:, at + half : at + alone] = jnp.zeros((rows, alone - half), ref.dtype)

    for m in range(2):

        @pl.when(member(lax.axis_index("kv")) == m)
        def _():
            fill(mine_ref, m, True)
            fill(sent_ref, 1 - m, False)


def pack(after, tok_t, ffn_gain, splits):
    width, rows = tok_t.shape
    _, both, alone = widths(splits[0].shape[1])
    lanes = both + rows + 2 * width
    arrays = (after, tok_t, ffn_gain, *splits)
    return pl.pallas_call(
        pack_kernel,
        out_shape=(
            pltpu.VMEM((width, lanes + alone), jnp.bfloat16),
            pltpu.VMEM((width, lanes), jnp.bfloat16),
            pltpu.VMEM((width, alone), jnp.bfloat16),
            pltpu.VMEM((rows, rows), jnp.bfloat16),
        ),
        in_specs=whole(len(arrays)),
        out_specs=whole(4),
        compiler_params=pltpu.CompilerParams(vmem_limit_bytes=8 << 20),
        name="pack",
    )(*(in_vmem(a) for a in arrays))


def attend_kernel(sums, bias, gain, state, key_ref, value_ref, decay_ref, out_ref, *, model_width):
    rows, _, kd, vd = state.shape
    base = sums[...]
    rms = lax.rsqrt(base[:, 3 * kd + 2 * vd : 3 * kd + 2 * vd + 1] / model_width + epsilon)
    q = base[:, :kd] * rms * kd**-0.5
    k = base[:, kd : 2 * kd] * rms
    v = base[:, 2 * kd : 2 * kd + vd] * rms
    g = base[:, 2 * kd + vd : 2 * kd + 2 * vd] * rms
    x = base[:, 2 * kd + 2 * vd : 3 * kd + 2 * vd] * rms + bias[...]
    log_sigmoid = jnp.minimum(x, 0.0) - jnp.log1p(jnp.exp(-jnp.abs(x)))
    decay = jnp.exp(log_sigmoid / 16.0)
    key_ref[...] = k
    value_ref[...] = v
    decay_ref[...] = decay
    fresh = jnp.sum(q * k, axis=1, keepdims=True) * v
    columns = jnp.concatenate([q * decay, jnp.zeros((8 - rows, kd), jnp.float32)], axis=0).T
    step = 32
    found = []
    for s in range(rows):
        total = jnp.zeros((8, vd), jnp.float32)
        for at in range(0, kd, step):
            read = columns[at : at + step, s : s + 1] * state[s, 0, at : at + step]
            total = total + jnp.sum(read.reshape(step // 8, 8, vd), axis=0)
        found.append(jnp.sum(total, axis=0, keepdims=True))
    attended = jnp.concatenate(found, axis=0) + fresh
    scale = lax.rsqrt(jnp.sum(attended * attended, axis=1, keepdims=True) / vd + epsilon)
    gains = jnp.concatenate([gain[i : i + 1] for i in range(gain.shape[0])], axis=1)
    gated = attended * scale * gains.astype(jnp.float32) * (g / (1.0 + jnp.exp(-g)))
    out_ref[...] = jnp.broadcast_to(gated.astype(jnp.bfloat16)[None], out_ref.shape)


def attend(sums, bias, gain, state, model_width, copies):
    rows, _, kd, vd = state.shape
    return pl.pallas_call(
        functools.partial(attend_kernel, model_width=model_width),
        out_shape=(
            pltpu.VMEM((rows, kd), jnp.float32),
            pltpu.VMEM((rows, vd), jnp.float32),
            pltpu.VMEM((rows, kd), jnp.float32),
            jax.ShapeDtypeStruct((copies, rows, vd), jnp.bfloat16),
        ),
        in_specs=whole(4),
        out_specs=whole(4),
        compiler_params=pltpu.CompilerParams(vmem_limit_bytes=8 << 20),
        name="attend",
    )(*(in_vmem(a) for a in (sums, bias, gain, state)))


def join_kernel(heads, own, other, out_ref, both):
    r = member(lax.axis_index("kv"))
    both[r] = own[...]
    both[1 - r] = other[...]
    weights = both[...].reshape(-1, own.shape[1])
    made = lax.dot_general(
        heads[...], weights, (((1,), (1,)), ((), ())), preferred_element_type=jnp.float32
    ).astype(jnp.bfloat16)
    for j in range(out_ref.shape[0]):
        out_ref[j] = made


def join(heads, own, other, copies):
    return pl.pallas_call(
        join_kernel,
        out_shape=pltpu.VMEM((copies, heads.shape[0], 2 * own.shape[0]), jnp.bfloat16),
        in_specs=whole(3),
        out_specs=pl.BlockSpec(memory_space=pltpu.VMEM),
        scratch_shapes=[pltpu.VMEM((2, *own.shape), own.dtype)],
        compiler_params=pltpu.CompilerParams(vmem_limit_bytes=8 << 20),
        name="join",
    )(*(in_vmem(a) for a in (heads, own, other)))


def total_kernel(parts, out_ref):
    out_ref[...] = jnp.sum(parts[...].astype(jnp.float32), axis=1)


def total(parts):
    return pl.pallas_call(
        total_kernel,
        out_shape=pltpu.VMEM((parts.shape[0], *parts.shape[2:]), jnp.float32),
        in_specs=whole(1),
        out_specs=pl.BlockSpec(memory_space=pltpu.VMEM),
        compiler_params=pltpu.CompilerParams(vmem_limit_bytes=8 << 20),
        name="total",
    )(in_vmem(parts))


def widen_kernel(parts, mine, got, order, _, out_ref, mid_ref):
    r = member(lax.axis_index("kv"))
    width, seqs = mid_ref.shape
    both = out_ref.shape[-1]
    end = both
    added = pltpu.roll(parts[...].reshape(seqs, 2 * width), r * width, 1)
    tokens = jnp.concatenate([ref[:, end : end + seqs] for ref in (mine, got)], axis=0)
    x = (tokens.astype(jnp.float32).T + added).astype(jnp.bfloat16).astype(jnp.float32)
    own = x.T[:width].astype(jnp.bfloat16)
    mid_ref[...] = jnp.dot(own, order[...], preferred_element_type=jnp.float32).astype(jnp.bfloat16)
    row = slice(end + seqs, end + seqs + 2 * width)
    gains = mine[0:1, row].astype(jnp.float32) + got[0:1, row].astype(jnp.float32)
    ffn_in = (x * gains).astype(jnp.bfloat16)
    squares = jnp.sum(x * x, axis=1, keepdims=True)
    weights = jnp.concatenate([mine[:, :both], got[:, :both]], axis=0)
    made = jnp.dot(ffn_in, weights, preferred_element_type=jnp.float32)
    lane = lax.broadcasted_iota(jnp.int32, (seqs, 128), 1)
    last = jnp.where(lane == 127, squares, made[:, both - 128 :])
    made = jnp.concatenate([made[:, : both - 128], last], axis=1)
    out_ref[...] = made.reshape(out_ref.shape).astype(jnp.bfloat16)


def widen(parts, mine, got, order, new_state, units, count):
    width, seqs = (mine.shape[0], order.shape[0])
    both = widths(units)[1]
    return pl.pallas_call(
        widen_kernel,
        out_shape=(
            pltpu.VMEM((count, seqs // count, both), jnp.bfloat16),
            pltpu.VMEM((width, seqs), jnp.bfloat16),
        ),
        in_specs=whole(5),
        out_specs=whole(2),
        compiler_params=pltpu.CompilerParams(vmem_limit_bytes=8 << 20),
        name="widen",
    )(*(in_vmem(a) for a in (parts, mine, got, order, new_state)))


def gate_kernel(sums, out_ref, *, half, model_width):
    rows, both = sums.shape
    alone = out_ref.shape[-1]
    rms = lax.rsqrt(sums[:, both - 1 :] / model_width + epsilon)
    gate = sums[:, :half] * rms
    up = sums[:, half : 2 * half] * rms
    hidden = gate / (1.0 + jnp.exp(-gate)) * up
    filled = jnp.concatenate([hidden, jnp.zeros((rows, alone - half), jnp.float32)], axis=1)
    out_ref[...] = jnp.broadcast_to(filled.astype(jnp.bfloat16)[None], out_ref.shape)


def gate_units(sums, units, model_width, copies):
    half, _, alone = widths(units)
    return pl.pallas_call(
        functools.partial(gate_kernel, half=half, model_width=model_width),
        out_shape=pltpu.VMEM((copies, sums.shape[0], alone), jnp.bfloat16),
        in_specs=whole(1),
        out_specs=pl.BlockSpec(memory_space=pltpu.VMEM),
        compiler_params=pltpu.CompilerParams(vmem_limit_bytes=8 << 20),
        name="gate",
    )(in_vmem(sums))


def narrow_kernel(hidden, mine, got, order, out_ref):
    r = member(lax.axis_index("kv"))
    alone = hidden.shape[1]
    copies, width = out_ref.shape[1:3]
    weights = jnp.concatenate([mine[:, mine.shape[1] - alone :], got[...]], axis=0)
    made = lax.dot_general(
        weights, hidden[...], (((1,), (1,)), ((), ())), preferred_element_type=jnp.float32
    ).astype(jnp.bfloat16)
    made = jnp.dot(made, order[...], preferred_element_type=jnp.float32).astype(jnp.bfloat16)
    for j in range(copies):
        out_ref[r, j] = made[:width]
        out_ref[1 - r, j] = made[width:]


def narrow(hidden, mine, got, order, tp):
    width, seqs = (mine.shape[0], hidden.shape[0])
    return pl.pallas_call(
        narrow_kernel,
        out_shape=pltpu.VMEM((2, tp, width, seqs), jnp.bfloat16),
        in_specs=whole(4),
        out_specs=pl.BlockSpec(memory_space=pltpu.VMEM),
        compiler_params=pltpu.CompilerParams(vmem_limit_bytes=8 << 20),
        name="narrow",
    )(*(in_vmem(a) for a in (hidden, mine, got, order)))


def exchanged(blocks, axis, groups=None):
    return lax.all_to_all(blocks, axis, 0, 0, axis_index_groups=groups, tiled=True)


def summed(blocks):
    return jnp.sum(blocks.astype(jnp.float32), axis=0)


def local(
    tokens,
    mix_gain,
    ffn_gain,
    w_query,
    w_key,
    w_value,
    w_gate,
    w_decay,
    decay_bias,
    head_gain,
    w_output,
    w_ffgate,
    w_ffup,
    w_down,
    state,
):
    own_rows, heads, _, _ = state.shape
    kv, tp = (lax.axis_size(a) for a in ("kv", "tp"))
    model_width = tokens.shape[1] * kv
    made, bias, head_scale, ffn_scale = project(
        tokens.T,
        mix_gain[None, :],
        (w_query, w_key, w_value, w_gate, w_decay),
        (decay_bias[None, :], head_gain.reshape(-1, 128), ffn_gain[None, :]),
    )
    arrived = exchanged(made.reshape(kv, own_rows, -1), "kv")
    pair, line, swap = (pairs(kv, tp), lines(kv), [(i, i ^ STRIDE) for i in range(kv)])
    count = len(line[0])
    seqs, width = tokens.shape
    units = w_ffgate.shape[1]
    keys, values, decay, head_out = attend(
        summed(arrived), bias, head_scale, state, model_width, count
    )
    heads = exchanged(head_out, "kv", line)
    other = lax.ppermute(w_output.T, "kv", swap)
    mine, sent, sent_down, order = pack(keys, tokens.T, ffn_scale, (w_ffgate, w_ffup, w_down.T))
    got = lax.ppermute(sent, "kv", swap)
    got_down = lax.ppermute(sent_down, "kv", swap)
    new_state = (
        decay[:, None, :, None] * state + keys[:, None, :, None] * values[:, None, None, :]
    )
    attn_copies = join(heads.reshape(-1, heads.shape[2]), w_output.T, other, 2 * tp)
    attn_copies, new_state = lax.optimization_barrier((attn_copies, new_state))
    attn_parts = exchanged(attn_copies, ("kv", "tp"), pair)
    attn_sums = total(attn_parts.reshape(2, tp, *attn_parts.shape[1:]))
    wide, mid_t = widen(attn_sums, mine, got, order, new_state, units, count)
    sums = summed(exchanged(wide, "kv", line))
    hidden = gate_units(sums, units, model_width, count)
    hidden, got_down = lax.optimization_barrier((hidden, got_down))
    hidden = exchanged(hidden, "kv", line)
    down_parts = narrow(hidden.reshape(seqs, -1), mine, got_down, order, tp)
    down_parts = down_parts.reshape(2 * tp, width, seqs)
    mixed = (
        mid_t.astype(jnp.float32) + summed(exchanged(down_parts, ("kv", "tp"), pair))
    ).astype(jnp.bfloat16)
    return (mixed.T, new_state)


def solution(mesh):
    in_specs = (
        P(None, "kv"),
        P("kv"),
        P("kv"),
        P("kv", "tp"),
        P("kv", "tp"),
        P("kv", "tp"),
        P("kv", "tp"),
        P("kv", "tp"),
        P("tp"),
        P(),
        P("tp", "kv"),
        P("kv", "tp"),
        P("kv", "tp"),
        P("tp", "kv"),
        P("kv", "tp", None, None),
    )
    out_specs = (P(None, "kv"), P("kv", "tp", None, None))
    return jax.shard_map(local, mesh=mesh, in_specs=in_specs, out_specs=out_specs, check_vma=False)
```

```python
import functools

import jax
import jax.numpy as jnp
from jax import lax
from jax.experimental import pallas as pl
from jax.experimental.pallas import tpu as pltpu
from jax.sharding import PartitionSpec as P

epsilon = 1e-06


STRIDE = 8


def member(kv):
    place = kv // STRIDE
    return (place ^ (place >> 2)) & 1


def lines(kv):
    return [[i for i in range(kv) if member(i) == m] for m in range(2)]


def pairs(kv, tp):
    return [
        [i * tp + t for i in sorted((j, j ^ STRIDE), key=member) for t in range(tp)]
        for j in range(kv)
        if j < j ^ STRIDE
    ]


def padded(n):
    return -(-n // 128) * 128


def in_vmem(x):
    return pltpu.with_memory_space_constraint(x, pltpu.VMEM)


def whole(count):
    return [pl.BlockSpec(memory_space=pltpu.VMEM)] * count


def widths(units):
    half = units // 2
    return half, padded(2 * half + 1), padded(half)


def fetch(sources, held, sems):
    copies = [pltpu.make_async_copy(a, b, sems.at[i]) for i, (a, b) in enumerate(zip(sources, held))]
    for c in copies:
        c.start()
    return copies


def project_kernel(*refs, count, kept):
    sources, out_ref = (refs[:count], refs[count])
    held = refs[count + 1 + kept : -1] + refs[count + 1 : count + 1 + kept]
    copies = fetch(sources, held, refs[-1])
    for copy in copies:
        copy.wait()
    tok, gain = held[:2]
    x = tok[...].astype(jnp.float32).T
    mix_in = (x * gain[...].astype(jnp.float32)).astype(jnp.bfloat16)
    at = 0
    for w in held[2 : count - kept]:
        n = w.shape[1]
        part = jnp.dot(mix_in, w[...], preferred_element_type=jnp.float32)
        out_ref[:, at : at + n] = part.astype(jnp.bfloat16)
        at += n
    squares = jnp.sum(x * x, axis=1, keepdims=True)
    rest = out_ref.shape[1] - at
    lane = lax.broadcasted_iota(jnp.int32, (x.shape[0], rest), 1)
    out_ref[:, at:] = jnp.where(lane == 0, squares, 0.0).astype(jnp.bfloat16)


def project(tok_t, gain, weights, kept):
    total = sum(w.shape[1] for w in weights)
    arrays = (tok_t, gain, *weights, *kept)
    return pl.pallas_call(
        functools.partial(project_kernel, count=len(arrays), kept=len(kept)),
        out_shape=(
            pltpu.VMEM((tok_t.shape[1], total + 128), jnp.bfloat16),
            *(pltpu.VMEM(a.shape, a.dtype) for a in kept),
        ),
        in_specs=[pl.BlockSpec(memory_space=pl.ANY)] * len(arrays),
        out_specs=whole(1 + len(kept)),
        scratch_shapes=[pltpu.VMEM(a.shape, a.dtype) for a in arrays[: len(arrays) - len(kept)]]
        + [pltpu.SemaphoreType.DMA((len(arrays),))],
        name="project",
    )(*arrays)


def pack_kernel(_, tok, ffn_gain, *refs):
    splits, (mine_ref, sent_ref) = (refs[:-2], refs[-2:])
    rows, units = splits[0].shape
    seqs = tok.shape[1]
    half, both, alone = widths(units)

    def fill(ref, m, first):
        gate, up, down = (w[:, m * half : (m + 1) * half] for w in splits)
        ref[:, :half] = gate
        ref[:, half : 2 * half] = up
        ref[:, 2 * half : both] = jnp.zeros((rows, both - 2 * half), ref.dtype)
        ref[:, both : both + half] = down
        ref[:, both + half : both + alone] = jnp.zeros((rows, alone - half), ref.dtype)
        end = both + alone
        ref[:, end : end + seqs] = tok[...]
        ref[:, end + seqs :] = jnp.zeros((rows, 2 * rows), ref.dtype)
        side = 0 if first else rows
        ref[0:1, end + seqs + side : end + seqs + side + rows] = ffn_gain[...]

    for m in range(2):

        @pl.when(member(lax.axis_index("kv")) == m)
        def _():
            fill(mine_ref, m, True)
            fill(sent_ref, 1 - m, False)


def pack(after, tok_t, ffn_gain, splits):
    width, rows = tok_t.shape
    lanes = sum(widths(splits[0].shape[1])[1:]) + rows + 2 * width
    arrays = (after, tok_t, ffn_gain, *splits)
    return pl.pallas_call(
        pack_kernel,
        out_shape=(pltpu.VMEM((width, lanes), jnp.bfloat16),) * 2,
        in_specs=whole(len(arrays)),
        out_specs=whole(2),
        compiler_params=pltpu.CompilerParams(vmem_limit_bytes=8 << 20),
        name="pack",
    )(*(in_vmem(a) for a in arrays))


def attend_kernel(sums, bias, gain, state, key_ref, value_ref, decay_ref, out_ref, *, model_width):
    rows, _, kd, vd = state.shape
    base = sums[...]
    rms = lax.rsqrt(base[:, 3 * kd + 2 * vd : 3 * kd + 2 * vd + 1] / model_width + epsilon)
    q = base[:, :kd] * rms * kd**-0.5
    k = base[:, kd : 2 * kd] * rms
    v = base[:, 2 * kd : 2 * kd + vd] * rms
    g = base[:, 2 * kd + vd : 2 * kd + 2 * vd] * rms
    x = base[:, 2 * kd + 2 * vd : 3 * kd + 2 * vd] * rms + bias[...]
    log_sigmoid = jnp.minimum(x, 0.0) - jnp.log1p(jnp.exp(-jnp.abs(x)))
    decay = jnp.exp(log_sigmoid / 16.0)
    key_ref[...] = k
    value_ref[...] = v
    decay_ref[...] = decay
    fresh = jnp.sum(q * k, axis=1, keepdims=True) * v
    columns = jnp.concatenate([q * decay, jnp.zeros((8 - rows, kd), jnp.float32)], axis=0).T
    step = 32
    found = []
    for s in range(rows):
        total = jnp.zeros((8, vd), jnp.float32)
        for at in range(0, kd, step):
            read = columns[at : at + step, s : s + 1] * state[s, 0, at : at + step]
            total = total + jnp.sum(read.reshape(step // 8, 8, vd), axis=0)
        found.append(jnp.sum(total, axis=0, keepdims=True))
    attended = jnp.concatenate(found, axis=0) + fresh
    scale = lax.rsqrt(jnp.sum(attended * attended, axis=1, keepdims=True) / vd + epsilon)
    gains = jnp.concatenate([gain[i : i + 1] for i in range(gain.shape[0])], axis=1)
    gated = attended * scale * gains.astype(jnp.float32) * (g / (1.0 + jnp.exp(-g)))
    out_ref[...] = jnp.broadcast_to(gated.astype(jnp.bfloat16)[None], out_ref.shape)


def attend(sums, bias, gain, state, model_width, copies):
    rows, _, kd, vd = state.shape
    return pl.pallas_call(
        functools.partial(attend_kernel, model_width=model_width),
        out_shape=(
            pltpu.VMEM((rows, kd), jnp.float32),
            pltpu.VMEM((rows, vd), jnp.float32),
            pltpu.VMEM((rows, kd), jnp.float32),
            jax.ShapeDtypeStruct((copies, rows, vd), jnp.bfloat16),
        ),
        in_specs=whole(4),
        out_specs=whole(4),
        compiler_params=pltpu.CompilerParams(vmem_limit_bytes=8 << 20),
        name="attend",
    )(*(in_vmem(a) for a in (sums, bias, gain, state)))


def join_kernel(heads, weights, out_ref):
    made = lax.dot_general(
        weights[...], heads[...], (((1,), (1,)), ((), ())), preferred_element_type=jnp.float32
    ).astype(jnp.bfloat16)
    for j in range(out_ref.shape[0]):
        out_ref[j] = made


def join(heads, weights, copies):
    return pl.pallas_call(
        join_kernel,
        out_shape=pltpu.VMEM((copies, weights.shape[0], heads.shape[0]), jnp.bfloat16),
        in_specs=whole(2),
        out_specs=pl.BlockSpec(memory_space=pltpu.VMEM),
        compiler_params=pltpu.CompilerParams(vmem_limit_bytes=8 << 20),
        name="join",
    )(*(in_vmem(a) for a in (heads, weights)))


def total_kernel(parts, out_ref):
    out_ref[...] = jnp.sum(parts[...].astype(jnp.float32), axis=1)


def total(parts):
    return pl.pallas_call(
        total_kernel,
        out_shape=pltpu.VMEM((parts.shape[0], *parts.shape[2:]), jnp.float32),
        in_specs=whole(1),
        out_specs=pl.BlockSpec(memory_space=pltpu.VMEM),
        compiler_params=pltpu.CompilerParams(vmem_limit_bytes=8 << 20),
        name="total",
    )(in_vmem(parts))


def widen_kernel(parts, mine, got, _, out_ref, mid_ref, *, alone):
    r = member(lax.axis_index("kv"))
    _, seqs = mid_ref.shape
    both = out_ref.shape[-1]
    end = both + alone

    def mid_of(ref, at):
        return (ref[:, end : end + seqs].astype(jnp.float32) + parts[at]).astype(jnp.bfloat16)

    own = mid_of(mine, r)
    mid_ref[...] = own
    x = jnp.concatenate([own, mid_of(got, 1 - r)], axis=0).astype(jnp.float32).T
    gains = mine[0:1, end + seqs :].astype(jnp.float32) + got[0:1, end + seqs :].astype(jnp.float32)
    ffn_in = (x * gains).astype(jnp.bfloat16)
    squares = jnp.sum(x * x, axis=1, keepdims=True)
    weights = jnp.concatenate([mine[:, :both], got[:, :both]], axis=0)
    made = jnp.dot(ffn_in, weights, preferred_element_type=jnp.float32)
    lane = lax.broadcasted_iota(jnp.int32, (seqs, 128), 1)
    last = jnp.where(lane == 127, squares, made[:, both - 128 :])
    made = jnp.concatenate([made[:, : both - 128], last], axis=1)
    copies, per, _ = out_ref.shape
    for i in range(2):
        rows = made[i * seqs // 2 : (i + 1) * seqs // 2].reshape(copies, per // 2, both)
        out_ref[:, i * per // 2 : (i + 1) * per // 2] = rows.astype(jnp.bfloat16)


def widen(parts, mine, got, new_state, units, count):
    width, seqs = parts.shape[1:]
    _, both, alone = widths(units)
    return pl.pallas_call(
        functools.partial(widen_kernel, alone=alone),
        out_shape=(
            pltpu.VMEM((count, seqs // count, both), jnp.bfloat16),
            pltpu.VMEM((width, seqs), jnp.bfloat16),
        ),
        in_specs=whole(4),
        out_specs=whole(2),
        compiler_params=pltpu.CompilerParams(vmem_limit_bytes=8 << 20),
        name="widen",
    )(*(in_vmem(a) for a in (parts, mine, got, new_state)))


def gate_kernel(sums, out_ref, *, half, model_width):
    rows, both = sums.shape
    rms = lax.rsqrt(sums[:, both - 1 :] / model_width + epsilon)
    gate = sums[:, :half] * rms
    up = sums[:, half : 2 * half] * rms
    hidden = gate / (1.0 + jnp.exp(-gate)) * up
    beside = jnp.concatenate([hidden[: rows // 2], hidden[rows // 2 :]], axis=1)
    out_ref[...] = jnp.broadcast_to(beside.astype(jnp.bfloat16)[None], out_ref.shape)


def gate_units(sums, units, model_width, copies):
    half = units // 2
    return pl.pallas_call(
        functools.partial(gate_kernel, half=half, model_width=model_width),
        out_shape=pltpu.VMEM((copies, sums.shape[0] // 2, 2 * half), jnp.bfloat16),
        in_specs=whole(1),
        out_specs=pl.BlockSpec(memory_space=pltpu.VMEM),
        compiler_params=pltpu.CompilerParams(vmem_limit_bytes=8 << 20),
        name="gate",
    )(in_vmem(sums))


def narrow_kernel(hidden, mine, got, out_ref, *, both):
    r = member(lax.axis_index("kv"))
    half = hidden.shape[1] // 2
    copies, width = out_ref.shape[1:3]
    weights = jnp.concatenate([ref[:, both : both + half] for ref in (mine, got)], axis=0)
    ordered = jnp.concatenate([hidden[:, :half], hidden[:, half:]], axis=0)
    made = lax.dot_general(
        weights, ordered, (((1,), (1,)), ((), ())), preferred_element_type=jnp.float32
    ).astype(jnp.bfloat16)
    for j in range(copies):
        out_ref[r, j] = made[:width]
        out_ref[1 - r, j] = made[width:]


def narrow(hidden, mine, got, units, tp):
    width, seqs = (mine.shape[0], 2 * hidden.shape[0])
    return pl.pallas_call(
        functools.partial(narrow_kernel, both=widths(units)[1]),
        out_shape=pltpu.VMEM((2, tp, width, seqs), jnp.bfloat16),
        in_specs=whole(3),
        out_specs=pl.BlockSpec(memory_space=pltpu.VMEM),
        compiler_params=pltpu.CompilerParams(vmem_limit_bytes=8 << 20),
        name="narrow",
    )(*(in_vmem(a) for a in (hidden, mine, got)))


def exchanged(blocks, axis, groups=None):
    return lax.all_to_all(blocks, axis, 0, 0, axis_index_groups=groups, tiled=True)


def summed(blocks):
    return jnp.sum(blocks.astype(jnp.float32), axis=0)


def local(
    tokens,
    mix_gain,
    ffn_gain,
    w_query,
    w_key,
    w_value,
    w_gate,
    w_decay,
    decay_bias,
    head_gain,
    w_output,
    w_ffgate,
    w_ffup,
    w_down,
    state,
):
    own_rows, heads, _, val_dim = state.shape
    kv, tp = (lax.axis_size(a) for a in ("kv", "tp"))
    model_width = tokens.shape[1] * kv
    made, bias, head_scale, ffn_scale = project(
        tokens.T,
        mix_gain[None, :],
        (w_query, w_key, w_value, w_gate, w_decay),
        (decay_bias[None, :], head_gain.reshape(-1, 128), ffn_gain[None, :]),
    )
    arrived = exchanged(made.reshape(kv, own_rows, -1), "kv")
    keys, values, decay, head_out = attend(
        summed(arrived), bias, head_scale, state, model_width, kv
    )
    heads_all = exchanged(head_out, "kv")
    mine, sent = pack(keys, tokens.T, ffn_scale, (w_ffgate, w_ffup, w_down.T))
    got = lax.ppermute(sent, "kv", [(i, i ^ STRIDE) for i in range(kv)])
    new_state = (
        decay[:, None, :, None] * state + keys[:, None, :, None] * values[:, None, None, :]
    )
    heads_all = heads_all.reshape(-1, heads * val_dim)
    attn_copies = join(heads_all, w_output.T, 2 * tp)
    attn_copies, new_state = lax.optimization_barrier((attn_copies, new_state))
    width, seqs = attn_copies.shape[1:]
    pair, line = (pairs(kv, tp), lines(kv))
    attn_parts = exchanged(attn_copies, ("kv", "tp"), pair)
    units = w_ffgate.shape[1]
    attn_sums = total(attn_parts.reshape(2, tp, width, seqs))
    count = len(line[0])
    wide, mid_t = widen(attn_sums, mine, got, new_state, units, count)
    sums = summed(exchanged(wide, "kv", line))
    hidden = exchanged(gate_units(sums, units, model_width, count), "kv", line)
    down_parts = narrow(hidden.reshape(-1, units), mine, got, units, tp).reshape(2 * tp, width, seqs)
    mixed = (
        mid_t.astype(jnp.float32) + summed(exchanged(down_parts, ("kv", "tp"), pair))
    ).astype(jnp.bfloat16)
    return (mixed.T, new_state)


def solution(mesh):
    in_specs = (
        P(None, "kv"),
        P("kv"),
        P("kv"),
        P("kv", "tp"),
        P("kv", "tp"),
        P("kv", "tp"),
        P("kv", "tp"),
        P("kv", "tp"),
        P("tp"),
        P(),
        P("tp", "kv"),
        P("kv", "tp"),
        P("kv", "tp"),
        P("tp", "kv"),
        P("kv", "tp", None, None),
    )
    out_specs = (P(None, "kv"), P("kv", "tp", None, None))
    return jax.shard_map(local, mesh=mesh, in_specs=in_specs, out_specs=out_specs, check_vma=False)
```

```python
import functools

import jax
import jax.numpy as jnp
from jax import lax
from jax.experimental import pallas as pl
from jax.experimental.pallas import tpu as pltpu
from jax.sharding import PartitionSpec as P

epsilon = 1e-06


STRIDE = 8


def member(kv):
    place = kv // STRIDE
    return (place ^ (place >> 2)) & 1


def lines(kv):
    return [[i for i in range(kv) if member(i) == m] for m in range(2)]


def pairs(kv, tp):
    return [
        [i * tp + t for i in sorted((j, j ^ STRIDE), key=member) for t in range(tp)]
        for j in range(kv)
        if j < j ^ STRIDE
    ]


def padded(n):
    return -(-n // 128) * 128


def in_vmem(x):
    return pltpu.with_memory_space_constraint(x, pltpu.VMEM)


def whole(count):
    return [pl.BlockSpec(memory_space=pltpu.VMEM)] * count


def widths(units):
    half = units // 2
    return half, padded(2 * half + 1), padded(half)


def fetch(sources, held, sems):
    copies = [pltpu.make_async_copy(a, b, sems.at[i]) for i, (a, b) in enumerate(zip(sources, held))]
    for c in copies:
        c.start()
    return copies


def project_kernel(*refs, count, kept):
    sources, out_ref = (refs[:count], refs[count])
    held = refs[count + 1 + kept : -1] + refs[count + 1 : count + 1 + kept]
    copies = fetch(sources, held, refs[-1])
    for copy in copies[:2]:
        copy.wait()
    tok, gain = held[:2]
    x = tok[...].astype(jnp.float32).T
    mix_in = (x * gain[...].astype(jnp.float32)).astype(jnp.bfloat16)
    for copy in copies[2:]:
        copy.wait()
    at = 0
    for w in held[2 : count - kept]:
        n = w.shape[1]
        part = jnp.dot(mix_in, w[...], preferred_element_type=jnp.float32)
        out_ref[:, at : at + n] = part.astype(jnp.bfloat16)
        at += n
    squares = jnp.sum(x * x, axis=1, keepdims=True)
    rest = out_ref.shape[1] - at
    lane = lax.broadcasted_iota(jnp.int32, (x.shape[0], rest), 1)
    out_ref[:, at:] = jnp.where(lane == 0, squares, 0.0).astype(jnp.bfloat16)


def project(tok_t, gain, weights, kept):
    total = sum(w.shape[1] for w in weights)
    arrays = (tok_t, gain, *weights, *kept)
    return pl.pallas_call(
        functools.partial(project_kernel, count=len(arrays), kept=len(kept)),
        out_shape=(
            pltpu.VMEM((tok_t.shape[1], total + 128), jnp.bfloat16),
            *(pltpu.VMEM(a.shape, a.dtype) for a in kept),
        ),
        in_specs=[pl.BlockSpec(memory_space=pl.ANY)] * len(arrays),
        out_specs=whole(1 + len(kept)),
        scratch_shapes=[pltpu.VMEM(a.shape, a.dtype) for a in arrays[: len(arrays) - len(kept)]]
        + [pltpu.SemaphoreType.DMA((len(arrays),))],
        name="project",
    )(*arrays)


def pack_kernel(_, tok, ffn_gain, *refs):
    splits, (mine_ref, sent_ref) = (refs[:-2], refs[-2:])
    rows, units = splits[0].shape
    seqs = tok.shape[1]
    half, both, alone = widths(units)

    def fill(ref, m, first):
        gate, up, down = (w[:, m * half : (m + 1) * half] for w in splits)
        ref[:, :half] = gate
        ref[:, half : 2 * half] = up
        ref[:, 2 * half : both] = jnp.zeros((rows, both - 2 * half), ref.dtype)
        ref[:, both : both + half] = down
        ref[:, both + half : both + alone] = jnp.zeros((rows, alone - half), ref.dtype)
        end = both + alone
        ref[:, end : end + seqs] = tok[...]
        ref[:, end + seqs :] = jnp.zeros((rows, 2 * rows), ref.dtype)
        side = 0 if first else rows
        ref[0:1, end + seqs + side : end + seqs + side + rows] = ffn_gain[...]

    for m in range(2):

        @pl.when(member(lax.axis_index("kv")) == m)
        def _():
            fill(mine_ref, m, True)
            fill(sent_ref, 1 - m, False)


def pack(after, tok_t, ffn_gain, splits):
    width, rows = tok_t.shape
    lanes = sum(widths(splits[0].shape[1])[1:]) + rows + 2 * width
    arrays = (after, tok_t, ffn_gain, *splits)
    return pl.pallas_call(
        pack_kernel,
        out_shape=(pltpu.VMEM((width, lanes), jnp.bfloat16),) * 2,
        in_specs=whole(len(arrays)),
        out_specs=whole(2),
        compiler_params=pltpu.CompilerParams(vmem_limit_bytes=8 << 20),
        name="pack",
    )(*(in_vmem(a) for a in arrays))


def attend_kernel(sums, bias, gain, state, key_ref, value_ref, decay_ref, out_ref, *, model_width):
    rows, _, kd, vd = state.shape
    base = sums[...]
    rms = lax.rsqrt(base[:, 3 * kd + 2 * vd : 3 * kd + 2 * vd + 1] / model_width + epsilon)
    q = base[:, :kd] * rms * kd**-0.5
    k = base[:, kd : 2 * kd] * rms
    v = base[:, 2 * kd : 2 * kd + vd] * rms
    g = base[:, 2 * kd + vd : 2 * kd + 2 * vd] * rms
    x = base[:, 2 * kd + 2 * vd : 3 * kd + 2 * vd] * rms + bias[...]
    log_sigmoid = jnp.minimum(x, 0.0) - jnp.log1p(jnp.exp(-jnp.abs(x)))
    decay = jnp.exp(log_sigmoid / 16.0)
    key_ref[...] = k
    value_ref[...] = v
    decay_ref[...] = decay
    fresh = jnp.sum(q * k, axis=1, keepdims=True) * v
    columns = jnp.concatenate([q * decay, jnp.zeros((8 - rows, kd), jnp.float32)], axis=0).T
    step = 32
    found = []
    for s in range(rows):
        total = jnp.zeros((8, vd), jnp.float32)
        for at in range(0, kd, step):
            read = columns[at : at + step, s : s + 1] * state[s, 0, at : at + step]
            total = total + jnp.sum(read.reshape(step // 8, 8, vd), axis=0)
        found.append(jnp.sum(total, axis=0, keepdims=True))
    attended = jnp.concatenate(found, axis=0) + fresh
    scale = lax.rsqrt(jnp.sum(attended * attended, axis=1, keepdims=True) / vd + epsilon)
    gains = jnp.concatenate([gain[i : i + 1] for i in range(gain.shape[0])], axis=1)
    gated = attended * scale * gains.astype(jnp.float32) * (g / (1.0 + jnp.exp(-g)))
    out_ref[...] = jnp.broadcast_to(gated.astype(jnp.bfloat16)[None], out_ref.shape)


def attend(sums, bias, gain, state, model_width, copies):
    rows, _, kd, vd = state.shape
    return pl.pallas_call(
        functools.partial(attend_kernel, model_width=model_width),
        out_shape=(
            pltpu.VMEM((rows, kd), jnp.float32),
            pltpu.VMEM((rows, vd), jnp.float32),
            pltpu.VMEM((rows, kd), jnp.float32),
            jax.ShapeDtypeStruct((copies, rows, vd), jnp.bfloat16),
        ),
        in_specs=whole(4),
        out_specs=whole(4),
        compiler_params=pltpu.CompilerParams(vmem_limit_bytes=8 << 20),
        name="attend",
    )(*(in_vmem(a) for a in (sums, bias, gain, state)))


def join_kernel(heads, weights, out_ref):
    made = lax.dot_general(
        weights[...], heads[...], (((1,), (1,)), ((), ())), preferred_element_type=jnp.float32
    ).astype(jnp.bfloat16)
    for j in range(out_ref.shape[0]):
        out_ref[j] = made


def join(heads, weights, copies):
    return pl.pallas_call(
        join_kernel,
        out_shape=pltpu.VMEM((copies, weights.shape[0], heads.shape[0]), jnp.bfloat16),
        in_specs=whole(2),
        out_specs=pl.BlockSpec(memory_space=pltpu.VMEM),
        compiler_params=pltpu.CompilerParams(vmem_limit_bytes=8 << 20),
        name="join",
    )(*(in_vmem(a) for a in (heads, weights)))


def total_kernel(parts, out_ref):
    out_ref[...] = jnp.sum(parts[...].astype(jnp.float32), axis=1)


def total(parts):
    return pl.pallas_call(
        total_kernel,
        out_shape=pltpu.VMEM((parts.shape[0], *parts.shape[2:]), jnp.float32),
        in_specs=whole(1),
        out_specs=pl.BlockSpec(memory_space=pltpu.VMEM),
        compiler_params=pltpu.CompilerParams(vmem_limit_bytes=8 << 20),
        name="total",
    )(in_vmem(parts))


def widen_kernel(parts, mine, got, _, out_ref, mid_ref, *, alone):
    r = member(lax.axis_index("kv"))
    _, seqs = mid_ref.shape
    both = out_ref.shape[-1]
    end = both + alone

    def mid_of(ref, at):
        return (ref[:, end : end + seqs].astype(jnp.float32) + parts[at]).astype(jnp.bfloat16)

    own = mid_of(mine, r)
    mid_ref[...] = own
    x = jnp.concatenate([own, mid_of(got, 1 - r)], axis=0).astype(jnp.float32).T
    gains = mine[0:1, end + seqs :].astype(jnp.float32) + got[0:1, end + seqs :].astype(jnp.float32)
    ffn_in = (x * gains).astype(jnp.bfloat16)
    squares = jnp.sum(x * x, axis=1, keepdims=True)
    weights = jnp.concatenate([mine[:, :both], got[:, :both]], axis=0)
    made = jnp.dot(ffn_in, weights, preferred_element_type=jnp.float32)
    lane = lax.broadcasted_iota(jnp.int32, (seqs, 128), 1)
    last = jnp.where(lane == 127, squares, made[:, both - 128 :])
    made = jnp.concatenate([made[:, : both - 128], last], axis=1)
    out_ref[...] = made.reshape(out_ref.shape).astype(jnp.bfloat16)


def widen(parts, mine, got, new_state, units, count):
    width, seqs = parts.shape[1:]
    _, both, alone = widths(units)
    return pl.pallas_call(
        functools.partial(widen_kernel, alone=alone),
        out_shape=(
            pltpu.VMEM((count, seqs // count, both), jnp.bfloat16),
            pltpu.VMEM((width, seqs), jnp.bfloat16),
        ),
        in_specs=whole(4),
        out_specs=whole(2),
        compiler_params=pltpu.CompilerParams(vmem_limit_bytes=8 << 20),
        name="widen",
    )(*(in_vmem(a) for a in (parts, mine, got, new_state)))


def gate_kernel(sums, out_ref, *, half, model_width):
    rows, both = sums.shape
    alone = out_ref.shape[-1]
    rms = lax.rsqrt(sums[:, both - 1 :] / model_width + epsilon)
    gate = sums[:, :half] * rms
    up = sums[:, half : 2 * half] * rms
    hidden = gate / (1.0 + jnp.exp(-gate)) * up
    filled = jnp.concatenate([hidden, jnp.zeros((rows, alone - half), jnp.float32)], axis=1)
    out_ref[...] = jnp.broadcast_to(filled.astype(jnp.bfloat16)[None], out_ref.shape)


def gate_units(sums, units, model_width, copies):
    half, _, alone = widths(units)
    return pl.pallas_call(
        functools.partial(gate_kernel, half=half, model_width=model_width),
        out_shape=pltpu.VMEM((copies, sums.shape[0], alone), jnp.bfloat16),
        in_specs=whole(1),
        out_specs=pl.BlockSpec(memory_space=pltpu.VMEM),
        compiler_params=pltpu.CompilerParams(vmem_limit_bytes=8 << 20),
        name="gate",
    )(in_vmem(sums))


def narrow_kernel(hidden, mine, got, out_ref, *, both):
    r = member(lax.axis_index("kv"))
    alone = hidden.shape[1]
    copies, width = out_ref.shape[1:3]
    weights = jnp.concatenate([ref[:, both : both + alone] for ref in (mine, got)], axis=0)
    made = lax.dot_general(
        weights, hidden[...], (((1,), (1,)), ((), ())), preferred_element_type=jnp.float32
    ).astype(jnp.bfloat16)
    for j in range(copies):
        out_ref[r, j] = made[:width]
        out_ref[1 - r, j] = made[width:]


def narrow(hidden, mine, got, units, tp):
    width, seqs = (mine.shape[0], hidden.shape[0])
    return pl.pallas_call(
        functools.partial(narrow_kernel, both=widths(units)[1]),
        out_shape=pltpu.VMEM((2, tp, width, seqs), jnp.bfloat16),
        in_specs=whole(3),
        out_specs=pl.BlockSpec(memory_space=pltpu.VMEM),
        compiler_params=pltpu.CompilerParams(vmem_limit_bytes=8 << 20),
        name="narrow",
    )(*(in_vmem(a) for a in (hidden, mine, got)))


def exchanged(blocks, axis, groups=None):
    return lax.all_to_all(blocks, axis, 0, 0, axis_index_groups=groups, tiled=True)


def summed(blocks):
    return jnp.sum(blocks.astype(jnp.float32), axis=0)


def local(
    tokens,
    mix_gain,
    ffn_gain,
    w_query,
    w_key,
    w_value,
    w_gate,
    w_decay,
    decay_bias,
    head_gain,
    w_output,
    w_ffgate,
    w_ffup,
    w_down,
    state,
):
    own_rows, heads, _, val_dim = state.shape
    kv, tp = (lax.axis_size(a) for a in ("kv", "tp"))
    model_width = tokens.shape[1] * kv
    made, bias, head_scale, ffn_scale = project(
        tokens.T,
        mix_gain[None, :],
        (w_query, w_key, w_value, w_gate, w_decay),
        (decay_bias[None, :], head_gain.reshape(-1, 128), ffn_gain[None, :]),
    )
    arrived = exchanged(made.reshape(kv, own_rows, -1), "kv")
    keys, values, decay, head_out = attend(
        summed(arrived), bias, head_scale, state, model_width, kv
    )
    heads_all = exchanged(head_out, "kv")
    mine, sent = pack(keys, tokens.T, ffn_scale, (w_ffgate, w_ffup, w_down.T))
    got = lax.ppermute(sent, "kv", [(i, i ^ STRIDE) for i in range(kv)])
    new_state = (
        decay[:, None, :, None] * state + keys[:, None, :, None] * values[:, None, None, :]
    )
    heads_all = heads_all.reshape(-1, heads * val_dim)
    attn_copies = join(heads_all, w_output.T, 2 * tp)
    attn_copies, new_state = lax.optimization_barrier((attn_copies, new_state))
    width, seqs = attn_copies.shape[1:]
    pair, line = (pairs(kv, tp), lines(kv))
    attn_parts = exchanged(attn_copies, ("kv", "tp"), pair)
    units = w_ffgate.shape[1]
    attn_sums = total(attn_parts.reshape(2, tp, width, seqs))
    count = len(line[0])
    wide, mid_t = widen(attn_sums, mine, got, new_state, units, count)
    sums = summed(exchanged(wide, "kv", line))
    hidden = exchanged(gate_units(sums, units, model_width, count), "kv", line)
    down_parts = narrow(hidden.reshape(seqs, -1), mine, got, units, tp).reshape(2 * tp, width, seqs)
    mixed = (
        mid_t.astype(jnp.float32) + summed(exchanged(down_parts, ("kv", "tp"), pair))
    ).astype(jnp.bfloat16)
    return (mixed.T, new_state)


def solution(mesh):
    in_specs = (
        P(None, "kv"),
        P("kv"),
        P("kv"),
        P("kv", "tp"),
        P("kv", "tp"),
        P("kv", "tp"),
        P("kv", "tp"),
        P("kv", "tp"),
        P("tp"),
        P(),
        P("tp", "kv"),
        P("kv", "tp"),
        P("kv", "tp"),
        P("tp", "kv"),
        P("kv", "tp", None, None),
    )
    out_specs = (P(None, "kv"), P("kv", "tp", None, None))
    return jax.shard_map(local, mesh=mesh, in_specs=in_specs, out_specs=out_specs, check_vma=False)
```
